32 devices in a mesh: sp: 4 (over z), tp: 8 (over y, x, core).
Axes of the slice: x: 2, y: 2, z: 4, core: 2. Of those that a mesh axis runs over, the one named last changes fastest.
Arguments:
- latent: bfloat16 [1536, 2048], P('sp', 'tp'), may hold values from -12 to 12
- context: bfloat16 [512, 2048], P('sp', 'tp'), may hold values from -6 to 6
- cond: bfloat16 [2048], P('sp'), may hold values from -6 to 6
- cond_ctx: bfloat16 [2048], P('sp'), may hold values from -6 to 6
- w_mod: bfloat16 [2048, 3, 2048], P('sp', None, 'tp'), may hold values from -0.25 to 0.25
- g_norm: float32 [2048], P('tp'), may hold values from 0.1 to 1.9
- w_dq: bfloat16 [2048, 512], P('tp'), may hold values from -0.125 to 0.125
- w_dkv: bfloat16 [2048, 512], P('tp'), may hold values from -0.125 to 0.125
- w_kr: bfloat16 [2048, 64], P('tp'), may hold values from -0.125 to 0.125
- g_cq: float32 [512], replicated, may hold values from 0.5 to 32
- g_ckv: float32 [512], replicated, may hold values from 0.1 to 1.9
- w_uq: bfloat16 [512, 32, 192], P(None, 'tp'), may hold values from -0.25 to 0.25
- w_ukv: bfloat16 [512, 32, 256], P(None, 'tp'), may hold values from -0.25 to 0.25
- ctx_lift: float32 [32], P('tp'), may hold values from 1 to 3
- w_out: bfloat16 [32, 128, 2048], P('tp'), may hold values from -6 to 6
Outputs:
- mixed: bfloat16 [1536, 2048], P('sp', 'tp')
The draws below stay inside these ranges and needn't reach their ends.
All inputs are finite; a program needn't handle non-finite values.
Results may differ from the reference program's by a relative error of at most 0.025.
The reference program's roundings to bfloat16 on the way count: a program that leaves them out, or rounds other values in their place, can miss the bound.
Values may be sent and summed in bfloat16 or wider, within the bound.
No kernel may reach another device: no remote copies, remote signals or barrier semaphores. Data moves between devices by JAX's collectives and lax.ppermute only.
A program may use at most 64 MiB of HBM per device.

```python
import jax
import jax.numpy as jnp
from jax import lax

D = 2048
HEADS = 32
NOPE = 128
ROPE = 64
DV = 128
QR = 512
KVR = 512
GRID_W = 64
CTX = 512
TOKENS = 1536


def draw_latent(key, part):
    noise = jax.random.normal(jax.random.fold_in(key, 11), (TOKENS, D), jnp.float32)
    rough = jax.random.uniform(jax.random.fold_in(key, 12), (1, D), jnp.float32, 0.7, 1.4)
    rising = 0.5 * jnp.exp(jnp.log(3.0) * jnp.arange(D, dtype=jnp.float32) / (D - 1))
    values = noise * rough * rising
    return jnp.clip(values, -12.0, 12.0).astype(jnp.bfloat16)


def draw_g_cq(key, part):
    return jax.random.uniform(jax.random.fold_in(key, 21), (QR,), jnp.float32, 0.5, 1.5)


def raised(drawn, stream_key, source, target, blocks, factor):
    def block_of(position):
        return (jnp.arange(drawn.shape[position]) // (drawn.shape[position] // blocks)).reshape((-1,) + (1,) * (drawn.ndim - 1 - position))

    near = jax.random.permutation(stream_key, blocks)[block_of(target)]
    far = (block_of(target) + blocks // 2) % blocks
    return jnp.where((block_of(source) == near) | (block_of(source) == far), factor * drawn, drawn)


def levels(rng, shape, split, least, largest):
    level = 1.0
    for position, blocks in split:
        draws = jax.random.uniform(jax.random.fold_in(jax.random.fold_in(rng, 6), position), (blocks,), jnp.float32, least / len(split), largest / len(split))
        level = level * jnp.repeat(jnp.exp(draws), shape[position] // blocks).reshape((-1,) + (1,) * (len(shape) - 1 - position))
    return level


def gaussian(rng, shape, scale, most, pieces=(), kind=jnp.bfloat16):
    result = jax.random.normal(rng, shape, jnp.float32) * scale
    if len(pieces) > 0:
        result = levels(rng, shape, pieces, -0.22, 0.18) * result
    return jnp.clip(result, min=-most, max=most).astype(kind)


def noise_with(stream_key, shape, width, most, shards, heavy, kind=jnp.bfloat16):
    drawn = width * jax.random.normal(stream_key, shape, jnp.float32)
    if shards:
        drawn = drawn * levels(stream_key, shape, shards, -0.22, 0.18)
    return jnp.clip(raised(drawn, jax.random.fold_in(stream_key, 3), *heavy), -most, most).astype(kind)


def setup_inputs(seed: int = 0) -> dict:
    arg_keys = jax.random.split(jax.random.key(seed), 16)
    latent = draw_latent(jax.random.fold_in(arg_keys[15], 71), 0)
    context = gaussian(arg_keys[1], (CTX, D), 1.0, 6.0, ((0, 4), (1, 8)))
    cond = gaussian(arg_keys[2], (D,), 1.0, 6.0, ((0, 4),))
    cond_ctx = gaussian(arg_keys[3], (D,), 1.0, 6.0, ((0, 4),))
    w_mod = gaussian(arg_keys[4], (D, 3, D), (D // 4) ** -0.5, 0.25, ((0, 4), (2, 8)))
    g_norm = jnp.clip(1.0 + 0.18 * jax.random.normal(arg_keys[5], (D,), jnp.float32), 0.1, 1.9)
    w_dq = gaussian(arg_keys[6], (D, QR), D ** -0.5, 0.125, ((0, 8),))
    w_dkv = gaussian(arg_keys[7], (D, KVR), D ** -0.5, 0.125, ((0, 8),))
    w_kr = gaussian(arg_keys[8], (D, ROPE), D ** -0.5, 0.125, ((0, 8),))
    g_cq = draw_g_cq(jax.random.fold_in(arg_keys[15], 71), 0)
    g_ckv = jnp.clip(1.0 + 0.18 * jax.random.normal(arg_keys[10], (KVR,), jnp.float32), 0.1, 1.9)
    w_uq = gaussian(arg_keys[11], (QR, HEADS, NOPE + ROPE), QR ** -0.5, 0.25, ((1, 8),))
    w_ukv = gaussian(arg_keys[12], (KVR, HEADS, NOPE + DV), KVR ** -0.5, 0.25, ((1, 8),))
    ctx_lift = jnp.clip(1.0 + 2.0 * jax.random.uniform(arg_keys[13], (HEADS,), jnp.float32) ** levels(arg_keys[13], (HEADS,), ((0, 8),), -0.2, 0.2), 1.0, 3.0)
    w_out = noise_with(arg_keys[14], (HEADS, DV, D), ((TOKENS + CTX) ** 0.5 * (2 * HEADS * DV) ** -0.5), 6.0, ((0, 8),), (0, 2, 8, 2.0))
    return {"latent": latent, "context": context, "cond": cond, "cond_ctx": cond_ctx, "w_mod": w_mod, "g_norm": g_norm, "w_dq": w_dq, "w_dkv": w_dkv, "w_kr": w_kr, "g_cq": g_cq, "g_ckv": g_ckv, "w_uq": w_uq, "w_ukv": w_ukv, "ctx_lift": ctx_lift, "w_out": w_out}


EPS = 1e-06
THETA = 10000.0

def tables(positions):
    row = (positions // GRID_W).astype(jnp.float32)
    col = (positions % GRID_W).astype(jnp.float32)
    half = ROPE // 2
    inverse = 1.0 / THETA ** (jnp.arange(0, half, 2, dtype=jnp.float32) / half)
    angle = jnp.concatenate([row[:, None] * inverse, col[:, None] * inverse], axis=-1)
    return (jnp.cos(angle), jnp.sin(angle))

def rotate(values, cosine, sine):
    shape = values.shape
    quarter = ROPE // 4
    parts = values.reshape(shape[:-1] + (2, 2, quarter))
    extra = (1,) * (len(shape) - 2)
    cosine = cosine.reshape((shape[0],) + extra + (2, quarter))
    sine = sine.reshape((shape[0],) + extra + (2, quarter))
    front_section = parts[..., 0, :]
    second = parts[..., 1, :]
    turned = jnp.stack([front_section * cosine - second * sine, front_section * sine + second * cosine], axis=-2)
    return turned.reshape(shape)

def modulated(values, gain, modulation):
    values = values.astype(jnp.float32)
    sumsq = lax.optimization_barrier(jnp.sum(values * values, axis=1))
    scaled = values * lax.rsqrt(sumsq / D + EPS)[:, None] * gain
    return (scaled * (1.0 + modulation[1]) + modulation[0]).astype(jnp.bfloat16)

def low_norm(values, gain):
    scale = lax.rsqrt(lax.optimization_barrier(jnp.mean(values * values, axis=-1, keepdims=True)) + EPS)
    return (values * scale * gain).astype(jnp.bfloat16)

def reference(latent, context, cond, cond_ctx, w_mod, g_norm, w_dq, w_dkv, w_kr, g_cq, g_ckv, w_uq, w_ukv, ctx_lift, w_out):
    signal = jnp.stack([jax.nn.silu(cond.astype(jnp.float32)), jax.nn.silu(cond_ctx.astype(jnp.float32))]).astype(jnp.bfloat16)
    modulation = jnp.dot(signal, w_mod.reshape(D, 3 * D), preferred_element_type=jnp.float32).reshape(2, 3, D)
    lat_h = modulated(latent, g_norm, modulation[0])
    ctx_h = modulated(context, g_norm, modulation[1])
    lat_q = jnp.dot(lat_h, w_dq, preferred_element_type=jnp.float32)
    lat_kv = jnp.dot(lat_h, w_dkv, preferred_element_type=jnp.float32)
    lat_rot = jnp.dot(lat_h, w_kr, preferred_element_type=jnp.float32)
    ctx_kv = jnp.dot(ctx_h, w_dkv, preferred_element_type=jnp.float32)
    ctx_rot = jnp.dot(ctx_h, w_kr, preferred_element_type=jnp.float32)
    positions = jnp.arange(TOKENS, dtype=jnp.int32)
    cosine, sine = tables(positions)
    cq_n = low_norm(lat_q, g_cq)
    ckv_n = low_norm(lat_kv, g_ckv)
    ctx_ckv_n = low_norm(ctx_kv, g_ckv)
    lat_kr = rotate(lat_rot, cosine, sine).astype(jnp.bfloat16)
    ctx_kr = ctx_rot.astype(jnp.bfloat16)
    query = jnp.dot(cq_n, w_uq.reshape(QR, HEADS * (NOPE + ROPE)), preferred_element_type=jnp.float32)
    query = query.reshape(TOKENS, HEADS, NOPE + ROPE)
    query = jnp.concatenate([query[..., :NOPE], rotate(query[..., NOPE:], cosine, sine)], axis=-1).astype(jnp.bfloat16)
    up_weight = w_ukv.reshape(KVR, HEADS * (NOPE + DV))
    lat_pairs = jnp.dot(ckv_n, up_weight, preferred_element_type=jnp.float32).astype(jnp.bfloat16)
    ctx_pairs = jnp.dot(ctx_ckv_n, up_weight, preferred_element_type=jnp.float32).astype(jnp.bfloat16)
    pairs = jnp.concatenate([ctx_pairs, lat_pairs], axis=0).reshape(CTX + TOKENS, HEADS, NOPE + DV)
    rope_keys = jnp.concatenate([ctx_kr, lat_kr], axis=0)
    key_index = jnp.arange(CTX + TOKENS, dtype=jnp.int32)
    scale = (NOPE + ROPE) ** (-0.5)

    def one_head(inputs):
        head_query, head_pairs, lift = inputs
        keys = jnp.concatenate([head_pairs[:, :NOPE], rope_keys], axis=1)
        raw_affinity_matrix = jnp.dot(head_query, keys.T, preferred_element_type=jnp.float32) * scale
        raw_affinity_matrix = raw_affinity_matrix + jnp.where(key_index < CTX, lift, 0.0 * lift)[None, :]
        peak = lax.optimization_barrier(jnp.max(raw_affinity_matrix, axis=1, keepdims=True))
        probs = jnp.exp(raw_affinity_matrix - peak)
        total = lax.optimization_barrier(jnp.sum(probs, axis=1))
        summed = jnp.dot(probs.astype(jnp.bfloat16), head_pairs[:, NOPE:], preferred_element_type=jnp.float32)
        return (summed / total[:, None]).astype(jnp.bfloat16)
    heads_out = lax.map(one_head, (jnp.transpose(query, (1, 0, 2)), jnp.transpose(pairs, (1, 0, 2)), ctx_lift))
    branch = jnp.einsum('hqd,hde->qe', heads_out.astype(jnp.float32), w_out.astype(jnp.float32))
    return (latent.astype(jnp.float32) + modulation[0, 2] * branch).astype(jnp.bfloat16)
```

```python
import functools

import jax
import jax.numpy as jnp
from jax import lax
from jax.experimental import pallas as pl
from jax.experimental.pallas import tpu as pltpu
from jax.sharding import PartitionSpec as P

D = 2048
NOPE = 128
ROPE = 64
DV = 128
GRID_W = 64


EPS = 1e-06
THETA = 10000.0


def tables(positions):
    row = (positions // GRID_W).astype(jnp.float32)
    col = (positions % GRID_W).astype(jnp.float32)
    half = ROPE // 2
    inverse = 1.0 / THETA ** (jnp.arange(0, half, 2, dtype=jnp.float32) / half)
    angle = jnp.concatenate([row[:, None] * inverse, col[:, None] * inverse], axis=-1)
    return (jnp.cos(angle), jnp.sin(angle))


def rotate(values, cosine, sine):
    shape = values.shape
    quarter = ROPE // 4
    parts = values.reshape(shape[:-1] + (2, 2, quarter))
    extra = (1,) * (len(shape) - 2)
    cosine = cosine.reshape((shape[0],) + extra + (2, quarter))
    sine = sine.reshape((shape[0],) + extra + (2, quarter))
    front_section = parts[..., 0, :]
    second = parts[..., 1, :]
    turned = jnp.stack(
        [front_section * cosine - second * sine, front_section * sine + second * cosine], axis=-2
    )
    return turned.reshape(shape)


def modulated(values, sumsq, gain, modulation):
    scaled = values * lax.rsqrt(sumsq / D + EPS)[:, None] * gain
    return (scaled * (1.0 + modulation[1]) + modulation[0]).astype(jnp.bfloat16)


def low_norm(values, gain):
    scale = lax.rsqrt(jnp.mean(values * values, axis=-1, keepdims=True) + EPS)
    return (values * scale * gain).astype(jnp.bfloat16)


def plain_device(
    latent,
    context,
    cond,
    cond_ctx,
    w_mod,
    g_norm,
    w_dq,
    w_dkv,
    w_kr,
    g_cq,
    g_ckv,
    w_uq,
    w_ukv,
    ctx_lift,
    w_out,
):
    rows = latent.shape[0]
    device_attention_groups = w_uq.shape[1]
    signal = jnp.stack(
        [jax.nn.silu(cond.astype(jnp.float32)), jax.nn.silu(cond_ctx.astype(jnp.float32))]
    ).astype(jnp.bfloat16)
    partial_mod = jnp.dot(
        signal, w_mod.reshape(w_mod.shape[0], -1), preferred_element_type=jnp.float32
    )
    modulation = lax.psum(partial_mod.reshape(2, 3, -1), "sp")
    lat_f = latent.astype(jnp.float32)
    ctx_f = context.astype(jnp.float32)
    lat_sq, ctx_sq = lax.psum(
        (jnp.sum(lat_f * lat_f, axis=1), jnp.sum(ctx_f * ctx_f, axis=1)), "tp"
    )
    lat_h = modulated(lat_f, lat_sq, g_norm, modulation[0])
    ctx_h = modulated(ctx_f, ctx_sq, g_norm, modulation[1])
    positions = lax.axis_index("sp") * rows + jnp.arange(rows, dtype=jnp.int32)
    cosine, sine = tables(positions)
    lat_q, lat_kv, lat_rot, ctx_kv, ctx_rot = lax.psum(
        (
            jnp.dot(lat_h, w_dq, preferred_element_type=jnp.float32),
            jnp.dot(lat_h, w_dkv, preferred_element_type=jnp.float32),
            jnp.dot(lat_h, w_kr, preferred_element_type=jnp.float32),
            jnp.dot(ctx_h, w_dkv, preferred_element_type=jnp.float32),
            jnp.dot(ctx_h, w_kr, preferred_element_type=jnp.float32),
        ),
        "tp",
    )
    cq_n = low_norm(lat_q, g_cq)
    ckv_n = low_norm(lat_kv, g_ckv)
    lat_kr = rotate(lat_rot, cosine, sine).astype(jnp.bfloat16)
    ctx_ckv_n = low_norm(ctx_kv, g_ckv)
    ctx_kr = ctx_rot.astype(jnp.bfloat16)
    query = jnp.dot(cq_n, w_uq.reshape(w_uq.shape[0], -1), preferred_element_type=jnp.float32)
    query = query.reshape(rows, device_attention_groups, NOPE + ROPE)
    query = jnp.concatenate(
        [query[..., :NOPE], rotate(query[..., NOPE:], cosine, sine)], axis=-1
    ).astype(jnp.bfloat16)
    up_weight = w_ukv.reshape(w_ukv.shape[0], -1)
    scale = (NOPE + ROPE) ** (-0.5)

    def expand(compressed):
        return jnp.dot(compressed, up_weight, preferred_element_type=jnp.float32).astype(
            jnp.bfloat16
        )

    def unpack(front_section):
        return expand(front_section).reshape(
            front_section.shape[0], device_attention_groups, NOPE + DV
        )

    def merged_question_vector(
        cumulative_loop_values, front_section, spinning_section, affinity_offset
    ):
        peak, total, accum = cumulative_loop_values
        pairs = unpack(front_section)
        count = pairs.shape[0]
        keys = jnp.concatenate(
            [
                pairs[..., :NOPE],
                jnp.broadcast_to(
                    spinning_section[:, None, :], (count, device_attention_groups, ROPE)
                ),
            ],
            axis=-1,
        )
        raw_affinity_matrix = (
            jnp.einsum("qhd,khd->hqk", query, keys, preferred_element_type=jnp.float32) * scale
        )
        raw_affinity_matrix = raw_affinity_matrix + affinity_offset[:, None, None]
        fresh = jnp.maximum(peak, jnp.max(raw_affinity_matrix, axis=-1))
        probs = jnp.exp(raw_affinity_matrix - fresh[..., None])
        fade = jnp.exp(peak - fresh)
        total = total * fade + jnp.sum(probs, axis=-1)
        accum = accum * fade[..., None] + jnp.einsum(
            "hqk,khd->hqd",
            probs.astype(jnp.bfloat16),
            pairs[..., NOPE:],
            preferred_element_type=jnp.float32,
        )
        return (fresh, total, accum)

    blank_offset_matrix = jnp.zeros((device_attention_groups,), jnp.float32)
    start_carry = (
        jnp.full((device_attention_groups, rows), -1e30, jnp.float32),
        jnp.zeros((device_attention_groups, rows), jnp.float32),
        jnp.zeros((device_attention_groups, rows, DV), jnp.float32),
    )
    ctx_all_first, ctx_all_kr = (
        lax.all_gather(ctx_ckv_n, "sp", axis=0, tiled=True),
        lax.all_gather(ctx_kr, "sp", axis=0, tiled=True),
    )
    cumulative_loop_values = merged_question_vector(
        start_carry, ctx_all_first, ctx_all_kr, ctx_lift
    )
    fold_cumulative_loop_values = cumulative_loop_values
    front_section = lax.all_gather(ckv_n, "sp", axis=0, tiled=True)
    spinning_section = lax.all_gather(lat_kr, "sp", axis=0, tiled=True)
    count = front_section.shape[0] // rows
    blocks = (
        front_section.reshape(count, rows, front_section.shape[1]),
        spinning_section.reshape(count, rows, spinning_section.shape[1]),
    )

    def step(normalizer_statistics, segment_window):
        return (
            merged_question_vector(
                normalizer_statistics, segment_window[0], segment_window[1], blank_offset_matrix
            ),
            None,
        )

    fold_cumulative_loop_values, unused = lax.scan(step, fold_cumulative_loop_values, blocks)
    cumulative_loop_values = fold_cumulative_loop_values
    peak, total, accum = cumulative_loop_values
    heads_out = (accum / total[..., None]).astype(jnp.bfloat16)
    branch = jnp.einsum("hqd,hde->qe", heads_out, w_out, preferred_element_type=jnp.float32)
    branch = lax.psum_scatter(
        branch.astype(jnp.bfloat16), "tp", scatter_dimension=1, tiled=True
    ).astype(jnp.float32)
    return (lat_f + modulation[0, 2] * branch).astype(jnp.bfloat16)


def whole(shape):
    return pl.BlockSpec(shape, lambda *_: (0,) * len(shape))


def cost(flops, moved):
    return pl.CostEstimate(flops=int(flops), bytes_accessed=int(moved), transcendentals=0)


def project_kernel(lat_ref, ctx_ref, sq_ref, mod_ref, w_ref, out_ref, *, chunks):
    rows, ctx_rows = lat_ref.shape[1], ctx_ref.shape[1]
    total = jnp.sum(sq_ref[...], axis=0)
    inverse = lax.rsqrt(total / D + EPS)
    inverse = jnp.transpose(jnp.broadcast_to(inverse, (8, inverse.shape[1])))[:, :1]
    modulation = jnp.sum(mod_ref[...], axis=0)
    low = w_ref.shape[2] - 128
    half = low // 2
    lat_acc = ctx_acc = None
    for core in range(2):
        gain = mod_ref[0, core, 6:7, :]
        for kind in range(2):
            source = lat_ref if kind == 0 else ctx_ref
            factor = inverse[:rows] if kind == 0 else inverse[rows:]
            shift = modulation[core, 3 * kind : 3 * kind + 1, :]
            scale = modulation[core, 3 * kind + 1 : 3 * kind + 2, :]
            scaled = source[core].astype(jnp.float32) * factor * gain
            h = (scaled * (1.0 + scale) + shift).astype(jnp.bfloat16)
            weight = w_ref[core] if kind == 0 else w_ref[core, :, half:]
            term = jnp.dot(h, weight, preferred_element_type=jnp.float32)
            if kind == 0:
                lat_acc = term if lat_acc is None else lat_acc + term
            else:
                ctx_acc = term if ctx_acc is None else ctx_acc + term
    lat, ctx = rows // chunks, ctx_rows // chunks
    quarter = (lat + ctx) // 4
    for d in range(chunks):
        at = 0
        for slab in range(low // 128):
            out_ref[d, at : at + lat, :] = lat_acc[
                d * lat : (d + 1) * lat, slab * 128 : (slab + 1) * 128
            ]
            at += lat
        for slab in range(half // 128):
            out_ref[d, at : at + ctx, :] = ctx_acc[
                d * ctx : (d + 1) * ctx, slab * 128 : (slab + 1) * 128
            ]
            at += ctx
        rot = jnp.concatenate(
            [
                lat_acc[d * lat : (d + 1) * lat, low:],
                ctx_acc[d * ctx : (d + 1) * ctx, half:],
            ],
            axis=0,
        )[:, : ROPE // 2]
        out_ref[d, at : at + quarter, :] = jnp.concatenate(
            [rot[i * quarter : (i + 1) * quarter] for i in range(4)], axis=1
        )


def norm_kernel(part_ref, gq_ref, gkv_ref, tab_ref, kv_ref, cq_ref, *, lat, ctx):
    chips = part_ref.shape[0] // 2
    halves = []
    for core in range(2):
        acc = part_ref[core]
        for chip in range(1, chips):
            acc = acc + part_ref[2 * chip + core]
        halves.append(acc)
    rank = gq_ref.shape[1]
    slabs = rank // 256

    def columns(start, count):
        return jnp.concatenate(
            [
                half[start + i * count : start + (i + 1) * count]
                for half in halves
                for i in range(slabs)
            ],
            axis=1,
        )

    def normed(values, gain):
        factor = lax.rsqrt(jnp.mean(values * values, axis=1, keepdims=True) + EPS)
        return (values * factor * gain).astype(jnp.bfloat16)

    cq = normed(columns(0, lat), gq_ref[...])
    lat_kv = normed(columns(slabs * lat, lat), gkv_ref[...])
    at = 2 * slabs * lat
    ctx_kv = normed(columns(at, ctx), gkv_ref[...])
    at += slabs * ctx
    quarter = (lat + ctx) // 4
    width = ROPE // 2
    lat_rot, ctx_rot = [], []
    for core in range(2):
        packed = halves[core][at : at + quarter]
        rot = jnp.concatenate(
            [packed[:, i * width : (i + 1) * width] for i in range(4)], axis=0
        )
        turned = rot[:lat]
        swapped = jnp.concatenate([turned[:, width // 2 :], turned[:, : width // 2]], axis=1)
        lat_rot.append(turned * tab_ref[0, core] + swapped * tab_ref[1, core])
        ctx_rot.append(rot[lat:])
    zeros = jnp.zeros((lat + ctx, 128 - ROPE), jnp.float32)
    keys = jnp.concatenate(
        [jnp.concatenate(lat_rot, axis=1), jnp.concatenate(ctx_rot, axis=1)], axis=0
    )
    keys = jnp.concatenate([keys, zeros], axis=1).astype(jnp.bfloat16)
    compressed = jnp.concatenate([lat_kv, ctx_kv], axis=0)
    for copy in range(kv_ref.shape[0]):
        kv_ref[copy, :, :rank] = compressed
        kv_ref[copy, :, rank:] = keys
    for copy in range(cq_ref.shape[0]):
        cq_ref[copy] = cq


def attend_kernel(
    side_ref,
    lift_ref,
    cq_own_ref,
    cq_other_ref,
    kv_own_ref,
    kv_other_ref,
    tab_ref,
    wq_ref,
    wkv_ref,
    out_ref,
    cq_ref,
    kv_ref,
    key_ref,
    *,
    lat,
):
    head = pl.program_id(0)
    chips, count = cq_own_ref.shape[:2]
    rank = cq_own_ref.shape[2]
    block = kv_own_ref.shape[1]

    @pl.when(head == 0)
    def _():
        first = side_ref[0] == 0
        for chip in range(chips):
            own, other = cq_own_ref[chip], cq_other_ref[chip]
            cq_ref[2 * chip * count : (2 * chip + 1) * count] = jnp.where(first, own, other)
            cq_ref[(2 * chip + 1) * count : (2 * chip + 2) * count] = jnp.where(first, other, own)
            for side, ref in ((0, kv_own_ref), (1, kv_other_ref)):
                at = (side * chips + chip) * block
                kv_ref[at : at + block] = ref[chip, :, :rank]
                key_ref[at : at + block, NOPE:] = ref[chip, :, rank:]

    raw = jnp.dot(cq_ref[...], wq_ref[0], preferred_element_type=jnp.float32)
    turned = raw[:, NOPE:] * tab_ref[...]
    turned = turned + pltpu.roll(turned, ROPE, 1)
    query = jnp.concatenate([raw[:, :NOPE], turned], axis=1).astype(jnp.bfloat16)
    pairs = jnp.dot(kv_ref[...], wkv_ref[...], preferred_element_type=jnp.float32).astype(
        jnp.bfloat16
    )
    key_ref[:, :NOPE] = pairs[:, :NOPE]
    score = lax.dot_general(
        query, key_ref[...], (((1,), (1,)), ((), ())), preferred_element_type=jnp.float32
    )
    period = lat[0] + lat[1]
    position = lax.rem(lax.broadcasted_iota(jnp.int32, (1, score.shape[1]), 1), period)
    lift = jnp.where(position >= lat[0], lift_ref[head], 0.0)
    score = score * (NOPE + ROPE) ** -0.5 + lift
    peak = jnp.max(score, axis=1, keepdims=True)
    probs = jnp.exp(score - peak)
    total = jnp.sum(probs, axis=1, keepdims=True)
    summed = jnp.dot(
        probs.astype(jnp.bfloat16), pairs[:, NOPE:], preferred_element_type=jnp.float32
    )
    out_ref[...] = (summed / total).astype(jnp.bfloat16)


def output_kernel(heads_ref, w_ref, out_ref):
    acc = jnp.dot(heads_ref[0], w_ref[0], preferred_element_type=jnp.float32)
    acc = acc + jnp.dot(heads_ref[1], w_ref[1], preferred_element_type=jnp.float32)
    out_ref[0] = acc.astype(jnp.bfloat16)


def split_device(
    latent,
    context,
    cond,
    cond_ctx,
    w_mod,
    g_norm,
    w_dq,
    w_dkv,
    w_kr,
    g_cq,
    g_ckv,
    w_uq,
    w_ukv,
    ctx_lift,
    w_out,
):
    f32, bf16 = jnp.float32, jnp.bfloat16
    sp, tp = lax.axis_size("sp"), lax.axis_size("tp")
    chips = tp // 2
    rows, features = latent.shape
    ctx_rows = context.shape[0]
    heads = w_uq.shape[1]
    rank = w_dq.shape[1]
    lat, ctx = rows // tp, ctx_rows // tp
    pairs = [[2 * i, 2 * i + 1] for i in range(chips)]
    sides = [list(range(k, tp, 2)) for k in range(2)]
    columns = [[s * tp + 2 * c + k for s in range(sp) for k in range(2)] for c in range(chips)]
    me, side = lax.axis_index("tp"), lax.rem(lax.axis_index("tp"), 2)
    across = [(i, i ^ 1) for i in range(tp)]

    lat_f, ctx_f = latent.astype(f32), context.astype(f32)
    sums = jnp.concatenate([jnp.sum(lat_f * lat_f, axis=1), jnp.sum(ctx_f * ctx_f, axis=1)])
    sums = jnp.broadcast_to(sums[None, None], (tp, 1, sums.shape[0]))
    sums = lax.all_to_all(sums, "tp", 0, 0)
    signal = jnp.stack([jax.nn.silu(cond.astype(f32)), jax.nn.silu(cond_ctx.astype(f32))])
    partial = jnp.dot(
        signal.astype(bf16), w_mod.reshape(w_mod.shape[0], -1), preferred_element_type=f32
    ).reshape(6, features)
    partial = jnp.concatenate([partial, g_norm[None], jnp.zeros((1, features), f32)])
    partial = jnp.broadcast_to(partial[None], (2 * sp,) + partial.shape)
    partial = lax.all_to_all(partial, ("sp", "tp"), 0, 0, axis_index_groups=columns)
    partial = partial.reshape(sp, 2, 8, features)

    lat_pair = lax.all_gather(latent, "tp", axis_index_groups=pairs)
    ctx_pair = lax.all_gather(context, "tp", axis_index_groups=pairs)
    half = rank // 2
    w_down = jnp.stack(
        [
            jnp.concatenate(
                [
                    w_dq[:, k * half : (k + 1) * half],
                    w_dkv[:, k * half : (k + 1) * half],
                    w_kr[:, k * ROPE // 2 : (k + 1) * ROPE // 2],
                    jnp.zeros((features, 128 - ROPE // 2), bf16),
                ],
                axis=1,
            )
            for k in range(2)
        ]
    )
    w_down = lax.all_to_all(w_down, "tp", 0, 0, axis_index_groups=pairs)
    w_up = w_out.reshape(heads * DV, chips, 2, features).transpose(2, 0, 1, 3)
    w_up = w_up.reshape(2, heads * DV, chips * features)
    w_up = lax.all_to_all(w_up, "tp", 0, 0, axis_index_groups=pairs)

    height = 2 * half // 128 * lat + half // 128 * ctx + (lat + ctx) // 4
    part = pl.pallas_call(
        functools.partial(project_kernel, chunks=tp),
        out_shape=jax.ShapeDtypeStruct((tp, height, 128), f32),
        cost_estimate=cost(4 * (rows + ctx_rows) * features * (rank + 128), 4e6),
        name="project",
    )(lat_pair, ctx_pair, sums, partial, w_down)
    part = lax.all_to_all(part, "tp", 0, 0)

    positions = lax.axis_index("sp") * rows + jnp.arange(rows, dtype=jnp.int32)
    cosine, sine = tables(positions)
    quarter = ROPE // 4
    c0, c1, s0, s1 = cosine[:, :quarter], cosine[:, quarter:], sine[:, :quarter], sine[:, quarter:]
    q_tab = jnp.concatenate([c0, c0, c1, c1, -s0, s0, -s1, s1], axis=1)
    k_tab = lax.dynamic_slice_in_dim(q_tab, me * lat, lat, 0)
    k_tab = k_tab.reshape(lat, 2, 2, ROPE // 2).transpose(1, 2, 0, 3)
    kv, cq = pl.pallas_call(
        functools.partial(norm_kernel, lat=lat, ctx=ctx),
        out_shape=(
            jax.ShapeDtypeStruct((sp, lat + ctx, rank + 128), bf16),
            jax.ShapeDtypeStruct((chips, lat, rank), bf16),
        ),
        cost_estimate=cost(1e7, 2e6),
        name="norm",
    )(part, g_cq[None], g_ckv[None], k_tab)

    cq_own = lax.all_to_all(cq, "tp", 0, 0, axis_index_groups=sides)
    cq_other = lax.ppermute(cq_own, "tp", across)
    kv = lax.all_to_all(kv, "sp", 0, 0).reshape(1, sp * (lat + ctx), rank + 128)
    kv = jnp.broadcast_to(kv, (chips,) + kv.shape[1:])
    kv_own = lax.all_to_all(kv, "tp", 0, 0, axis_index_groups=sides)
    kv_other = lax.ppermute(kv_own, "tp", across)

    w_q = jnp.transpose(w_uq, (1, 0, 2))
    turn = w_q[..., NOPE:].reshape(heads, rank, 2, 2, quarter)[:, :, :, ::-1]
    w_q = jnp.concatenate([w_q, turn.reshape(heads, rank, ROPE)], axis=2)
    keys = sp * (rows + ctx_rows)
    heads_out = pl.pallas_call(
        functools.partial(attend_kernel, lat=(lat, ctx)),
        grid=(heads,),
        in_specs=[
            pl.BlockSpec(memory_space=pltpu.SMEM),
            pl.BlockSpec(memory_space=pltpu.SMEM),
            whole(cq_own.shape),
            whole(cq_own.shape),
            whole(kv_own.shape),
            whole(kv_own.shape),
            whole(q_tab.shape),
            pl.BlockSpec((1, rank, 2 * NOPE), lambda h: (h, 0, 0)),
            pl.BlockSpec((rank, NOPE + DV), lambda h: (0, h)),
        ],
        out_specs=pl.BlockSpec((rows, DV), lambda h: (0, h)),
        out_shape=jax.ShapeDtypeStruct((rows, heads * DV), bf16),
        scratch_shapes=[
            pltpu.VMEM((rows, rank), bf16),
            pltpu.VMEM((keys, rank), bf16),
            pltpu.VMEM((keys, 2 * NOPE), bf16),
        ],
        cost_estimate=cost(heads * 2 * keys * (rows * 384 + rank * 256), 8e6),
        compiler_params=pltpu.CompilerParams(vmem_limit_bytes=48 << 20),
        name="attend",
    )(
        side[None],
        ctx_lift,
        cq_own,
        cq_other,
        kv_own,
        kv_other,
        q_tab,
        w_q,
        w_ukv.reshape(rank, heads * (NOPE + DV)),
    )

    heads_out = lax.all_gather(heads_out, "tp", axis_index_groups=pairs)
    branch = pl.pallas_call(
        output_kernel,
        grid=(chips,),
        in_specs=[
            whole(heads_out.shape),
            pl.BlockSpec((2, heads * DV, features), lambda c: (0, 0, c)),
        ],
        out_specs=pl.BlockSpec((1, rows, features), lambda c: (c, 0, 0)),
        out_shape=jax.ShapeDtypeStruct((chips, rows, features), bf16),
        cost_estimate=cost(4 * rows * heads * DV * chips * features, 4e6),
        name="project_out",
    )(heads_out, w_up)
    branch = lax.all_to_all(branch, "tp", 0, 0, axis_index_groups=sides)
    gate = jnp.sum(partial, axis=0)[side, 2]
    return (lat_f + gate * jnp.sum(branch.astype(f32), axis=0)).astype(bf16)


def per_device(*arrays):
    rows, ctx_rows, features = arrays[0].shape[0], arrays[1].shape[0], arrays[0].shape[1]
    tp = lax.axis_size("tp")
    aligned = rows % (16 * tp) == 0 and ctx_rows % (16 * tp) == 0 and features % 128 == 0
    return (split_device if tp % 2 == 0 and aligned else plain_device)(*arrays)


def solution(mesh):
    return jax.shard_map(
        per_device,
        mesh=mesh,
        in_specs=(
            P("sp", "tp"),
            P("sp", "tp"),
            P("sp"),
            P("sp"),
            P("sp", None, "tp"),
            P("tp"),
            P("tp", None),
            P("tp", None),
            P("tp", None),
            P(),
            P(),
            P(None, "tp", None),
            P(None, "tp", None),
            P("tp"),
            P("tp", None, None),
        ),
        out_specs=P("sp", "tp"),
        check_vma=False,
    )
```

```python
import functools

import jax
import jax.numpy as jnp
from jax import lax
from jax.experimental import pallas as pl
from jax.experimental.pallas import tpu as pltpu
from jax.sharding import PartitionSpec as P

D = 2048
NOPE = 128
ROPE = 64
DV = 128
GRID_W = 64


EPS = 1e-06
THETA = 10000.0


def tables(positions):
    row = (positions // GRID_W).astype(jnp.float32)
    col = (positions % GRID_W).astype(jnp.float32)
    half = ROPE // 2
    inverse = 1.0 / THETA ** (jnp.arange(0, half, 2, dtype=jnp.float32) / half)
    angle = jnp.concatenate([row[:, None] * inverse, col[:, None] * inverse], axis=-1)
    return (jnp.cos(angle), jnp.sin(angle))


def rotate(values, cosine, sine):
    shape = values.shape
    quarter = ROPE // 4
    parts = values.reshape(shape[:-1] + (2, 2, quarter))
    extra = (1,) * (len(shape) - 2)
    cosine = cosine.reshape((shape[0],) + extra + (2, quarter))
    sine = sine.reshape((shape[0],) + extra + (2, quarter))
    front_section = parts[..., 0, :]
    second = parts[..., 1, :]
    turned = jnp.stack(
        [front_section * cosine - second * sine, front_section * sine + second * cosine], axis=-2
    )
    return turned.reshape(shape)


def modulated(values, sumsq, gain, modulation):
    scaled = values * lax.rsqrt(sumsq / D + EPS)[:, None] * gain
    return (scaled * (1.0 + modulation[1]) + modulation[0]).astype(jnp.bfloat16)


def low_norm(values, gain):
    scale = lax.rsqrt(jnp.mean(values * values, axis=-1, keepdims=True) + EPS)
    return (values * scale * gain).astype(jnp.bfloat16)


def plain_device(
    latent,
    context,
    cond,
    cond_ctx,
    w_mod,
    g_norm,
    w_dq,
    w_dkv,
    w_kr,
    g_cq,
    g_ckv,
    w_uq,
    w_ukv,
    ctx_lift,
    w_out,
):
    rows = latent.shape[0]
    device_attention_groups = w_uq.shape[1]
    signal = jnp.stack(
        [jax.nn.silu(cond.astype(jnp.float32)), jax.nn.silu(cond_ctx.astype(jnp.float32))]
    ).astype(jnp.bfloat16)
    partial_mod = jnp.dot(
        signal, w_mod.reshape(w_mod.shape[0], -1), preferred_element_type=jnp.float32
    )
    modulation = lax.psum(partial_mod.reshape(2, 3, -1), "sp")
    lat_f = latent.astype(jnp.float32)
    ctx_f = context.astype(jnp.float32)
    lat_sq, ctx_sq = lax.psum(
        (jnp.sum(lat_f * lat_f, axis=1), jnp.sum(ctx_f * ctx_f, axis=1)), "tp"
    )
    lat_h = modulated(lat_f, lat_sq, g_norm, modulation[0])
    ctx_h = modulated(ctx_f, ctx_sq, g_norm, modulation[1])
    positions = lax.axis_index("sp") * rows + jnp.arange(rows, dtype=jnp.int32)
    cosine, sine = tables(positions)
    lat_q, lat_kv, lat_rot, ctx_kv, ctx_rot = lax.psum(
        (
            jnp.dot(lat_h, w_dq, preferred_element_type=jnp.float32),
            jnp.dot(lat_h, w_dkv, preferred_element_type=jnp.float32),
            jnp.dot(lat_h, w_kr, preferred_element_type=jnp.float32),
            jnp.dot(ctx_h, w_dkv, preferred_element_type=jnp.float32),
            jnp.dot(ctx_h, w_kr, preferred_element_type=jnp.float32),
        ),
        "tp",
    )
    cq_n = low_norm(lat_q, g_cq)
    ckv_n = low_norm(lat_kv, g_ckv)
    lat_kr = rotate(lat_rot, cosine, sine).astype(jnp.bfloat16)
    ctx_ckv_n = low_norm(ctx_kv, g_ckv)
    ctx_kr = ctx_rot.astype(jnp.bfloat16)
    query = jnp.dot(cq_n, w_uq.reshape(w_uq.shape[0], -1), preferred_element_type=jnp.float32)
    query = query.reshape(rows, device_attention_groups, NOPE + ROPE)
    query = jnp.concatenate(
        [query[..., :NOPE], rotate(query[..., NOPE:], cosine, sine)], axis=-1
    ).astype(jnp.bfloat16)
    up_weight = w_ukv.reshape(w_ukv.shape[0], -1)
    scale = (NOPE + ROPE) ** (-0.5)

    def expand(compressed):
        return jnp.dot(compressed, up_weight, preferred_element_type=jnp.float32).astype(
            jnp.bfloat16
        )

    def unpack(front_section):
        return expand(front_section).reshape(
            front_section.shape[0], device_attention_groups, NOPE + DV
        )

    def merged_question_vector(
        cumulative_loop_values, front_section, spinning_section, affinity_offset
    ):
        peak, total, accum = cumulative_loop_values
        pairs = unpack(front_section)
        count = pairs.shape[0]
        keys = jnp.concatenate(
            [
                pairs[..., :NOPE],
                jnp.broadcast_to(
                    spinning_section[:, None, :], (count, device_attention_groups, ROPE)
                ),
            ],
            axis=-1,
        )
        raw_affinity_matrix = (
            jnp.einsum("qhd,khd->hqk", query, keys, preferred_element_type=jnp.float32) * scale
        )
        raw_affinity_matrix = raw_affinity_matrix + affinity_offset[:, None, None]
        fresh = jnp.maximum(peak, jnp.max(raw_affinity_matrix, axis=-1))
        probs = jnp.exp(raw_affinity_matrix - fresh[..., None])
        fade = jnp.exp(peak - fresh)
        total = total * fade + jnp.sum(probs, axis=-1)
        accum = accum * fade[..., None] + jnp.einsum(
            "hqk,khd->hqd",
            probs.astype(jnp.bfloat16),
            pairs[..., NOPE:],
            preferred_element_type=jnp.float32,
        )
        return (fresh, total, accum)

    blank_offset_matrix = jnp.zeros((device_attention_groups,), jnp.float32)
    start_carry = (
        jnp.full((device_attention_groups, rows), -1e30, jnp.float32),
        jnp.zeros((device_attention_groups, rows), jnp.float32),
        jnp.zeros((device_attention_groups, rows, DV), jnp.float32),
    )
    ctx_all_first, ctx_all_kr = (
        lax.all_gather(ctx_ckv_n, "sp", axis=0, tiled=True),
        lax.all_gather(ctx_kr, "sp", axis=0, tiled=True),
    )
    cumulative_loop_values = merged_question_vector(
        start_carry, ctx_all_first, ctx_all_kr, ctx_lift
    )
    fold_cumulative_loop_values = cumulative_loop_values
    front_section = lax.all_gather(ckv_n, "sp", axis=0, tiled=True)
    spinning_section = lax.all_gather(lat_kr, "sp", axis=0, tiled=True)
    count = front_section.shape[0] // rows
    blocks = (
        front_section.reshape(count, rows, front_section.shape[1]),
        spinning_section.reshape(count, rows, spinning_section.shape[1]),
    )

    def step(normalizer_statistics, segment_window):
        return (
            merged_question_vector(
                normalizer_statistics, segment_window[0], segment_window[1], blank_offset_matrix
            ),
            None,
        )

    fold_cumulative_loop_values, unused = lax.scan(step, fold_cumulative_loop_values, blocks)
    cumulative_loop_values = fold_cumulative_loop_values
    peak, total, accum = cumulative_loop_values
    heads_out = (accum / total[..., None]).astype(jnp.bfloat16)
    branch = jnp.einsum("hqd,hde->qe", heads_out, w_out, preferred_element_type=jnp.float32)
    branch = lax.psum_scatter(
        branch.astype(jnp.bfloat16), "tp", scatter_dimension=1, tiled=True
    ).astype(jnp.float32)
    return (lat_f + modulation[0, 2] * branch).astype(jnp.bfloat16)


def call(kernel, outs, *args, flops=1e6, scratch=(), limit=8, name=None, held=True, kept=True):
    single = not isinstance(outs, tuple)
    vmem = pl.BlockSpec(memory_space=pltpu.VMEM)
    outs = (outs,) if single else outs
    if kept:
        outs = tuple(pltpu.VMEM(o.shape, o.dtype) for o in outs)
    if held:
        args = tuple(pltpu.with_memory_space_constraint(a, pltpu.VMEM) for a in args)
    result = pl.pallas_call(
        kernel,
        in_specs=[vmem] * len(args),
        out_specs=(vmem,) * len(outs),
        out_shape=outs,
        scratch_shapes=scratch,
        cost_estimate=pl.CostEstimate(
            flops=int(flops), bytes_accessed=int(1e5), transcendentals=0
        ),
        compiler_params=pltpu.CompilerParams(vmem_limit_bytes=limit << 20),
        name=name,
    )(*args)
    return result[0] if single else result


def place():
    me = lax.axis_index("tp")
    return lax.axis_index("sp") * lax.axis_size("tp"), me // 2, lax.rem(me, 2), me


def dot_t(left, right, **options):
    return lax.dot_general(
        left, right, (((1,), (1,)), ((), ())), preferred_element_type=jnp.float32, **options
    )


def share_kernel(wq_ref, wkv_ref, wr_ref, own_ref, other_ref):
    features, rank = wq_ref.shape
    half, width = rank // 2, ROPE // 2
    side = place()[2]
    for which, ref in ((side, own_ref), (1 - side, other_ref)):
        start = pl.multiple_of(which * half, half)
        ref[:features, :half] = wq_ref[:, pl.ds(start, half)]
        ref[:features, half:] = wkv_ref[:, pl.ds(start, half)]
        low = pl.multiple_of(which * width, width)
        rot = wr_ref[pl.ds(low, width), :]
        count = width * features // rank
        for i in range(rank // features):
            ref[features:, i * features : (i + 1) * features] = rot[i * count : (i + 1) * count]


def stats_kernel(lat_ref, ctx_ref, cond_ref, cond_ctx_ref, w_ref, g_ref, out_ref, rows_ref, *, sp, tp):
    chip = place()[1]
    features = lat_ref.shape[1]
    size = out_ref.shape[2]
    rows_ref[: lat_ref.shape[0]] = lat_ref[...]
    rows_ref[lat_ref.shape[0] :] = ctx_ref[...]
    ones = jnp.ones((8, features), jnp.float32)
    sums = []
    for ref in (lat_ref, ctx_ref):
        values = ref[...].astype(jnp.float32)
        sums.append(dot_t(ones, values * values, precision=lax.Precision.HIGHEST)[:1])
    sums.append(jnp.zeros((1, size - lat_ref.shape[0] - ctx_ref.shape[0]), jnp.float32))
    sums = jnp.concatenate(sums, axis=1)
    lat_c = jax.nn.silu(cond_ref[...].astype(jnp.float32))
    ctx_c = jax.nn.silu(cond_ctx_ref[...].astype(jnp.float32))
    row = lax.broadcasted_iota(jnp.int32, (16, lat_c.shape[1]), 0)
    signal = jnp.where(row < 8, lat_c, ctx_c).astype(jnp.bfloat16)
    parts = [jnp.dot(signal, w_ref[j], preferred_element_type=jnp.float32) for j in range(3)]
    gain = g_ref[...]
    gains = parts[1] * gain + gain * (1.0 / sp)
    modulation = jnp.concatenate(
        [
            parts[0][:1],
            gains[:1],
            parts[0][8:9],
            gains[8:9],
            parts[2][:1],
            jnp.zeros((1, size - 5 * features), jnp.float32),
        ][: 5 if size == 5 * features else 6],
        axis=1,
    )
    for d in range(sp * tp):
        out_ref[d] = jnp.where((d % tp) // 2 == chip, modulation, sums)


def project_kernel(
    own_ref, other_ref, stat_ref, w_own_ref, w_other_ref, out_ref, gate_ref, *, sp, tp, rows
):
    count, features = own_ref.shape
    ctx_rows = count - rows
    rank = w_own_ref.shape[1]
    half, width = rank // 2, ROPE // 2
    base, chip, side, me = place()
    apart = jnp.zeros((1, count), jnp.float32)
    for t in range(tp):
        term = stat_ref[base + t][:, :count]
        apart = apart + jnp.where(chip == t // 2, jnp.zeros_like(term), term)
    apart = jnp.transpose(jnp.broadcast_to(apart, (8, count)))[:, :1]
    mine, partner = stat_ref[me], stat_ref[me + 1 - 2 * side]
    for s in range(1, sp):
        mine = mine + stat_ref[s * tp + me]
        partner = partner + stat_ref[s * tp + me + 1 - 2 * side]
    gate_ref[...] = mine[:, 4 * features : 5 * features]

    def split(ref):
        packed = ref[features:]
        rot = [packed[:, i * features : (i + 1) * features] for i in range(rank // features)]
        return ref[:features, :half], ref[:features, half:], jnp.concatenate(rot, axis=0)

    w_own, w_other = split(w_own_ref), split(w_other_ref)

    def rows_of(part, apart, kind):
        own, other = own_ref[part].astype(jnp.float32), other_ref[part].astype(jnp.float32)
        total = jnp.sum(own * own + other * other, axis=1, keepdims=True) + apart
        inverse = lax.rsqrt(total / D + EPS)
        first = second = rot = None
        for values, vectors, weights in ((own, mine, w_own), (other, partner, w_other)):
            shift = vectors[:, 2 * kind * features : (2 * kind + 1) * features]
            gain = vectors[:, (2 * kind + 1) * features : (2 * kind + 2) * features]
            h = (values * inverse * gain + shift).astype(jnp.bfloat16)
            terms = [None if kind else jnp.dot(h, weights[0], preferred_element_type=jnp.float32)]
            terms.append(jnp.dot(h, weights[1], preferred_element_type=jnp.float32))
            terms.append(dot_t(h, weights[2]))
            if second is None:
                first, second, rot = terms
            else:
                first = None if kind else first + terms[0]
                second, rot = second + terms[1], rot + terms[2]
        return first, second, rot

    lat_q, lat_kv, lat_rot = rows_of(slice(0, rows), apart[:rows], 0)
    unused, ctx_kv, ctx_rot = rows_of(slice(rows, count), apart[rows:], 1)
    lat, ctx = rows // tp, ctx_rows // tp
    quarter = (lat + ctx) // 4
    for d in range(tp):
        at = 0
        for source, size in ((lat_q, lat), (lat_kv, lat), (ctx_kv, ctx)):
            for slab in range(half // 128):
                out_ref[d, at : at + size, :] = source[
                    d * size : (d + 1) * size, slab * 128 : (slab + 1) * 128
                ]
                at += size
        rot = jnp.concatenate(
            [lat_rot[d * lat : (d + 1) * lat], ctx_rot[d * ctx : (d + 1) * ctx]], axis=0
        )
        out_ref[d, at : at + quarter, :] = jnp.concatenate(
            [rot[i * quarter : (i + 1) * quarter] for i in range(4)], axis=1
        )


def norm_kernel(part_ref, gq_ref, gkv_ref, tab_ref, kv_ref, cq_ref, *, lat, ctx):
    chips = part_ref.shape[0] // 2
    halves = []
    for core in range(2):
        acc = part_ref[core]
        for chip in range(1, chips):
            acc = acc + part_ref[2 * chip + core]
        halves.append(acc)
    rank = gq_ref.shape[1]
    slabs = rank // 256

    def columns(start, count):
        return jnp.concatenate(
            [
                half[start + i * count : start + (i + 1) * count]
                for half in halves
                for i in range(slabs)
            ],
            axis=1,
        )

    def normed(values, gain):
        factor = lax.rsqrt(jnp.mean(values * values, axis=1, keepdims=True) + EPS)
        return (values * factor * gain).astype(jnp.bfloat16)

    cq = normed(columns(0, lat), gq_ref[...])
    lat_kv = normed(columns(slabs * lat, lat), gkv_ref[...])
    at = 2 * slabs * lat
    ctx_kv = normed(columns(at, ctx), gkv_ref[...])
    at += slabs * ctx
    quarter = (lat + ctx) // 4
    width = ROPE // 2
    lat_rot, ctx_rot = [], []
    for core in range(2):
        packed = halves[core][at : at + quarter]
        rot = jnp.concatenate(
            [packed[:, i * width : (i + 1) * width] for i in range(4)], axis=0
        )
        turned = rot[:lat]
        swapped = jnp.concatenate([turned[:, width // 2 :], turned[:, : width // 2]], axis=1)
        lat_rot.append(turned * tab_ref[0, core] + swapped * tab_ref[1, core])
        ctx_rot.append(rot[lat:])
    zeros = jnp.zeros((lat + ctx, 128 - ROPE), jnp.float32)
    keys = jnp.concatenate(
        [jnp.concatenate(lat_rot, axis=1), jnp.concatenate(ctx_rot, axis=1)], axis=0
    )
    keys = jnp.concatenate([keys, zeros], axis=1).astype(jnp.bfloat16)
    compressed = jnp.concatenate([lat_kv, ctx_kv], axis=0)
    for copy in range(kv_ref.shape[0]):
        kv_ref[copy, :, :rank] = compressed
        kv_ref[copy, :, rank:] = keys
    cq_ref[...] = cq


def query_kernel(own_ref, other_ref, tab_ref, w_ref, out_ref, cq_ref):
    chips, count = own_ref.shape[:2]
    unused, here, side, unused = place()
    first = side == 0
    for chip in range(chips):
        own, other = own_ref[chip ^ here], other_ref[chip ^ here]
        at = 2 * chip * count
        cq_ref[at : at + count] = jnp.where(first, own, other)
        cq_ref[at + count : at + 2 * count] = jnp.where(first, other, own)
    quarter = ROPE // 4
    for head in range(w_ref.shape[0]):
        pieces = [w_ref[head]]
        for block in (1, 0, 3, 2):
            pieces.append(w_ref[head, NOPE + block * quarter : NOPE + (block + 1) * quarter])
        raw = dot_t(cq_ref[...], jnp.concatenate(pieces, axis=0))
        turned = raw[:, NOPE:] * tab_ref[...]
        turned = turned + pltpu.roll(turned, ROPE, 1)
        out_ref[head] = jnp.concatenate([raw[:, :NOPE], turned], axis=1).astype(jnp.bfloat16)


def expand_kernel(kv_ref, w_ref, out_ref):
    rank = w_ref.shape[0]
    values = kv_ref[...].reshape(out_ref.shape[1], kv_ref.shape[2])[:, :rank]
    for head in range(out_ref.shape[0]):
        weight = w_ref[:, head * (NOPE + DV) : (head + 1) * (NOPE + DV)]
        out_ref[head] = jnp.dot(values, weight, preferred_element_type=jnp.float32).astype(
            jnp.bfloat16
        )


def attend_kernel(
    lift_ref, query_ref, pairs_ref, own_ref, other_ref, w_ref, out_ref, key_ref, value_ref, *, lat
):
    rank = w_ref.shape[0]
    heads, count = pairs_ref.shape[:2]
    for at, ref in ((0, own_ref), (count, other_ref)):
        key_ref[at : at + count, NOPE:] = ref[:, :, rank:].reshape(count, 128)
    position = lax.broadcasted_iota(jnp.int32, (1, 2 * count), 1)
    context = lax.rem(position, lat[0] + lat[1]) >= lat[0]

    @pl.loop(0, heads)
    def _(head):
        other = other_ref[...].reshape(count, other_ref.shape[2])[:, :rank]
        width = NOPE + DV
        weight = w_ref[:, pl.ds(pl.multiple_of(head * width, width), width)]
        pairs = jnp.dot(other, weight, preferred_element_type=jnp.float32).astype(jnp.bfloat16)
        key_ref[:count, :NOPE] = pairs_ref[head, :, :NOPE]
        key_ref[count:, :NOPE] = pairs[:, :NOPE]
        value_ref[:count] = pairs_ref[head, :, NOPE:]
        value_ref[count:] = pairs[:, NOPE:]
        score = dot_t(query_ref[head], key_ref[...])
        lift = lift_ref[pl.ds(head, 1), :1]
        score = score * (NOPE + ROPE) ** -0.5 + jnp.where(context, lift, 0.0)
        peak = jnp.max(score, axis=1, keepdims=True)
        probs = jnp.exp(score - peak)
        total = jnp.sum(probs, axis=1, keepdims=True)
        summed = jnp.dot(
            probs.astype(jnp.bfloat16), value_ref[...], preferred_element_type=jnp.float32
        )
        out_ref[:, pl.ds(pl.multiple_of(head * DV, DV), DV)] = (summed / total).astype(jnp.bfloat16)


def share_out_kernel(w_ref, out_ref):
    chips, unused, features = out_ref.shape
    side = place()[2]
    for chip in range(chips):
        start = pl.multiple_of((2 * chip + 1 - side) * features, features)
        out_ref[chip] = w_ref[:, pl.ds(start, features)]


def output_own_kernel(heads_ref, w_ref, out_ref):
    chips, unused, features = out_ref.shape
    side = place()[2]
    for chip in range(chips):
        start = pl.multiple_of((2 * chip + side) * features, features)
        out_ref[chip] = jnp.dot(
            heads_ref[...], w_ref[:, pl.ds(start, features)], preferred_element_type=jnp.float32
        )


def output_kernel(heads_ref, w_ref, acc_ref, out_ref):
    for chip in range(out_ref.shape[0]):
        acc = acc_ref[chip] + jnp.dot(
            heads_ref[...], w_ref[chip], preferred_element_type=jnp.float32
        )
        out_ref[chip] = acc.astype(jnp.bfloat16)


def mix_kernel(latent_ref, gate_ref, branch_ref, out_ref):
    branch = branch_ref[0].astype(jnp.float32)
    for chip in range(1, branch_ref.shape[0]):
        branch = branch + branch_ref[chip].astype(jnp.float32)
    out_ref[...] = (latent_ref[...].astype(jnp.float32) + gate_ref[...] * branch).astype(
        jnp.bfloat16
    )


def split_device(
    latent,
    context,
    cond,
    cond_ctx,
    w_mod,
    g_norm,
    w_dq,
    w_dkv,
    w_kr,
    g_cq,
    g_ckv,
    w_uq,
    w_ukv,
    ctx_lift,
    w_out,
):
    f32, bf16 = jnp.float32, jnp.bfloat16
    sp, tp = lax.axis_size("sp"), lax.axis_size("tp")
    chips = tp // 2
    rows, features = latent.shape
    ctx_rows = context.shape[0]
    heads = w_uq.shape[1]
    rank = w_dq.shape[1]
    lat, ctx = rows // tp, ctx_rows // tp
    half = rank // 2
    sides = [list(range(k, tp, 2)) for k in range(2)]
    across = [(i, i ^ 1) for i in range(tp)]
    me = lax.axis_index("tp")

    def array(shape, dtype=bf16):
        return jax.ShapeDtypeStruct(shape, dtype)

    size = max(5 * features, rows + ctx_rows)
    stat, tokens = call(
        functools.partial(stats_kernel, sp=sp, tp=tp),
        (array((sp * tp, 1, size), f32), array((rows + ctx_rows, features))),
        latent,
        context,
        cond[None],
        cond_ctx[None],
        jnp.transpose(w_mod, (1, 0, 2)),
        g_norm[None],
        name="stats",
        held=False,
    )
    stat = lax.all_to_all(stat, ("sp", "tp"), 0, 0)

    share = array((features + ROPE // 2 * features // rank, rank))
    w_own, w_other = call(share_kernel, (share, share), w_dq, w_dkv, w_kr.T, name="share", held=False)
    tokens_other = lax.ppermute(tokens, "tp", across)
    w_other = lax.ppermute(w_other, "tp", across)
    w_up = w_out.reshape(heads * DV, 2 * chips * features)
    w_up_share = call(
        share_out_kernel, array((chips, heads * DV, features)), w_up, flops=1e9, name="share_out"
    )
    stat, w_up_share = lax.optimization_barrier((stat, w_up_share))
    w_up_other = lax.ppermute(w_up_share, "tp", across)

    height = half // 128 * (2 * lat + ctx) + (lat + ctx) // 4
    part, gate = call(
        functools.partial(project_kernel, sp=sp, tp=tp, rows=rows),
        (array((tp, height, 128), f32), array((1, features), f32)),
        tokens,
        tokens_other,
        stat,
        w_own,
        w_other,
        flops=4 * (rows + ctx_rows) * features * (rank + 128),
        limit=16,
        name="project",
    )
    part, w_kv, zero = lax.optimization_barrier((part, w_ukv, jnp.int32(0)))
    part = lax.all_to_all(part, "tp", 0, 0)

    positions = zero + lax.axis_index("sp") * rows + jnp.arange(rows, dtype=jnp.int32)
    cosine, sine = tables(positions)
    quarter = ROPE // 4
    c0, c1, s0, s1 = cosine[:, :quarter], cosine[:, quarter:], sine[:, :quarter], sine[:, quarter:]
    q_tab = jnp.concatenate([c0, c0, c1, c1, -s0, s0, -s1, s1], axis=1)
    k_tab = lax.dynamic_slice_in_dim(q_tab, me * lat, lat, 0)
    k_tab = k_tab.reshape(lat, 2, 2, ROPE // 2).transpose(1, 2, 0, 3)
    w_kv = w_kv.reshape(rank, heads * (NOPE + DV))
    part, q_tab, w_up_other, w_kv = lax.optimization_barrier((part, q_tab, w_up_other, w_kv))

    kv, cq = call(
        functools.partial(norm_kernel, lat=lat, ctx=ctx),
        (array((sp, lat + ctx, rank + 128)), array((lat, rank))),
        part,
        g_cq[None],
        g_ckv[None],
        k_tab,
        name="norm",
    )

    kv = lax.all_to_all(kv, "sp", 0, 0).reshape(1, sp * (lat + ctx), rank + 128)
    near = [cq]
    for hop in range(1, chips):
        swap = [(i, i ^ (2 * hop)) for i in range(tp)]
        near.append(lax.ppermute(cq, "tp", swap))
    cq_own, kv = lax.optimization_barrier((jnp.stack(near), kv))
    cq_other = lax.ppermute(cq_own, "tp", across)
    kv = jnp.broadcast_to(kv, (chips,) + kv.shape[1:])
    kv_own = lax.all_to_all(kv, "tp", 0, 0, axis_index_groups=sides)
    kv_other = lax.ppermute(kv_own, "tp", across)

    keys = sp * (rows + ctx_rows)
    query = call(
        query_kernel,
        array((heads, rows, 2 * NOPE)),
        cq_own,
        cq_other,
        q_tab,
        jnp.transpose(w_uq, (1, 2, 0)),
        scratch=[pltpu.VMEM((rows, rank), bf16)],
        flops=2 * rows * rank * 256 * heads,
        name="query",
    )
    pairs = call(
        expand_kernel,
        array((heads, keys // 2, NOPE + DV)),
        kv_own,
        w_kv,
        flops=keys * rank * 256 * heads,
        name="expand",
    )
    heads_out = call(
        functools.partial(attend_kernel, lat=(lat, ctx)),
        array((rows, heads * DV)),
        jnp.broadcast_to(ctx_lift[:, None], (heads, 128)),
        query,
        pairs,
        kv_own,
        kv_other,
        w_kv,
        scratch=[pltpu.VMEM((keys, 2 * NOPE), bf16), pltpu.VMEM((keys, DV), bf16)],
        flops=heads * keys * (2 * rows * 384 + rank * 256),
        limit=24,
        name="attend",
    )

    heads_other = lax.ppermute(heads_out, "tp", across)
    flops = 2 * rows * heads * DV * chips * features
    branch = call(
        output_own_kernel,
        array((chips, rows, features), f32),
        heads_out,
        w_up,
        flops=flops,
        name="output_own",
    )
    branch = call(
        output_kernel,
        array((chips, rows, features)),
        heads_other,
        w_up_other,
        branch,
        flops=flops,
        name="output",
    )
    branch = lax.all_to_all(branch, "tp", 0, 0, axis_index_groups=sides)
    return call(mix_kernel, array(latent.shape), latent, gate, branch, name="mix", kept=False)


def per_device(*arrays):
    rows, ctx_rows, features = arrays[0].shape[0], arrays[1].shape[0], arrays[0].shape[1]
    tp = lax.axis_size("tp")
    aligned = rows % (16 * tp) == 0 and ctx_rows % (16 * tp) == 0 and features % 128 == 0 and arrays[6].shape[1] % features == 0
    return (split_device if tp in (2, 4, 8, 16) and aligned else plain_device)(*arrays)


def solution(mesh):
    return jax.shard_map(
        per_device,
        mesh=mesh,
        in_specs=(
            P("sp", "tp"),
            P("sp", "tp"),
            P("sp"),
            P("sp"),
            P("sp", None, "tp"),
            P("tp"),
            P("tp", None),
            P("tp", None),
            P("tp", None),
            P(),
            P(),
            P(None, "tp", None),
            P(None, "tp", None),
            P("tp"),
            P("tp", None, None),
        ),
        out_specs=P("sp", "tp"),
        check_vma=False,
    )
```

```python
import functools

import jax
import jax.numpy as jnp
from jax import lax
from jax.experimental import pallas as pl
from jax.experimental.pallas import tpu as pltpu
from jax.sharding import PartitionSpec as P

D = 2048
NOPE = 128
ROPE = 64
DV = 128
GRID_W = 64


EPS = 1e-06
THETA = 10000.0
LOG2E = 1.4426950408889634


def tables(positions):
    row = (positions // GRID_W).astype(jnp.float32)
    col = (positions % GRID_W).astype(jnp.float32)
    half = ROPE // 2
    inverse = 1.0 / THETA ** (jnp.arange(0, half, 2, dtype=jnp.float32) / half)
    angle = jnp.concatenate([row[:, None] * inverse, col[:, None] * inverse], axis=-1)
    return (jnp.cos(angle), jnp.sin(angle))


def rotate(values, cosine, sine):
    shape = values.shape
    quarter = ROPE // 4
    parts = values.reshape(shape[:-1] + (2, 2, quarter))
    extra = (1,) * (len(shape) - 2)
    cosine = cosine.reshape((shape[0],) + extra + (2, quarter))
    sine = sine.reshape((shape[0],) + extra + (2, quarter))
    front_section = parts[..., 0, :]
    second = parts[..., 1, :]
    turned = jnp.stack(
        [front_section * cosine - second * sine, front_section * sine + second * cosine], axis=-2
    )
    return turned.reshape(shape)


def modulated(values, sumsq, gain, modulation):
    scaled = values * lax.rsqrt(sumsq / D + EPS)[:, None] * gain
    return (scaled * (1.0 + modulation[1]) + modulation[0]).astype(jnp.bfloat16)


def low_norm(values, gain):
    scale = lax.rsqrt(jnp.mean(values * values, axis=-1, keepdims=True) + EPS)
    return (values * scale * gain).astype(jnp.bfloat16)


def plain_device(
    latent,
    context,
    cond,
    cond_ctx,
    w_mod,
    g_norm,
    w_dq,
    w_dkv,
    w_kr,
    g_cq,
    g_ckv,
    w_uq,
    w_ukv,
    ctx_lift,
    w_out,
):
    rows = latent.shape[0]
    device_attention_groups = w_uq.shape[1]
    signal = jnp.stack(
        [jax.nn.silu(cond.astype(jnp.float32)), jax.nn.silu(cond_ctx.astype(jnp.float32))]
    ).astype(jnp.bfloat16)
    partial_mod = jnp.dot(
        signal, w_mod.reshape(w_mod.shape[0], -1), preferred_element_type=jnp.float32
    )
    modulation = lax.psum(partial_mod.reshape(2, 3, -1), "sp")
    lat_f = latent.astype(jnp.float32)
    ctx_f = context.astype(jnp.float32)
    lat_sq, ctx_sq = lax.psum(
        (jnp.sum(lat_f * lat_f, axis=1), jnp.sum(ctx_f * ctx_f, axis=1)), "tp"
    )
    lat_h = modulated(lat_f, lat_sq, g_norm, modulation[0])
    ctx_h = modulated(ctx_f, ctx_sq, g_norm, modulation[1])
    positions = lax.axis_index("sp") * rows + jnp.arange(rows, dtype=jnp.int32)
    cosine, sine = tables(positions)
    lat_q, lat_kv, lat_rot, ctx_kv, ctx_rot = lax.psum(
        (
            jnp.dot(lat_h, w_dq, preferred_element_type=jnp.float32),
            jnp.dot(lat_h, w_dkv, preferred_element_type=jnp.float32),
            jnp.dot(lat_h, w_kr, preferred_element_type=jnp.float32),
            jnp.dot(ctx_h, w_dkv, preferred_element_type=jnp.float32),
            jnp.dot(ctx_h, w_kr, preferred_element_type=jnp.float32),
        ),
        "tp",
    )
    cq_n = low_norm(lat_q, g_cq)
    ckv_n = low_norm(lat_kv, g_ckv)
    lat_kr = rotate(lat_rot, cosine, sine).astype(jnp.bfloat16)
    ctx_ckv_n = low_norm(ctx_kv, g_ckv)
    ctx_kr = ctx_rot.astype(jnp.bfloat16)
    query = jnp.dot(cq_n, w_uq.reshape(w_uq.shape[0], -1), preferred_element_type=jnp.float32)
    query = query.reshape(rows, device_attention_groups, NOPE + ROPE)
    query = jnp.concatenate(
        [query[..., :NOPE], rotate(query[..., NOPE:], cosine, sine)], axis=-1
    ).astype(jnp.bfloat16)
    up_weight = w_ukv.reshape(w_ukv.shape[0], -1)
    scale = (NOPE + ROPE) ** (-0.5)

    def expand(compressed):
        return jnp.dot(compressed, up_weight, preferred_element_type=jnp.float32).astype(
            jnp.bfloat16
        )

    def unpack(front_section):
        return expand(front_section).reshape(
            front_section.shape[0], device_attention_groups, NOPE + DV
        )

    def merged_question_vector(
        cumulative_loop_values, front_section, spinning_section, affinity_offset
    ):
        peak, total, accum = cumulative_loop_values
        pairs = unpack(front_section)
        count = pairs.shape[0]
        keys = jnp.concatenate(
            [
                pairs[..., :NOPE],
                jnp.broadcast_to(
                    spinning_section[:, None, :], (count, device_attention_groups, ROPE)
                ),
            ],
            axis=-1,
        )
        raw_affinity_matrix = (
            jnp.einsum("qhd,khd->hqk", query, keys, preferred_element_type=jnp.float32) * scale
        )
        raw_affinity_matrix = raw_affinity_matrix + affinity_offset[:, None, None]
        fresh = jnp.maximum(peak, jnp.max(raw_affinity_matrix, axis=-1))
        probs = jnp.exp(raw_affinity_matrix - fresh[..., None])
        fade = jnp.exp(peak - fresh)
        total = total * fade + jnp.sum(probs, axis=-1)
        accum = accum * fade[..., None] + jnp.einsum(
            "hqk,khd->hqd",
            probs.astype(jnp.bfloat16),
            pairs[..., NOPE:],
            preferred_element_type=jnp.float32,
        )
        return (fresh, total, accum)

    blank_offset_matrix = jnp.zeros((device_attention_groups,), jnp.float32)
    start_carry = (
        jnp.full((device_attention_groups, rows), -1e30, jnp.float32),
        jnp.zeros((device_attention_groups, rows), jnp.float32),
        jnp.zeros((device_attention_groups, rows, DV), jnp.float32),
    )
    ctx_all_first, ctx_all_kr = (
        lax.all_gather(ctx_ckv_n, "sp", axis=0, tiled=True),
        lax.all_gather(ctx_kr, "sp", axis=0, tiled=True),
    )
    cumulative_loop_values = merged_question_vector(
        start_carry, ctx_all_first, ctx_all_kr, ctx_lift
    )
    fold_cumulative_loop_values = cumulative_loop_values
    front_section = lax.all_gather(ckv_n, "sp", axis=0, tiled=True)
    spinning_section = lax.all_gather(lat_kr, "sp", axis=0, tiled=True)
    count = front_section.shape[0] // rows
    blocks = (
        front_section.reshape(count, rows, front_section.shape[1]),
        spinning_section.reshape(count, rows, spinning_section.shape[1]),
    )

    def step(normalizer_statistics, segment_window):
        return (
            merged_question_vector(
                normalizer_statistics, segment_window[0], segment_window[1], blank_offset_matrix
            ),
            None,
        )

    fold_cumulative_loop_values, _ = lax.scan(step, fold_cumulative_loop_values, blocks)
    cumulative_loop_values = fold_cumulative_loop_values
    _, total, accum = cumulative_loop_values
    heads_out = (accum / total[..., None]).astype(jnp.bfloat16)
    branch = jnp.einsum("hqd,hde->qe", heads_out, w_out, preferred_element_type=jnp.float32)
    branch = lax.psum_scatter(
        branch.astype(jnp.bfloat16), "tp", scatter_dimension=1, tiled=True
    ).astype(jnp.float32)
    return (lat_f + modulation[0, 2] * branch).astype(jnp.bfloat16)


def call(kernel, outs, *args, flops=1e6, scratch=(), limit=8, held=pltpu.VMEM, kept=True):
    single = not isinstance(outs, tuple)
    vmem = pl.BlockSpec(memory_space=pltpu.VMEM)
    outs = (outs,) if single else outs
    if kept:
        outs = tuple(pltpu.VMEM(o.shape, o.dtype) for o in outs)
    if held is not None:
        args = tuple(pltpu.with_memory_space_constraint(a, held) for a in args)
    result = pl.pallas_call(
        kernel,
        in_specs=[vmem] * len(args),
        out_specs=(vmem,) * len(outs),
        out_shape=outs,
        scratch_shapes=scratch,
        cost_estimate=pl.CostEstimate(
            flops=int(flops), bytes_accessed=int(1e5), transcendentals=0
        ),
        compiler_params=pltpu.CompilerParams(vmem_limit_bytes=limit << 20),
    )(*args)
    return result[0] if single else result


def place():
    me = lax.axis_index("tp")
    return lax.axis_index("sp") * lax.axis_size("tp"), me // 2, lax.rem(me, 2), me


def dot_t(left, right, **options):
    return lax.dot_general(
        left, right, (((1,), (1,)), ((), ())), preferred_element_type=jnp.float32, **options
    )


def share_kernel(wq_ref, wkv_ref, wr_ref, own_ref, other_ref):
    features, rank = wq_ref.shape
    half, width = rank // 2, ROPE // 2
    side = place()[2]
    for which, ref in ((side, own_ref), (1 - side, other_ref)):
        start = pl.multiple_of(which * half, half)
        ref[:features, :half] = wq_ref[:, pl.ds(start, half)]
        ref[:features, half:] = wkv_ref[:, pl.ds(start, half)]
        low = pl.multiple_of(which * width, width)
        rot = wr_ref[pl.ds(low, width), :]
        count = width * features // rank
        for i in range(rank // features):
            ref[features:, i * features : (i + 1) * features] = rot[i * count : (i + 1) * count]


def stats_kernel(lat_ref, ctx_ref, cond_ref, cond_ctx_ref, w_ref, g_ref, out_ref, rows_ref, *, sp):
    rows_ref[: lat_ref.shape[0]] = lat_ref[...]
    rows_ref[lat_ref.shape[0] :] = ctx_ref[...]
    inner = cond_ref.shape[0]
    lat_c = jax.nn.silu(cond_ref[...].astype(jnp.float32).reshape(1, inner))
    ctx_c = jax.nn.silu(cond_ctx_ref[...].astype(jnp.float32).reshape(1, inner))
    row = lax.broadcasted_iota(jnp.int32, (16, inner), 0)
    signal = jnp.where(row < 8, lat_c, ctx_c).astype(jnp.bfloat16)
    parts = [jnp.dot(signal, w_ref[j], preferred_element_type=jnp.float32) for j in range(3)]
    gain = g_ref[...].reshape(1, g_ref.shape[0])
    gains = parts[1] * gain + gain * (1.0 / sp)
    modulation = jnp.concatenate(
        [parts[0][:1], gains[:1], parts[0][8:9], gains[8:9], parts[2][:1]], axis=1
    )
    for d in range(out_ref.shape[0]):
        out_ref[d] = modulation


def square_kernel(own_ref, other_ref, out_ref):
    ones = jnp.ones((8, own_ref.shape[1]), jnp.float32)
    total = None
    for ref in (own_ref, other_ref):
        values = ref[...].astype(jnp.float32)
        term = dot_t(ones, values * values, precision=lax.Precision.HIGHEST)
        total = term if total is None else total + term
    out_ref[...] = total


def project_kernel(
    own_ref, other_ref, mod_ref, w_own_ref, w_other_ref, sq_ref, *refs, sp, tp, rows
):
    out_ref, gate_ref = refs[-2:]
    count, features = own_ref.shape
    ctx_rows = count - rows
    rank = w_own_ref.shape[1]
    half = rank // 2
    side = place()[2]
    total = sq_ref[...]
    for ref in refs[:-2]:
        total = total + ref[...]
    total = jnp.transpose(total)[:, :1]
    mine, partner = mod_ref[side], mod_ref[1 - side]
    for s in range(1, sp):
        mine = mine + mod_ref[2 * s + side]
        partner = partner + mod_ref[2 * s + 1 - side]
    gate_ref[...] = mine[:, 4 * features :]

    def split(ref):
        packed = ref[features:]
        rot = [packed[:, i * features : (i + 1) * features] for i in range(rank // features)]
        return ref[:features, :half], ref[:features, half:], jnp.concatenate(rot, axis=0)

    w_own, w_other = split(w_own_ref), split(w_other_ref)

    def rows_of(part, kind):
        own, other = own_ref[part].astype(jnp.float32), other_ref[part].astype(jnp.float32)
        inverse = lax.rsqrt(total[part] / D + EPS)
        first = second = rot = None
        for values, vectors, weights in ((own, mine, w_own), (other, partner, w_other)):
            shift = vectors[:, 2 * kind * features : (2 * kind + 1) * features]
            gain = vectors[:, (2 * kind + 1) * features : (2 * kind + 2) * features]
            h = (values * inverse * gain + shift).astype(jnp.bfloat16)
            terms = [None if kind else jnp.dot(h, weights[0], preferred_element_type=jnp.float32)]
            terms.append(jnp.dot(h, weights[1], preferred_element_type=jnp.float32))
            terms.append(dot_t(h, weights[2]))
            if second is None:
                first, second, rot = terms
            else:
                first = None if kind else first + terms[0]
                second, rot = second + terms[1], rot + terms[2]
        return first, second, rot

    lat_q, lat_kv, lat_rot = rows_of(slice(0, rows), 0)
    _, ctx_kv, ctx_rot = rows_of(slice(rows, count), 1)
    lat, ctx = rows // tp, ctx_rows // tp
    quarter = (lat + ctx) // 4
    for d in range(tp):
        at = 0
        for source, size in ((lat_q, lat), (lat_kv, lat), (ctx_kv, ctx)):
            for slab in range(half // 128):
                out_ref[d, at : at + size, :] = source[
                    d * size : (d + 1) * size, slab * 128 : (slab + 1) * 128
                ]
                at += size
        rot = jnp.concatenate(
            [lat_rot[d * lat : (d + 1) * lat], ctx_rot[d * ctx : (d + 1) * ctx]], axis=0
        )
        out_ref[d, at : at + quarter, :] = jnp.concatenate(
            [rot[i * quarter : (i + 1) * quarter] for i in range(4)], axis=1
        )


def norm_kernel(part_ref, gq_ref, gkv_ref, tab_ref, kv_ref, near_ref, *, lat, ctx):
    chips = part_ref.shape[0] // 2
    halves = []
    for core in range(2):
        acc = part_ref[core]
        for chip in range(1, chips):
            acc = acc + part_ref[2 * chip + core]
        halves.append(acc)
    rank = gq_ref.shape[1]
    slabs = rank // 256

    def columns(start, count):
        return jnp.concatenate(
            [
                half[start + i * count : start + (i + 1) * count]
                for half in halves
                for i in range(slabs)
            ],
            axis=1,
        )

    def normed(values, gain):
        factor = lax.rsqrt(jnp.mean(values * values, axis=1, keepdims=True) + EPS)
        return (values * factor * gain).astype(jnp.bfloat16)

    cq = normed(columns(0, lat), gq_ref[...])
    lat_kv = normed(columns(slabs * lat, lat), gkv_ref[...])
    at = 2 * slabs * lat
    ctx_kv = normed(columns(at, ctx), gkv_ref[...])
    at += slabs * ctx
    quarter = (lat + ctx) // 4
    width = ROPE // 2
    lat_rot, ctx_rot = [], []
    for core in range(2):
        packed = halves[core][at : at + quarter]
        rot = jnp.concatenate(
            [packed[:, i * width : (i + 1) * width] for i in range(4)], axis=0
        )
        turned = rot[:lat]
        swapped = jnp.concatenate([turned[:, width // 2 :], turned[:, : width // 2]], axis=1)
        lat_rot.append(turned * tab_ref[0, core] + swapped * tab_ref[1, core])
        ctx_rot.append(rot[lat:])
    keys = jnp.concatenate(
        [jnp.concatenate(lat_rot, axis=1), jnp.concatenate(ctx_rot, axis=1)], axis=0
    )
    pieces = rank // ROPE
    low = (lat + ctx) // pieces
    keys = jnp.concatenate(
        [keys[i * low : (i + 1) * low] for i in range(pieces)], axis=1
    ).astype(jnp.bfloat16)
    compressed = jnp.concatenate([lat_kv, ctx_kv], axis=0)
    for ref in [kv_ref.at[copy] for copy in range(kv_ref.shape[0])] + [near_ref]:
        ref[: lat + ctx] = compressed
        ref[lat + ctx : lat + ctx + low] = keys
    near_ref[lat + ctx + low :] = cq


def gather_kernel(kv_ref, out_ref):
    planes, size = kv_ref.shape[:2]
    here = lax.axis_index("sp")
    for i in range(planes - 1):
        out_ref[i * size : (i + 1) * size] = kv_ref[lax.rem(here + 1 + i, planes)]


def unpack(chunks, kv_ref, key_ref, lat, ctx):
    count = lat + ctx
    rank = kv_ref.shape[1]
    row = lax.broadcasted_iota(jnp.int32, (count, 128 - ROPE), 0)
    lane = lax.broadcasted_iota(jnp.int32, (count, 128 - ROPE), 1)
    flags = jnp.where((row >= lat) & (lane < 3), 1.0, 0.0)
    for i, (ref, at) in enumerate(chunks):
        kv_ref[i * count : (i + 1) * count] = ref[at : at + count]
        low = count * ROPE // rank
        packed = ref[at + count : at + count + low].astype(jnp.float32)
        rot = [packed[:, j * ROPE : (j + 1) * ROPE] for j in range(rank // ROPE)]
        rot = jnp.concatenate([jnp.concatenate(rot, axis=0), flags], axis=1)
        key_ref[i * count : (i + 1) * count] = rot.astype(jnp.bfloat16)


def expanded(kv_ref, w_ref, head):
    weight = w_ref[:, head * (NOPE + DV) : (head + 1) * (NOPE + DV)]
    return jnp.dot(kv_ref[...], weight, preferred_element_type=jnp.float32).astype(jnp.bfloat16)


def weighted(query, keys, values):
    score = dot_t(query, keys)
    peak = jnp.max(score, axis=1, keepdims=True)
    probs = jnp.exp2((score - peak) * ((NOPE + ROPE) ** -0.5 * LOG2E))
    total = jnp.sum(probs, axis=1, keepdims=True)
    summed = jnp.dot(probs.astype(jnp.bfloat16), values, preferred_element_type=jnp.float32)
    return peak, total, summed


def near_kernel(tab_ref, lift_ref, wq_ref, wkv_ref, *refs, lat, ctx, chips):
    own_refs, other_refs = refs[:chips], refs[chips : 2 * chips]
    query_ref, stat_ref, sum_ref, cq_ref, kv_ref, key_ref = refs[-6:]
    size = own_refs[0].shape[0]
    unused, here, side, unused = place()
    for hop in range(chips):
        own, other = own_refs[hop][size - lat :], other_refs[hop][size - lat :]
        at = pl.multiple_of(2 * (here ^ hop) * lat, 16)
        cq_ref[pl.ds(at, lat)] = jnp.where(side == 0, own, other)
        cq_ref[pl.ds(at + lat, lat)] = jnp.where(side == 0, other, own)
    chunks = [(ref, 0) for ref in own_refs + other_refs]
    chunks += chunks_of(refs[2 * chips : -6], size - lat)
    unpack(chunks, kv_ref, key_ref, lat, ctx)
    stats = jnp.zeros(stat_ref.shape, jnp.float32)
    spot = lax.broadcasted_iota(jnp.int32, stat_ref.shape, 1)
    heads = wq_ref.shape[0]
    quarter = ROPE // 4
    lane = lax.broadcasted_iota(jnp.int32, (1, 2 * ROPE), 1)
    for head in range(wq_ref.shape[0]):
        pieces = [wq_ref[head]]
        for block in (1, 0, 3, 2):
            pieces.append(wq_ref[head, NOPE + block * quarter : NOPE + (block + 1) * quarter])
        raw = dot_t(cq_ref[...], jnp.concatenate(pieces, axis=0))
        turned = raw[:, NOPE:] * tab_ref[...]
        turned = turned + pltpu.roll(turned, ROPE, 1)
        lift = lift_ref[head : head + 1] * (NOPE + ROPE) ** 0.5
        first = lift.astype(jnp.bfloat16).astype(jnp.float32)
        second = (lift - first).astype(jnp.bfloat16).astype(jnp.float32)
        third = lift - first - second
        lifts = jnp.where(lane == ROPE, first, jnp.where(lane == ROPE + 1, second, third))
        lifts = jnp.where(lane < ROPE + 3, lifts, 0.0)
        turned = jnp.where(lane < ROPE, turned, lifts)
        query = jnp.concatenate([raw[:, :NOPE], turned], axis=1).astype(jnp.bfloat16)
        query_ref[head] = query
        pairs = expanded(kv_ref, wkv_ref, head)
        keys = jnp.concatenate([pairs[:, :NOPE], key_ref[...]], axis=1)
        peak, total, summed = weighted(query, keys, pairs[:, NOPE:])
        stats = jnp.where(spot == head, peak, jnp.where(spot == heads + head, total, stats))
        sum_ref[head] = summed
    stat_ref[...] = stats


def chunks_of(refs, step):
    return [(ref, at) for ref in refs for at in range(0, refs[0].shape[0], step)]


def expand_kernel(w_ref, *refs, lat, ctx):
    key_ref, value_ref, kv_ref, rot_ref = refs[-4:]
    step = lat + ctx + (lat + ctx) * ROPE // w_ref.shape[0]
    unpack(chunks_of(refs[:-4], step), kv_ref, rot_ref, lat, ctx)
    for head in range(key_ref.shape[0]):
        pairs = expanded(kv_ref, w_ref, head)
        key_ref[head, :, :NOPE] = pairs[:, :NOPE]
        key_ref[head, :, NOPE:] = rot_ref[...]
        value_ref[head] = pairs[:, NOPE:]


def far_kernel(query_ref, stat_ref, sum_ref, key_ref, value_ref, w_ref, *refs, lat, ctx):
    out_ref, kv_ref, rot_ref = refs[-3:]
    step = lat + ctx + (lat + ctx) * ROPE // w_ref.shape[0]
    unpack(chunks_of(refs[:-3], step), kv_ref, rot_ref, lat, ctx)
    heads = query_ref.shape[0]
    factor = (NOPE + ROPE) ** -0.5 * LOG2E
    for head in range(query_ref.shape[0]):
        pairs = expanded(kv_ref, w_ref, head)
        keys = jnp.concatenate([pairs[:, :NOPE], rot_ref[...]], axis=1)
        keys = jnp.concatenate([key_ref[head], keys], axis=0)
        values = jnp.concatenate([value_ref[head], pairs[:, NOPE:]], axis=0)
        peak, total, summed = weighted(query_ref[head], keys, values)
        near = stat_ref[:, head : head + 1]
        top = jnp.maximum(peak, near)
        new, old = jnp.exp2((peak - top) * factor), jnp.exp2((near - top) * factor)
        total = total * new + stat_ref[:, heads + head : heads + head + 1] * old
        summed = summed * new + sum_ref[head] * old
        out_ref[:, head * DV : (head + 1) * DV] = (summed / total).astype(jnp.bfloat16)


def share_out_kernel(w_ref, out_ref):
    chips, unused, features = out_ref.shape
    unused, here, side, unused = place()
    for hop in range(chips):
        start = pl.multiple_of((2 * (here ^ hop) + 1 - side) * features, features)
        out_ref[hop] = w_ref[:, pl.ds(start, features)]


def output_own_kernel(heads_ref, w_ref, out_ref):
    chips, unused, features = out_ref.shape
    unused, here, side, unused = place()
    for hop in range(chips):
        start = pl.multiple_of((2 * (here ^ hop) + side) * features, features)
        out_ref[hop] = jnp.dot(
            heads_ref[...], w_ref[:, pl.ds(start, features)], preferred_element_type=jnp.float32
        )


def output_kernel(heads_ref, w_ref, acc_ref, *out_refs):
    for hop in reversed(range(len(out_refs))):
        acc = acc_ref[hop] + jnp.dot(
            heads_ref[...], w_ref[hop], preferred_element_type=jnp.float32
        )
        out_refs[hop][...] = acc.astype(out_refs[hop].dtype)


def mix_kernel(latent_ref, gate_ref, *refs):
    branch = refs[0][...]
    for ref in refs[1:-1]:
        branch = branch + ref[...].astype(jnp.float32)
    refs[-1][...] = (latent_ref[...].astype(jnp.float32) + gate_ref[...] * branch).astype(
        jnp.bfloat16
    )


def split_device(
    latent,
    context,
    cond,
    cond_ctx,
    w_mod,
    g_norm,
    w_dq,
    w_dkv,
    w_kr,
    g_cq,
    g_ckv,
    w_uq,
    w_ukv,
    ctx_lift,
    w_out,
):
    f32, bf16 = jnp.float32, jnp.bfloat16
    sp, tp = lax.axis_size("sp"), lax.axis_size("tp")
    chips = tp // 2
    rows, features = latent.shape
    ctx_rows = context.shape[0]
    heads = w_uq.shape[1]
    rank = w_dq.shape[1]
    lat, ctx = rows // tp, ctx_rows // tp
    half = rank // 2
    across = [(i, i ^ 1) for i in range(tp)]
    me = lax.axis_index("tp")

    def array(shape, dtype=bf16):
        return jax.ShapeDtypeStruct(shape, dtype)

    def hopped(value):
        return [value] + [
            lax.ppermute(value, "tp", [(i, i ^ (2 * hop)) for i in range(tp)])
            for hop in range(1, chips)
        ]

    modulation, tokens = call(
        functools.partial(stats_kernel, sp=sp),
        (array((2 * sp, 1, 5 * features), f32), array((rows + ctx_rows, features))),
        latent,
        context,
        cond,
        cond_ctx,
        jnp.transpose(w_mod, (1, 0, 2)),
        g_norm,
        held=pltpu.HBM,
    )
    tokens_other = lax.ppermute(tokens, "tp", across)
    columns = [[s * tp + 2 * c + k for s in range(sp) for k in range(2)] for c in range(chips)]
    modulation = lax.all_to_all(modulation, ("sp", "tp"), 0, 0, axis_index_groups=columns)
    squares = call(square_kernel, array((8, rows + ctx_rows), f32), tokens, tokens_other)
    squares = hopped(squares)

    share = array((features + ROPE // 2 * features // rank, rank))
    w_own, w_other = call(share_kernel, (share, share), w_dq, w_dkv, w_kr.T, held=pltpu.HBM)
    w_other = lax.ppermute(w_other, "tp", across)
    w_up = w_out.reshape(heads * DV, 2 * chips * features)
    w_up_share = call(share_out_kernel, array((chips, heads * DV, features)), w_up, flops=1e9)
    modulation, w_up_share = lax.optimization_barrier((modulation, w_up_share))
    w_up_other = lax.ppermute(w_up_share, "tp", across)

    height = half // 128 * (2 * lat + ctx) + (lat + ctx) // 4
    part, gate = call(
        functools.partial(project_kernel, sp=sp, tp=tp, rows=rows),
        (array((tp, height, 128), f32), array((1, features), f32)),
        tokens,
        tokens_other,
        modulation,
        w_own,
        w_other,
        *squares,
        flops=4 * (rows + ctx_rows) * features * (rank + 128),
        limit=16,
    )
    part, w_kv, zero = lax.optimization_barrier((part, w_ukv, jnp.int32(0)))
    part = lax.all_to_all(part, "tp", 0, 0)

    positions = zero + lax.axis_index("sp") * rows + jnp.arange(rows, dtype=jnp.int32)
    cosine, sine = tables(positions)
    quarter = ROPE // 4
    c0, c1, s0, s1 = cosine[:, :quarter], cosine[:, quarter:], sine[:, :quarter], sine[:, quarter:]
    q_tab = jnp.concatenate([c0, c0, c1, c1, -s0, s0, -s1, s1], axis=1)
    k_tab = lax.dynamic_slice_in_dim(q_tab, me * lat, lat, 0)
    k_tab = k_tab.reshape(lat, 2, 2, ROPE // 2).transpose(1, 2, 0, 3)
    w_kv = w_kv.reshape(rank, heads * (NOPE + DV))
    part, q_tab, w_up_other, w_kv = lax.optimization_barrier((part, q_tab, w_up_other, w_kv))

    count = lat + ctx
    step = count + count * ROPE // rank
    kv, near = call(
        functools.partial(norm_kernel, lat=lat, ctx=ctx),
        (array((sp, step, rank)), array((step + lat, rank))),
        part,
        g_cq[None],
        g_ckv[None],
        k_tab,
    )

    kv = lax.all_to_all(kv, "sp", 0, 0)
    near_own = hopped(near)
    *near_own, kv = lax.optimization_barrier((*near_own, kv))
    near_other = [lax.ppermute(n, "tp", across) for n in near_own]
    far = call(gather_kernel, array(((sp - 1) * step, rank)), kv)
    far_own = hopped(far)
    far_other = [lax.ppermute(f, "tp", across) for f in far_own]

    keys = (tp + 2 * (sp - 1)) * count
    query, stats, summed = call(
        functools.partial(near_kernel, lat=lat, ctx=ctx, chips=chips),
        (
            array((heads, rows, 2 * NOPE)),
            array((rows, 128), f32),
            array((heads, rows, DV), f32),
        ),
        q_tab,
        jnp.broadcast_to(ctx_lift[:, None], (heads, 128)),
        jnp.transpose(w_uq, (1, 2, 0)),
        w_kv,
        *near_own,
        *near_other,
        far_own[0],
        far_other[0],
        scratch=[
            pltpu.VMEM((rows, rank), bf16),
            pltpu.VMEM((keys, rank), bf16),
            pltpu.VMEM((keys, 128), bf16),
        ],
        flops=heads * rows * (2 * rank * 256 + 2 * keys * 384),
        limit=16,
    )
    keys = (chips - 1) * (sp - 1) * count
    scratch = [pltpu.VMEM((keys, rank), bf16), pltpu.VMEM((keys, 128), bf16)]
    far_keys, far_values = call(
        functools.partial(expand_kernel, lat=lat, ctx=ctx),
        (array((heads, keys, 2 * NOPE)), array((heads, keys, DV))),
        w_kv,
        *far_own[1:],
        scratch=scratch,
        flops=2 * keys * rank * 256 * heads,
    )
    heads_out = call(
        functools.partial(far_kernel, lat=lat, ctx=ctx),
        array((rows, heads * DV)),
        query,
        stats,
        summed,
        far_keys,
        far_values,
        w_kv,
        *far_other[1:],
        scratch=scratch,
        flops=2 * heads * keys * (2 * rows * 384 + rank * 256),
        limit=28,
    )

    heads_other = lax.ppermute(heads_out, "tp", across)
    flops = 2 * rows * heads * DV * chips * features
    branch = call(
        output_own_kernel, array((chips, rows, features), f32), heads_out, w_up, flops=flops
    )
    block = array((rows, features))
    branch, *apart = call(
        output_kernel,
        (array((rows, features), f32),) + (block,) * (chips - 1),
        heads_other,
        w_up_other,
        branch,
        flops=flops,
    )
    apart = [
        lax.ppermute(a, "tp", [(i, i ^ (2 * hop + 2)) for i in range(tp)])
        for hop, a in enumerate(apart)
    ]
    return call(mix_kernel, array(latent.shape), latent, gate, branch, *apart, kept=False)


def chosen(*arrays):
    rows, ctx_rows, features = arrays[0].shape[0], arrays[1].shape[0], arrays[0].shape[1]
    tp = lax.axis_size("tp")
    aligned = rows % (16 * tp) == 0 and ctx_rows % (16 * tp) == 0 and features % 128 == 0 and arrays[6].shape[1] % features == 0
    return (split_device if tp in (2, 4, 8, 16) and aligned else plain_device)(*arrays)


def solution(mesh):
    return jax.shard_map(
        chosen,
        mesh=mesh,
        in_specs=(
            P("sp", "tp"),
            P("sp", "tp"),
            P("sp"),
            P("sp"),
            P("sp", None, "tp"),
            P("tp"),
            P("tp", None),
            P("tp", None),
            P("tp", None),
            P(),
            P(),
            P(None, "tp", None),
            P(None, "tp", None),
            P("tp"),
            P("tp", None, None),
        ),
        out_specs=P("sp", "tp"),
        check_vma=False,
    )
```

```python
import functools

import jax
import jax.numpy as jnp
import numpy as np
from jax import lax
from jax.experimental import pallas as pl
from jax.experimental.pallas import tpu as pltpu
from jax.sharding import PartitionSpec as P

D = 2048
NOPE = 128
ROPE = 64
DV = 128
GRID_W = 64


EPS = 1e-06
THETA = 10000.0
LOG2E = 1.4426950408889634


def tables(positions):
    row = (positions // GRID_W).astype(jnp.float32)
    col = (positions % GRID_W).astype(jnp.float32)
    half = ROPE // 2
    inverse = 1.0 / THETA ** (jnp.arange(0, half, 2, dtype=jnp.float32) / half)
    angle = jnp.concatenate([row[:, None] * inverse, col[:, None] * inverse], axis=-1)
    return (jnp.cos(angle), jnp.sin(angle))


def rotate(values, cosine, sine):
    shape = values.shape
    quarter = ROPE // 4
    parts = values.reshape(shape[:-1] + (2, 2, quarter))
    extra = (1,) * (len(shape) - 2)
    cosine = cosine.reshape((shape[0],) + extra + (2, quarter))
    sine = sine.reshape((shape[0],) + extra + (2, quarter))
    front_section = parts[..., 0, :]
    second = parts[..., 1, :]
    turned = jnp.stack(
        [front_section * cosine - second * sine, front_section * sine + second * cosine], axis=-2
    )
    return turned.reshape(shape)


def modulated(values, sumsq, gain, modulation):
    scaled = values * lax.rsqrt(sumsq / D + EPS)[:, None] * gain
    return (scaled * (1.0 + modulation[1]) + modulation[0]).astype(jnp.bfloat16)


def low_norm(values, gain):
    scale = lax.rsqrt(jnp.mean(values * values, axis=-1, keepdims=True) + EPS)
    return (values * scale * gain).astype(jnp.bfloat16)


def plain_device(
    latent,
    context,
    cond,
    cond_ctx,
    w_mod,
    g_norm,
    w_dq,
    w_dkv,
    w_kr,
    g_cq,
    g_ckv,
    w_uq,
    w_ukv,
    ctx_lift,
    w_out,
):
    rows = latent.shape[0]
    device_attention_groups = w_uq.shape[1]
    signal = jnp.stack(
        [jax.nn.silu(cond.astype(jnp.float32)), jax.nn.silu(cond_ctx.astype(jnp.float32))]
    ).astype(jnp.bfloat16)
    partial_mod = jnp.dot(
        signal, w_mod.reshape(w_mod.shape[0], -1), preferred_element_type=jnp.float32
    )
    modulation = lax.psum(partial_mod.reshape(2, 3, -1), "sp")
    lat_f = latent.astype(jnp.float32)
    ctx_f = context.astype(jnp.float32)
    lat_sq, ctx_sq = lax.psum(
        (jnp.sum(lat_f * lat_f, axis=1), jnp.sum(ctx_f * ctx_f, axis=1)), "tp"
    )
    lat_h = modulated(lat_f, lat_sq, g_norm, modulation[0])
    ctx_h = modulated(ctx_f, ctx_sq, g_norm, modulation[1])
    positions = lax.axis_index("sp") * rows + jnp.arange(rows, dtype=jnp.int32)
    cosine, sine = tables(positions)
    lat_q, lat_kv, lat_rot, ctx_kv, ctx_rot = lax.psum(
        (
            jnp.dot(lat_h, w_dq, preferred_element_type=jnp.float32),
            jnp.dot(lat_h, w_dkv, preferred_element_type=jnp.float32),
            jnp.dot(lat_h, w_kr, preferred_element_type=jnp.float32),
            jnp.dot(ctx_h, w_dkv, preferred_element_type=jnp.float32),
            jnp.dot(ctx_h, w_kr, preferred_element_type=jnp.float32),
        ),
        "tp",
    )
    cq_n = low_norm(lat_q, g_cq)
    ckv_n = low_norm(lat_kv, g_ckv)
    lat_kr = rotate(lat_rot, cosine, sine).astype(jnp.bfloat16)
    ctx_ckv_n = low_norm(ctx_kv, g_ckv)
    ctx_kr = ctx_rot.astype(jnp.bfloat16)
    query = jnp.dot(cq_n, w_uq.reshape(w_uq.shape[0], -1), preferred_element_type=jnp.float32)
    query = query.reshape(rows, device_attention_groups, NOPE + ROPE)
    query = jnp.concatenate(
        [query[..., :NOPE], rotate(query[..., NOPE:], cosine, sine)], axis=-1
    ).astype(jnp.bfloat16)
    up_weight = w_ukv.reshape(w_ukv.shape[0], -1)
    scale = (NOPE + ROPE) ** (-0.5)

    def expand(compressed):
        return jnp.dot(compressed, up_weight, preferred_element_type=jnp.float32).astype(
            jnp.bfloat16
        )

    def unpack(front_section):
        return expand(front_section).reshape(
            front_section.shape[0], device_attention_groups, NOPE + DV
        )

    def merged_question_vector(
        cumulative_loop_values, front_section, spinning_section, affinity_offset
    ):
        peak, total, accum = cumulative_loop_values
        pairs = unpack(front_section)
        count = pairs.shape[0]
        keys = jnp.concatenate(
            [
                pairs[..., :NOPE],
                jnp.broadcast_to(
                    spinning_section[:, None, :], (count, device_attention_groups, ROPE)
                ),
            ],
            axis=-1,
        )
        raw_affinity_matrix = (
            jnp.einsum("qhd,khd->hqk", query, keys, preferred_element_type=jnp.float32) * scale
        )
        raw_affinity_matrix = raw_affinity_matrix + affinity_offset[:, None, None]
        fresh = jnp.maximum(peak, jnp.max(raw_affinity_matrix, axis=-1))
        probs = jnp.exp(raw_affinity_matrix - fresh[..., None])
        fade = jnp.exp(peak - fresh)
        total = total * fade + jnp.sum(probs, axis=-1)
        accum = accum * fade[..., None] + jnp.einsum(
            "hqk,khd->hqd",
            probs.astype(jnp.bfloat16),
            pairs[..., NOPE:],
            preferred_element_type=jnp.float32,
        )
        return (fresh, total, accum)

    blank_offset_matrix = jnp.zeros((device_attention_groups,), jnp.float32)
    start_carry = (
        jnp.full((device_attention_groups, rows), -1e30, jnp.float32),
        jnp.zeros((device_attention_groups, rows), jnp.float32),
        jnp.zeros((device_attention_groups, rows, DV), jnp.float32),
    )
    ctx_all_first, ctx_all_kr = (
        lax.all_gather(ctx_ckv_n, "sp", axis=0, tiled=True),
        lax.all_gather(ctx_kr, "sp", axis=0, tiled=True),
    )
    cumulative_loop_values = merged_question_vector(
        start_carry, ctx_all_first, ctx_all_kr, ctx_lift
    )
    fold_cumulative_loop_values = cumulative_loop_values
    front_section = lax.all_gather(ckv_n, "sp", axis=0, tiled=True)
    spinning_section = lax.all_gather(lat_kr, "sp", axis=0, tiled=True)
    count = front_section.shape[0] // rows
    blocks = (
        front_section.reshape(count, rows, front_section.shape[1]),
        spinning_section.reshape(count, rows, spinning_section.shape[1]),
    )

    def step(normalizer_statistics, segment_window):
        return (
            merged_question_vector(
                normalizer_statistics, segment_window[0], segment_window[1], blank_offset_matrix
            ),
            None,
        )

    fold_cumulative_loop_values, _ = lax.scan(step, fold_cumulative_loop_values, blocks)
    cumulative_loop_values = fold_cumulative_loop_values
    _, total, accum = cumulative_loop_values
    heads_out = (accum / total[..., None]).astype(jnp.bfloat16)
    branch = jnp.einsum("hqd,hde->qe", heads_out, w_out, preferred_element_type=jnp.float32)
    branch = lax.psum_scatter(
        branch.astype(jnp.bfloat16), "tp", scatter_dimension=1, tiled=True
    ).astype(jnp.float32)
    return (lat_f + modulation[0, 2] * branch).astype(jnp.bfloat16)


def call(kernel, outs, *args, flops=1e6, scratch=(), limit=8, held=pltpu.VMEM, kept=True, remote=()):
    single = not isinstance(outs, tuple)
    vmem = pl.BlockSpec(memory_space=pltpu.VMEM)
    outs = (outs,) if single else outs
    if kept:
        outs = tuple(pltpu.VMEM(o.shape, o.dtype) for o in outs)
    if held is not None:
        args = tuple(pltpu.with_memory_space_constraint(a, held) for a in args)
    result = pl.pallas_call(
        kernel,
        in_specs=[vmem] * len(args) + [pl.BlockSpec(memory_space=pltpu.HBM)] * len(remote),
        out_specs=(vmem,) * len(outs),
        out_shape=outs,
        scratch_shapes=scratch,
        cost_estimate=pl.CostEstimate(
            flops=int(flops), bytes_accessed=int(1e5), transcendentals=0
        ),
        compiler_params=pltpu.CompilerParams(vmem_limit_bytes=limit << 20),
    )(*args, *remote)
    return result[0] if single else result


def place():
    me = lax.axis_index("tp")
    return lax.axis_index("sp") * lax.axis_size("tp"), me // 2, lax.rem(me, 2), me


def dot_t(left, right, **options):
    return lax.dot_general(
        left, right, (((1,), (1,)), ((), ())), preferred_element_type=jnp.float32, **options
    )


def stats_kernel(
    lat_ref,
    ctx_ref,
    cond_ref,
    cond_ctx_ref,
    w_ref,
    g_ref,
    wq_ref,
    wkv_ref,
    wr_ref,
    out_ref,
    rows_ref,
    own_ref,
    other_ref,
    *,
    sp,
):
    rows_ref[: lat_ref.shape[0]] = lat_ref[...]
    rows_ref[lat_ref.shape[0] :] = ctx_ref[...]
    features, rank = wq_ref.shape
    half, width = rank // 2, ROPE // 2
    side = place()[2]
    for which, ref in ((side, own_ref), (1 - side, other_ref)):
        start = pl.multiple_of(which * half, half)
        ref[:features, :half] = wq_ref[:, pl.ds(start, half)]
        ref[:features, half:] = wkv_ref[:, pl.ds(start, half)]
        rot = wr_ref[pl.ds(pl.multiple_of(which * width, width), width), :]
        count = width * features // rank
        for i in range(rank // features):
            ref[features:, i * features : (i + 1) * features] = rot[i * count : (i + 1) * count]
    inner = cond_ref.shape[0]
    lat_c = jax.nn.silu(cond_ref[...].astype(jnp.float32).reshape(1, inner))
    ctx_c = jax.nn.silu(cond_ctx_ref[...].astype(jnp.float32).reshape(1, inner))
    row = lax.broadcasted_iota(jnp.int32, (16, inner), 0)
    signal = jnp.where(row < 8, lat_c, ctx_c).astype(jnp.bfloat16)
    parts = [jnp.dot(signal, w_ref[j], preferred_element_type=jnp.float32) for j in range(3)]
    gain = g_ref[...].reshape(1, g_ref.shape[0])
    gains = parts[1] * gain + gain * (1.0 / sp)
    modulation = jnp.concatenate(
        [parts[0][:1], gains[:1], parts[0][8:9], gains[8:9], parts[2][:1]], axis=1
    )
    for d in range(out_ref.shape[0]):
        out_ref[d] = modulation


def square_kernel(own_ref, other_ref, out_ref):
    ones = jnp.ones((8, own_ref.shape[1]), jnp.float32)
    total = None
    for ref in (own_ref, other_ref):
        values = ref[...].astype(jnp.float32)
        term = dot_t(ones, values * values, precision=lax.Precision.HIGHEST)
        total = term if total is None else total + term
    out_ref[...] = total


def project_kernel(
    own_ref, other_ref, mod_ref, w_own_ref, w_other_ref, *refs, sp, tp, rows
):
    chips = tp // 2
    squares, out_refs = refs[:chips], refs[chips : 2 * chips]
    gate_ref, lat_ref, ctx_ref, lat_rot_ref, ctx_rot_ref = refs[2 * chips :]
    count, features = own_ref.shape
    ctx_rows = count - rows
    rank = w_own_ref.shape[1]
    half = rank // 2
    unused, here, side, unused = place()
    total = squares[0][...]
    for ref in squares[1:]:
        total = total + ref[...]
    total = jnp.transpose(total)[:, :1]
    mine, partner = mod_ref[side], mod_ref[1 - side]
    for s in range(1, sp):
        mine = mine + mod_ref[2 * s + side]
        partner = partner + mod_ref[2 * s + 1 - side]
    gate_ref[...] = mine[:, 4 * features :]

    def split(ref):
        packed = ref[features:]
        rot = [packed[:, i * features : (i + 1) * features] for i in range(rank // features)]
        return ref[:features, :half], ref[:features, half:], jnp.concatenate(rot, axis=0)

    w_own, w_other = split(w_own_ref), split(w_other_ref)

    def rows_of(part, kind):
        own, other = own_ref[part].astype(jnp.float32), other_ref[part].astype(jnp.float32)
        inverse = lax.rsqrt(total[part] / D + EPS)
        first = second = rot = None
        for values, vectors, weights in ((own, mine, w_own), (other, partner, w_other)):
            shift = vectors[:, 2 * kind * features : (2 * kind + 1) * features]
            gain = vectors[:, (2 * kind + 1) * features : (2 * kind + 2) * features]
            h = (values * inverse * gain + shift).astype(jnp.bfloat16)
            terms = [None if kind else jnp.dot(h, weights[0], preferred_element_type=jnp.float32)]
            terms.append(jnp.dot(h, weights[1], preferred_element_type=jnp.float32))
            terms.append(dot_t(h, weights[2]))
            if second is None:
                first, second, rot = terms
            else:
                first = None if kind else first + terms[0]
                second, rot = second + terms[1], rot + terms[2]
        return first, second, rot

    lat_q, lat_kv, lat_rot = rows_of(slice(0, rows), 0)
    lat_ref[:, :half], lat_ref[:, half:], lat_rot_ref[...] = lat_q, lat_kv, lat_rot
    unused, ctx_ref[...], ctx_rot_ref[...] = rows_of(slice(rows, count), 1)
    lat, ctx = rows // tp, ctx_rows // tp
    quarter = (lat + ctx) // 4
    for hop in range(chips):
        for core in range(2):
            d = 2 * (here ^ hop) + core
            lats, ctxs = pl.ds(pl.multiple_of(d * lat, 8), lat), pl.ds(pl.multiple_of(d * ctx, 8), ctx)
            at = 0
            for source, part, size in ((lat_ref, lats, lat), (ctx_ref, ctxs, ctx)):
                for slab in range(source.shape[1] // 128):
                    out_refs[hop][core, at : at + size, :] = source[
                        part, slab * 128 : (slab + 1) * 128
                    ]
                    at += size
            rot = jnp.concatenate([lat_rot_ref[lats], ctx_rot_ref[ctxs]], axis=0)
            out_refs[hop][core, at : at + quarter, :] = jnp.concatenate(
                [rot[i * quarter : (i + 1) * quarter] for i in range(4)], axis=1
            )


def reduce_kernel(*refs):
    own_ref, other_ref = refs[-2:]
    side = place()[2]
    for which, ref in ((side, own_ref), (1 - side, other_ref)):
        total = refs[0][which]
        for part in refs[1:-2]:
            total = total + part[which]
        ref[...] = total


def prepare_kernel(inverse_ref, w_ref, tab_ref, out_ref):
    rows, lanes = tab_ref.shape
    position = lax.broadcasted_iota(jnp.int32, (rows, lanes), 0) + lax.axis_index("sp") * rows
    lane = lax.broadcasted_iota(jnp.int32, (rows, lanes), 1)
    along = jnp.where(lane % ROPE < ROPE // 2, position // GRID_W, position % GRID_W)
    angle = along.astype(jnp.float32) * inverse_ref[...]
    sine = jnp.sin(angle)
    sine = jnp.where(lane % (ROPE // 2) < ROPE // 4, -sine, sine)
    tab_ref[...] = jnp.where(lane < ROPE, jnp.cos(angle), sine)
    width = w_ref.shape[2]
    for head in range(w_ref.shape[1]):
        out_ref[:, head * width : (head + 1) * width] = w_ref[:, head, :]


def norm_kernel(own_ref, other_ref, gq_ref, gkv_ref, tab_ref, kv_ref, near_ref, *, lat, ctx):
    unused, unused, side, me = place()
    first = side == 0
    own, other = own_ref[...], other_ref[...]
    tab = tab_ref[pl.ds(pl.multiple_of(me * lat, 8), lat), :]
    halves = [jnp.where(first, own, other), jnp.where(first, other, own)]
    rank = gq_ref.shape[1]
    slabs = rank // 256

    def columns(start, count):
        return jnp.concatenate(
            [
                half[start + i * count : start + (i + 1) * count]
                for half in halves
                for i in range(slabs)
            ],
            axis=1,
        )

    def normed(values, gain):
        factor = lax.rsqrt(jnp.mean(values * values, axis=1, keepdims=True) + EPS)
        return (values * factor * gain).astype(jnp.bfloat16)

    cq = normed(columns(0, lat), gq_ref[...])
    lat_kv = normed(columns(slabs * lat, lat), gkv_ref[...])
    at = 2 * slabs * lat
    ctx_kv = normed(columns(at, ctx), gkv_ref[...])
    at += slabs * ctx
    quarter = (lat + ctx) // 4
    width = ROPE // 2
    lat_rot, ctx_rot = [], []
    for core in range(2):
        packed = halves[core][at : at + quarter]
        rot = jnp.concatenate(
            [packed[:, i * width : (i + 1) * width] for i in range(4)], axis=0
        )
        turned = rot[:lat]
        swapped = jnp.concatenate([turned[:, width // 2 :], turned[:, : width // 2]], axis=1)
        cosine = tab[:, core * width : (core + 1) * width]
        sine = tab[:, ROPE + core * width : ROPE + (core + 1) * width]
        lat_rot.append(turned * cosine + swapped * sine)
        ctx_rot.append(rot[lat:])
    keys = jnp.concatenate(
        [jnp.concatenate(lat_rot, axis=1), jnp.concatenate(ctx_rot, axis=1)], axis=0
    )
    pieces = rank // ROPE
    low = (lat + ctx) // pieces
    keys = jnp.concatenate(
        [keys[i * low : (i + 1) * low] for i in range(pieces)], axis=1
    ).astype(jnp.bfloat16)
    compressed = jnp.concatenate([lat_kv, ctx_kv], axis=0)
    for ref in (kv_ref, near_ref):
        ref[: lat + ctx] = compressed
        ref[lat + ctx : lat + ctx + low] = keys
    near_ref[lat + ctx + low :] = cq


def gather_kernel(*refs):
    size = refs[0].shape[0]
    for i, ref in enumerate(refs[:-1]):
        refs[-1][i * size : (i + 1) * size] = ref[...]


def unpack(chunks, kv_ref, key_ref, lat, ctx):
    count = lat + ctx
    rank = kv_ref.shape[1]
    row = lax.broadcasted_iota(jnp.int32, (count, 128 - ROPE), 0)
    lane = lax.broadcasted_iota(jnp.int32, (count, 128 - ROPE), 1)
    flags = jnp.where((row >= lat) & (lane < 3), 1.0, 0.0)
    for i, (ref, at) in enumerate(chunks):
        kv_ref[i * count : (i + 1) * count] = ref[at : at + count]
        low = count * ROPE // rank
        packed = ref[at + count : at + count + low].astype(jnp.float32)
        rot = [packed[:, j * ROPE : (j + 1) * ROPE] for j in range(rank // ROPE)]
        rot = jnp.concatenate([jnp.concatenate(rot, axis=0), flags], axis=1)
        key_ref[i * count : (i + 1) * count] = rot.astype(jnp.bfloat16)


def expanded(kv_ref, w_ref, head):
    weight = w_ref[:, head * (NOPE + DV) : (head + 1) * (NOPE + DV)]
    return jnp.dot(kv_ref[...], weight, preferred_element_type=jnp.float32).astype(jnp.bfloat16)


def weighted(score, values):
    peak = jnp.max(score, axis=1, keepdims=True)
    probs = jnp.exp2((score - peak) * ((NOPE + ROPE) ** -0.5 * LOG2E))
    total = jnp.sum(probs, axis=1, keepdims=True)
    summed = jnp.dot(probs.astype(jnp.bfloat16), values, preferred_element_type=jnp.float32)
    return peak, total, summed


def staged(steps):
    score = steps[0][0]()
    for i, (unused, finish) in enumerate(steps):
        after = steps[i + 1][0]() if i + 1 < len(steps) else None
        finish(score)
        score = after


def near_kernel(tab_ref, lift_ref, wq_ref, wkv_ref, *refs, lat, ctx, chips):
    own_refs, other_refs = refs[:chips], refs[chips : 2 * chips]
    query_ref, stat_ref, sum_ref, cq_ref, kv_ref, key_ref = refs[-6:]
    size = own_refs[0].shape[0]
    unused, here, side, unused = place()
    for hop in range(chips):
        own, other = own_refs[hop][size - lat :], other_refs[hop][size - lat :]
        at = pl.multiple_of(2 * (here ^ hop) * lat, 16)
        cq_ref[pl.ds(at, lat)] = jnp.where(side == 0, own, other)
        cq_ref[pl.ds(at + lat, lat)] = jnp.where(side == 0, other, own)
    chunks = [(ref, 0) for ref in own_refs + other_refs]
    chunks += chunks_of(refs[2 * chips : -6], size - lat)
    unpack(chunks, kv_ref, key_ref, lat, ctx)
    heads = wq_ref.shape[0]
    quarter = ROPE // 4
    lane = lax.broadcasted_iota(jnp.int32, (1, 2 * ROPE), 1)

    def prepare(head):
        pieces = [wq_ref[head]]
        for block in (1, 0, 3, 2):
            pieces.append(wq_ref[head, NOPE + block * quarter : NOPE + (block + 1) * quarter])
        raw = dot_t(cq_ref[...], jnp.concatenate(pieces, axis=0))
        turned = raw[:, NOPE:] * tab_ref[...]
        turned = turned + pltpu.roll(turned, ROPE, 1)
        lift = lift_ref[head : head + 1] * (NOPE + ROPE) ** 0.5
        first = lift.astype(jnp.bfloat16).astype(jnp.float32)
        second = (lift - first).astype(jnp.bfloat16).astype(jnp.float32)
        third = lift - first - second
        lifts = jnp.where(lane == ROPE, first, jnp.where(lane == ROPE + 1, second, third))
        lifts = jnp.where(lane < ROPE + 3, lifts, 0.0)
        turned = jnp.where(lane < ROPE, turned, lifts)
        query = jnp.concatenate([raw[:, :NOPE], turned], axis=1).astype(jnp.bfloat16)
        query_ref[head] = query

    stats = {}

    def step(head):
        def score():
            prepare(head)
            stats[head] = expanded(kv_ref, wkv_ref, head)
            keys = jnp.concatenate([stats[head][:, :NOPE], key_ref[...]], axis=1)
            return dot_t(query_ref[head], keys)

        def finish(values):
            peak, total, summed = weighted(values, stats[head][:, NOPE:])
            stat_ref[:, head : head + 1] = peak
            stat_ref[:, heads + head : heads + head + 1] = total
            sum_ref[head] = summed

        return score, finish

    staged([step(head) for head in range(heads)])


def chunks_of(refs, step):
    return [(ref, at) for ref in refs for at in range(0, refs[0].shape[0], step)]


def expand_kernel(w_ref, *refs, lat, ctx):
    key_ref, value_ref, kv_ref, rot_ref = refs[-4:]
    step = lat + ctx + (lat + ctx) * ROPE // w_ref.shape[0]
    unpack(chunks_of(refs[:-4], step), kv_ref, rot_ref, lat, ctx)
    for head in range(key_ref.shape[0]):
        pairs = expanded(kv_ref, w_ref, head)
        key_ref[head, :, :NOPE] = pairs[:, :NOPE]
        key_ref[head, :, NOPE:] = rot_ref[...]
        value_ref[head] = pairs[:, NOPE:]


def far_kernel(query_ref, stat_ref, sum_ref, key_ref, value_ref, w_ref, *refs, lat, ctx):
    up_ref, out_ref, up_out_ref, kv_ref, rot_ref, done = refs[-6:]
    copy = pltpu.make_async_copy(up_ref, up_out_ref, done)
    copy.start()
    step = lat + ctx + (lat + ctx) * ROPE // w_ref.shape[0]
    unpack(chunks_of(refs[:-6], step), kv_ref, rot_ref, lat, ctx)
    heads = query_ref.shape[0]
    factor = (NOPE + ROPE) ** -0.5 * LOG2E
    held = {}

    def step_of(head):
        def score():
            pairs = expanded(kv_ref, w_ref, head)
            keys = jnp.concatenate([pairs[:, :NOPE], rot_ref[...]], axis=1)
            held[head] = (keys, pairs[:, NOPE:])
            query = query_ref[head]
            return dot_t(query, key_ref[head]), dot_t(query, held[head][0])

        def finish(scores):
            near = stat_ref[:, head : head + 1]
            top = near
            for values in scores:
                top = jnp.maximum(top, jnp.max(values, axis=1, keepdims=True))
            old = jnp.exp2((near - top) * factor)
            total = stat_ref[:, heads + head : heads + head + 1] * old
            summed = sum_ref[head] * old
            for values, weights in zip(scores, (value_ref[head], held[head][1]), strict=True):
                probs = jnp.exp2((values - top) * factor)
                total = total + jnp.sum(probs, axis=1, keepdims=True)
                summed = summed + jnp.dot(
                    probs.astype(jnp.bfloat16), weights, preferred_element_type=jnp.float32
                )
            out_ref[:, head * DV : (head + 1) * DV] = (summed / total).astype(jnp.bfloat16)

        return score, finish

    staged([step_of(head) for head in range(heads)])
    copy.wait()


def share_out_kernel(w_ref, out_ref):
    chips, unused, features = out_ref.shape
    unused, here, side, unused = place()
    for hop in range(chips):
        start = pl.multiple_of((2 * (here ^ hop) + 1 - side) * features, features)
        out_ref[hop] = w_ref[:, pl.ds(start, features)]


def output_own_kernel(heads_ref, w_ref, out_ref):
    chips, unused, features = out_ref.shape
    unused, here, side, unused = place()
    for hop in range(chips):
        start = pl.multiple_of((2 * (here ^ hop) + side) * features, features)
        out_ref[hop] = jnp.dot(
            heads_ref[...], w_ref[:, pl.ds(start, features)], preferred_element_type=jnp.float32
        )


def output_kernel(heads_ref, w_ref, acc_ref, *out_refs):
    for hop in reversed(range(len(out_refs))):
        acc = acc_ref[hop] + jnp.dot(
            heads_ref[...], w_ref[hop], preferred_element_type=jnp.float32
        )
        out_refs[hop][...] = acc.astype(out_refs[hop].dtype)


def mix_kernel(latent_ref, gate_ref, *refs):
    branch = refs[0][...]
    for ref in refs[1:-1]:
        branch = branch + ref[...].astype(jnp.float32)
    refs[-1][...] = (latent_ref[...].astype(jnp.float32) + gate_ref[...] * branch).astype(
        jnp.bfloat16
    )


def split_device(
    latent,
    context,
    cond,
    cond_ctx,
    w_mod,
    g_norm,
    w_dq,
    w_dkv,
    w_kr,
    g_cq,
    g_ckv,
    w_uq,
    w_ukv,
    ctx_lift,
    w_out,
):
    f32, bf16 = jnp.float32, jnp.bfloat16
    sp, tp = lax.axis_size("sp"), lax.axis_size("tp")
    chips = tp // 2
    rows, features = latent.shape
    ctx_rows = context.shape[0]
    heads = w_uq.shape[1]
    rank = w_dq.shape[1]
    lat, ctx = rows // tp, ctx_rows // tp
    half = rank // 2
    across = [(i, i ^ 1) for i in range(tp)]

    def array(shape, dtype=bf16):
        return jax.ShapeDtypeStruct(shape, dtype)

    def hopped(value):
        return [value] + [
            lax.ppermute(value, "tp", [(i, i ^ (2 * hop)) for i in range(tp)])
            for hop in range(1, chips)
        ]

    share = array((features + ROPE // 2 * features // rank, rank))
    modulation, tokens, w_own, w_other = call(
        functools.partial(stats_kernel, sp=sp),
        (
            array((2 * sp, 1, 5 * features), f32),
            array((rows + ctx_rows, features)),
            share,
            share,
        ),
        latent,
        context,
        cond,
        cond_ctx,
        jnp.transpose(w_mod, (1, 0, 2)),
        g_norm,
        w_dq,
        w_dkv,
        w_kr.T,
        held=pltpu.HBM,
    )
    w_other = lax.ppermute(w_other, "tp", across)
    tokens_other = lax.ppermute(tokens, "tp", across)
    columns = [[s * tp + 2 * c + k for s in range(sp) for k in range(2)] for c in range(chips)]
    modulation = lax.all_to_all(modulation, ("sp", "tp"), 0, 0, axis_index_groups=columns)
    squares = call(square_kernel, array((8, rows + ctx_rows), f32), tokens, tokens_other)
    squares = hopped(squares)

    height = half // 128 * (2 * lat + ctx) + (lat + ctx) // 4
    share = array((2, height, 128), f32)
    *parts, gate = call(
        functools.partial(project_kernel, sp=sp, tp=tp, rows=rows),
        (share,) * chips + (array((1, features), f32),),
        tokens,
        tokens_other,
        modulation,
        w_own,
        w_other,
        *squares,
        scratch=[
            pltpu.VMEM((rows, rank), f32),
            pltpu.VMEM((ctx_rows, half), f32),
            pltpu.VMEM((rows, ROPE // 2), f32),
            pltpu.VMEM((ctx_rows, ROPE // 2), f32),
        ],
        flops=4 * (rows + ctx_rows) * features * (rank + 128),
        limit=16,
    )
    *parts, w_kv, w_up, zero = lax.optimization_barrier((*parts, w_ukv, w_out, jnp.float32(0)))
    parts = [parts[0]] + [
        lax.ppermute(part, "tp", [(i, i ^ (2 * hop + 2)) for i in range(tp)])
        for hop, part in enumerate(parts[1:])
    ]

    quarter = ROPE // 4
    inverse = THETA ** (-np.arange(quarter) / quarter)
    inverse = jnp.asarray(np.tile(inverse, 128 // quarter)[None], f32) + zero
    q_tab, w_kv = call(
        prepare_kernel,
        (array((rows, 128), f32), array((rank, heads * (NOPE + DV)))),
        inverse,
        w_kv,
        flops=1e9,
    )
    w_up = w_up.reshape(heads * DV, 2 * chips * features)
    w_up_other = call(
        share_out_kernel, array((chips, heads * DV, features)), w_up, flops=1e9, kept=False
    )
    w_up_other = lax.ppermute(w_up_other, "tp", across)
    *parts, q_tab, w_up_other, w_kv = lax.optimization_barrier((*parts, q_tab, w_up_other, w_kv))
    share = array((height, 128), f32)
    part, part_other = call(reduce_kernel, (share, share), *parts)
    part_other = lax.ppermute(part_other, "tp", across)

    count = lat + ctx
    step = count + count * ROPE // rank
    kv, near = call(
        functools.partial(norm_kernel, lat=lat, ctx=ctx),
        (array((step, rank)), array((step + lat, rank))),
        part,
        part_other,
        g_cq[None],
        g_ckv[None],
        q_tab,
    )

    planes = [
        lax.ppermute(kv, "sp", [(i, (i + shift) % sp) for i in range(sp)])
        for shift in range(1, sp)
    ]
    near_own = hopped(near)
    near_own, planes = lax.optimization_barrier((near_own, planes))
    near_other = [lax.ppermute(n, "tp", across) for n in near_own]
    far = call(gather_kernel, array(((sp - 1) * step, rank)), *planes)
    far_own = hopped(far)
    far_other = [lax.ppermute(f, "tp", across) for f in far_own]

    keys = (tp + 2 * (sp - 1)) * count
    query, stats, summed = call(
        functools.partial(near_kernel, lat=lat, ctx=ctx, chips=chips),
        (
            array((heads, rows, 2 * NOPE)),
            array((rows, 128), f32),
            array((heads, rows, DV), f32),
        ),
        q_tab,
        jnp.broadcast_to(ctx_lift[:, None], (heads, 128)),
        jnp.transpose(w_uq, (1, 2, 0)),
        w_kv,
        *near_own,
        *near_other,
        far_own[0],
        far_other[0],
        scratch=[
            pltpu.VMEM((rows, rank), bf16),
            pltpu.VMEM((keys, rank), bf16),
            pltpu.VMEM((keys, 128), bf16),
        ],
        flops=heads * rows * (2 * rank * 256 + 2 * keys * 384),
        limit=16,
    )
    keys = (chips - 1) * (sp - 1) * count
    scratch = [pltpu.VMEM((keys, rank), bf16), pltpu.VMEM((keys, 128), bf16)]
    far_keys, far_values = call(
        functools.partial(expand_kernel, lat=lat, ctx=ctx),
        (array((heads, keys, 2 * NOPE)), array((heads, keys, DV))),
        w_kv,
        *far_own[1:],
        scratch=scratch,
        flops=2 * keys * rank * 256 * heads,
    )
    heads_out, w_up_other = call(
        functools.partial(far_kernel, lat=lat, ctx=ctx),
        (array((rows, heads * DV)), array(w_up_other.shape)),
        query,
        stats,
        summed,
        far_keys,
        far_values,
        w_kv,
        *far_other[1:],
        remote=(w_up_other,),
        scratch=scratch + [pltpu.SemaphoreType.DMA],
        flops=2 * heads * keys * (2 * rows * 384 + rank * 256),
        limit=28,
    )

    heads_other = lax.ppermute(heads_out, "tp", across)
    flops = 2 * rows * heads * DV * chips * features
    branch = call(
        output_own_kernel, array((chips, rows, features), f32), heads_out, w_up, flops=flops
    )
    block = array((rows, features))
    branch, *apart = call(
        output_kernel,
        (array((rows, features), f32),) + (block,) * (chips - 1),
        heads_other,
        w_up_other,
        branch,
        flops=flops,
    )
    apart = [
        lax.ppermute(a, "tp", [(i, i ^ (2 * hop + 2)) for i in range(tp)])
        for hop, a in enumerate(apart)
    ]
    return call(mix_kernel, array(latent.shape), latent, gate, branch, *apart, kept=False)


def chosen(*arrays):
    rows, ctx_rows, features = arrays[0].shape[0], arrays[1].shape[0], arrays[0].shape[1]
    tp = lax.axis_size("tp")
    aligned = rows % (16 * tp) == 0 and ctx_rows % (16 * tp) == 0 and features % 128 == 0 and arrays[6].shape[1] % features == 0
    return (split_device if tp in (2, 4, 8, 16) and aligned else plain_device)(*arrays)


def solution(mesh):
    return jax.shard_map(
        chosen,
        mesh=mesh,
        in_specs=(
            P("sp", "tp"),
            P("sp", "tp"),
            P("sp"),
            P("sp"),
            P("sp", None, "tp"),
            P("tp"),
            P("tp", None),
            P("tp", None),
            P("tp", None),
            P(),
            P(),
            P(None, "tp", None),
            P(None, "tp", None),
            P("tp"),
            P("tp", None, None),
        ),
        out_specs=P("sp", "tp"),
        check_vma=False,
    )
```

```python
import functools

import jax
import jax.numpy as jnp
import numpy as np
from jax import lax
from jax.experimental import pallas as pl
from jax.experimental.pallas import tpu as pltpu
from jax.sharding import PartitionSpec as P

D = 2048
NOPE = 128
ROPE = 64
DV = 128
GRID_W = 64


EPS = 1e-06
THETA = 10000.0
LOG2E = 1.4426950408889634


def tables(positions):
    row = (positions // GRID_W).astype(jnp.float32)
    col = (positions % GRID_W).astype(jnp.float32)
    half = ROPE // 2
    inverse = 1.0 / THETA ** (jnp.arange(0, half, 2, dtype=jnp.float32) / half)
    angle = jnp.concatenate([row[:, None] * inverse, col[:, None] * inverse], axis=-1)
    return (jnp.cos(angle), jnp.sin(angle))


def rotate(values, cosine, sine):
    shape = values.shape
    quarter = ROPE // 4
    parts = values.reshape(shape[:-1] + (2, 2, quarter))
    extra = (1,) * (len(shape) - 2)
    cosine = cosine.reshape((shape[0],) + extra + (2, quarter))
    sine = sine.reshape((shape[0],) + extra + (2, quarter))
    front_section = parts[..., 0, :]
    second = parts[..., 1, :]
    turned = jnp.stack(
        [front_section * cosine - second * sine, front_section * sine + second * cosine], axis=-2
    )
    return turned.reshape(shape)


def modulated(values, sumsq, gain, modulation):
    scaled = values * lax.rsqrt(sumsq / D + EPS)[:, None] * gain
    return (scaled * (1.0 + modulation[1]) + modulation[0]).astype(jnp.bfloat16)


def low_norm(values, gain):
    scale = lax.rsqrt(jnp.mean(values * values, axis=-1, keepdims=True) + EPS)
    return (values * scale * gain).astype(jnp.bfloat16)


def plain_device(
    latent,
    context,
    cond,
    cond_ctx,
    w_mod,
    g_norm,
    w_dq,
    w_dkv,
    w_kr,
    g_cq,
    g_ckv,
    w_uq,
    w_ukv,
    ctx_lift,
    w_out,
):
    rows = latent.shape[0]
    device_attention_groups = w_uq.shape[1]
    signal = jnp.stack(
        [jax.nn.silu(cond.astype(jnp.float32)), jax.nn.silu(cond_ctx.astype(jnp.float32))]
    ).astype(jnp.bfloat16)
    partial_mod = jnp.dot(
        signal, w_mod.reshape(w_mod.shape[0], -1), preferred_element_type=jnp.float32
    )
    modulation = lax.psum(partial_mod.reshape(2, 3, -1), "sp")
    lat_f = latent.astype(jnp.float32)
    ctx_f = context.astype(jnp.float32)
    lat_sq, ctx_sq = lax.psum(
        (jnp.sum(lat_f * lat_f, axis=1), jnp.sum(ctx_f * ctx_f, axis=1)), "tp"
    )
    lat_h = modulated(lat_f, lat_sq, g_norm, modulation[0])
    ctx_h = modulated(ctx_f, ctx_sq, g_norm, modulation[1])
    positions = lax.axis_index("sp") * rows + jnp.arange(rows, dtype=jnp.int32)
    cosine, sine = tables(positions)
    lat_q, lat_kv, lat_rot, ctx_kv, ctx_rot = lax.psum(
        (
            jnp.dot(lat_h, w_dq, preferred_element_type=jnp.float32),
            jnp.dot(lat_h, w_dkv, preferred_element_type=jnp.float32),
            jnp.dot(lat_h, w_kr, preferred_element_type=jnp.float32),
            jnp.dot(ctx_h, w_dkv, preferred_element_type=jnp.float32),
            jnp.dot(ctx_h, w_kr, preferred_element_type=jnp.float32),
        ),
        "tp",
    )
    cq_n = low_norm(lat_q, g_cq)
    ckv_n = low_norm(lat_kv, g_ckv)
    lat_kr = rotate(lat_rot, cosine, sine).astype(jnp.bfloat16)
    ctx_ckv_n = low_norm(ctx_kv, g_ckv)
    ctx_kr = ctx_rot.astype(jnp.bfloat16)
    query = jnp.dot(cq_n, w_uq.reshape(w_uq.shape[0], -1), preferred_element_type=jnp.float32)
    query = query.reshape(rows, device_attention_groups, NOPE + ROPE)
    query = jnp.concatenate(
        [query[..., :NOPE], rotate(query[..., NOPE:], cosine, sine)], axis=-1
    ).astype(jnp.bfloat16)
    up_weight = w_ukv.reshape(w_ukv.shape[0], -1)
    scale = (NOPE + ROPE) ** (-0.5)

    def expand(compressed):
        return jnp.dot(compressed, up_weight, preferred_element_type=jnp.float32).astype(
            jnp.bfloat16
        )

    def unpack(front_section):
        return expand(front_section).reshape(
            front_section.shape[0], device_attention_groups, NOPE + DV
        )

    def merged_question_vector(
        cumulative_loop_values, front_section, spinning_section, affinity_offset
    ):
        peak, total, accum = cumulative_loop_values
        pairs = unpack(front_section)
        count = pairs.shape[0]
        keys = jnp.concatenate(
            [
                pairs[..., :NOPE],
                jnp.broadcast_to(
                    spinning_section[:, None, :], (count, device_attention_groups, ROPE)
                ),
            ],
            axis=-1,
        )
        raw_affinity_matrix = (
            jnp.einsum("qhd,khd->hqk", query, keys, preferred_element_type=jnp.float32) * scale
        )
        raw_affinity_matrix = raw_affinity_matrix + affinity_offset[:, None, None]
        fresh = jnp.maximum(peak, jnp.max(raw_affinity_matrix, axis=-1))
        probs = jnp.exp(raw_affinity_matrix - fresh[..., None])
        fade = jnp.exp(peak - fresh)
        total = total * fade + jnp.sum(probs, axis=-1)
        accum = accum * fade[..., None] + jnp.einsum(
            "hqk,khd->hqd",
            probs.astype(jnp.bfloat16),
            pairs[..., NOPE:],
            preferred_element_type=jnp.float32,
        )
        return (fresh, total, accum)

    blank_offset_matrix = jnp.zeros((device_attention_groups,), jnp.float32)
    start_carry = (
        jnp.full((device_attention_groups, rows), -1e30, jnp.float32),
        jnp.zeros((device_attention_groups, rows), jnp.float32),
        jnp.zeros((device_attention_groups, rows, DV), jnp.float32),
    )
    ctx_all_first, ctx_all_kr = (
        lax.all_gather(ctx_ckv_n, "sp", axis=0, tiled=True),
        lax.all_gather(ctx_kr, "sp", axis=0, tiled=True),
    )
    cumulative_loop_values = merged_question_vector(
        start_carry, ctx_all_first, ctx_all_kr, ctx_lift
    )
    fold_cumulative_loop_values = cumulative_loop_values
    front_section = lax.all_gather(ckv_n, "sp", axis=0, tiled=True)
    spinning_section = lax.all_gather(lat_kr, "sp", axis=0, tiled=True)
    count = front_section.shape[0] // rows
    blocks = (
        front_section.reshape(count, rows, front_section.shape[1]),
        spinning_section.reshape(count, rows, spinning_section.shape[1]),
    )

    def step(normalizer_statistics, segment_window):
        return (
            merged_question_vector(
                normalizer_statistics, segment_window[0], segment_window[1], blank_offset_matrix
            ),
            None,
        )

    fold_cumulative_loop_values, _ = lax.scan(step, fold_cumulative_loop_values, blocks)
    cumulative_loop_values = fold_cumulative_loop_values
    _, total, accum = cumulative_loop_values
    heads_out = (accum / total[..., None]).astype(jnp.bfloat16)
    branch = jnp.einsum("hqd,hde->qe", heads_out, w_out, preferred_element_type=jnp.float32)
    branch = lax.psum_scatter(
        branch.astype(jnp.bfloat16), "tp", scatter_dimension=1, tiled=True
    ).astype(jnp.float32)
    return (lat_f + modulation[0, 2] * branch).astype(jnp.bfloat16)


def call(kernel, outs, *args, flops=1e6, scratch=(), limit=8, held=pltpu.VMEM, kept=True, remote=()):
    single = not isinstance(outs, tuple)
    vmem = pl.BlockSpec(memory_space=pltpu.VMEM)
    outs = (outs,) if single else outs
    if kept:
        outs = tuple(pltpu.VMEM(o.shape, o.dtype) for o in outs)
    if held is not None:
        args = tuple(pltpu.with_memory_space_constraint(a, held) for a in args)
    result = pl.pallas_call(
        kernel,
        in_specs=[vmem] * len(args) + [pl.BlockSpec(memory_space=pltpu.HBM)] * len(remote),
        out_specs=(vmem,) * len(outs),
        out_shape=outs,
        scratch_shapes=scratch,
        cost_estimate=pl.CostEstimate(
            flops=int(flops), bytes_accessed=int(1e5), transcendentals=0
        ),
        compiler_params=pltpu.CompilerParams(vmem_limit_bytes=limit << 20),
    )(*args, *remote)
    return result[0] if single else result


def place():
    me = lax.axis_index("tp")
    return lax.axis_index("sp") * lax.axis_size("tp"), me // 2, lax.rem(me, 2), me


def dot_t(left, right, **options):
    return lax.dot_general(
        left, right, (((1,), (1,)), ((), ())), preferred_element_type=jnp.float32, **options
    )


def stats_kernel(
    lat_ref,
    ctx_ref,
    cond_ref,
    cond_ctx_ref,
    w_ref,
    g_ref,
    wq_ref,
    wkv_ref,
    wr_ref,
    out_ref,
    rows_ref,
    own_ref,
    other_ref,
    *,
    sp,
):
    rows_ref[: lat_ref.shape[0]] = lat_ref[...]
    rows_ref[lat_ref.shape[0] :] = ctx_ref[...]
    features, rank = wq_ref.shape
    half, width = rank // 2, ROPE // 2
    side = place()[2]
    for which, ref in ((side, own_ref), (1 - side, other_ref)):
        start = pl.multiple_of(which * half, half)
        ref[:features, :half] = wq_ref[:, pl.ds(start, half)]
        ref[:features, half:] = wkv_ref[:, pl.ds(start, half)]
        rot = wr_ref[pl.ds(pl.multiple_of(which * width, width), width), :]
        count = width * features // rank
        for i in range(rank // features):
            ref[features:, i * features : (i + 1) * features] = rot[i * count : (i + 1) * count]
    inner = cond_ref.shape[0]
    lat_c = jax.nn.silu(cond_ref[...].astype(jnp.float32).reshape(1, inner))
    ctx_c = jax.nn.silu(cond_ctx_ref[...].astype(jnp.float32).reshape(1, inner))
    row = lax.broadcasted_iota(jnp.int32, (16, inner), 0)
    signal = jnp.where(row < 8, lat_c, ctx_c).astype(jnp.bfloat16)
    parts = [jnp.dot(signal, w_ref[j], preferred_element_type=jnp.float32) for j in range(3)]
    gain = g_ref[...].reshape(1, g_ref.shape[0])
    gains = parts[1] * gain + gain * (1.0 / sp)
    modulation = jnp.concatenate(
        [parts[0][:1], gains[:1], parts[0][8:9], gains[8:9], parts[2][:1]], axis=1
    )
    for d in range(out_ref.shape[0]):
        out_ref[d] = modulation


def square_kernel(own_ref, other_ref, out_ref):
    ones = jnp.ones((8, own_ref.shape[1]), jnp.float32)
    total = None
    for ref in (own_ref, other_ref):
        values = ref[...].astype(jnp.float32)
        term = dot_t(ones, values * values, precision=lax.Precision.HIGHEST)
        total = term if total is None else total + term
    out_ref[...] = total


def project_kernel(
    own_ref, other_ref, mod_ref, w_own_ref, w_other_ref, *refs, sp, tp, rows
):
    chips = tp // 2
    squares, kv_refs, q_refs = refs[:chips], refs[chips : 2 * chips], refs[2 * chips : 3 * chips]
    gate_ref, lat_ref, ctx_ref, lat_rot_ref, ctx_rot_ref = refs[3 * chips :]
    count, features = own_ref.shape
    ctx_rows = count - rows
    rank = w_own_ref.shape[1]
    half = rank // 2
    unused, here, side, unused = place()
    total = squares[0][...]
    for ref in squares[1:]:
        total = total + ref[...]
    total = jnp.transpose(total)[:, :1]
    mine, partner = mod_ref[side], mod_ref[1 - side]
    for s in range(1, sp):
        mine = mine + mod_ref[2 * s + side]
        partner = partner + mod_ref[2 * s + 1 - side]
    gate_ref[...] = mine[:, 4 * features :]

    def split(ref):
        packed = ref[features:]
        rot = [packed[:, i * features : (i + 1) * features] for i in range(rank // features)]
        return ref[:features, :half], ref[:features, half:], jnp.concatenate(rot, axis=0)

    w_own, w_other = split(w_own_ref), split(w_other_ref)

    def rows_of(part, kind):
        own, other = own_ref[part].astype(jnp.float32), other_ref[part].astype(jnp.float32)
        inverse = lax.rsqrt(total[part] / D + EPS)
        first = second = rot = None
        for values, vectors, weights in ((own, mine, w_own), (other, partner, w_other)):
            shift = vectors[:, 2 * kind * features : (2 * kind + 1) * features]
            gain = vectors[:, (2 * kind + 1) * features : (2 * kind + 2) * features]
            h = (values * inverse * gain + shift).astype(jnp.bfloat16)
            terms = [None if kind else jnp.dot(h, weights[0], preferred_element_type=jnp.float32)]
            terms.append(jnp.dot(h, weights[1], preferred_element_type=jnp.float32))
            terms.append(dot_t(h, weights[2]))
            if second is None:
                first, second, rot = terms
            else:
                first = None if kind else first + terms[0]
                second, rot = second + terms[1], rot + terms[2]
        return first, second, rot

    lat_q, lat_kv, lat_rot = rows_of(slice(0, rows), 0)
    lat_ref[:, :half], lat_ref[:, half:], lat_rot_ref[...] = lat_q, lat_kv, lat_rot
    unused, ctx_ref[...], ctx_rot_ref[...] = rows_of(slice(rows, count), 1)
    lat, ctx = rows // tp, ctx_rows // tp
    quarter = (lat + ctx) // 4
    for hop in range(chips):
        for core in range(2):
            d = 2 * (here ^ hop) + core
            lats, ctxs = pl.ds(pl.multiple_of(d * lat, 8), lat), pl.ds(pl.multiple_of(d * ctx, 8), ctx)
            for slab in range(half // 128):
                q_refs[hop][core, slab * lat : (slab + 1) * lat, :] = lat_ref[
                    lats, slab * 128 : (slab + 1) * 128
                ]
            at = 0
            for source, part, first, size in (
                (lat_ref, lats, half, lat),
                (ctx_ref, ctxs, 0, ctx),
            ):
                for column in range(first, source.shape[1], 128):
                    kv_refs[hop][core, at : at + size, :] = source[part, column : column + 128]
                    at += size
            rot = jnp.concatenate([lat_rot_ref[lats], ctx_rot_ref[ctxs]], axis=0)
            kv_refs[hop][core, at : at + quarter, :] = jnp.concatenate(
                [rot[i * quarter : (i + 1) * quarter] for i in range(4)], axis=1
            )


def reduce_kernel(*refs):
    own_ref, other_ref = refs[-2:]
    side = place()[2]
    for which, ref in ((side, own_ref), (1 - side, other_ref)):
        total = refs[0][which]
        for part in refs[1:-2]:
            total = total + part[which]
        ref[...] = total


def tables_kernel(inverse_ref, tab_ref):
    rows, lanes = tab_ref.shape
    position = lax.broadcasted_iota(jnp.int32, (rows, lanes), 0) + lax.axis_index("sp") * rows
    lane = lax.broadcasted_iota(jnp.int32, (rows, lanes), 1)
    along = jnp.where(lane % ROPE < ROPE // 2, position // GRID_W, position % GRID_W)
    angle = along.astype(jnp.float32) * inverse_ref[...]
    sine = jnp.sin(angle)
    sine = jnp.where(lane % (ROPE // 2) < ROPE // 4, -sine, sine)
    tab_ref[...] = jnp.where(lane < ROPE, jnp.cos(angle), sine)


def relay_kernel(w_ref, out_ref):
    width = w_ref.shape[2]
    for head in range(w_ref.shape[1]):
        out_ref[:, head * width : (head + 1) * width] = w_ref[:, head, :]


def halves_of(own_ref, other_ref):
    first = place()[2] == 0
    own, other = own_ref[...], other_ref[...]
    return [jnp.where(first, own, other), jnp.where(first, other, own)]


def normed(halves, start, count, gain_ref):
    slabs = gain_ref.shape[1] // 256
    values = jnp.concatenate(
        [
            half[start + i * count : start + (i + 1) * count]
            for half in halves
            for i in range(slabs)
        ],
        axis=1,
    )
    factor = lax.rsqrt(jnp.mean(values * values, axis=1, keepdims=True) + EPS)
    return (values * factor * gain_ref[...]).astype(jnp.bfloat16)


def norm_kernel(own_ref, other_ref, gain_ref, tab_ref, kv_ref, *, lat, ctx):
    me = place()[3]
    tab = tab_ref[pl.ds(pl.multiple_of(me * lat, 8), lat), :]
    halves = halves_of(own_ref, other_ref)
    rank = gain_ref.shape[1]
    slabs = rank // 256
    lat_kv = normed(halves, 0, lat, gain_ref)
    at = slabs * lat
    ctx_kv = normed(halves, at, ctx, gain_ref)
    at += slabs * ctx
    quarter = (lat + ctx) // 4
    width = ROPE // 2
    lat_rot, ctx_rot = [], []
    for core in range(2):
        packed = halves[core][at : at + quarter]
        rot = jnp.concatenate(
            [packed[:, i * width : (i + 1) * width] for i in range(4)], axis=0
        )
        turned = rot[:lat]
        swapped = jnp.concatenate([turned[:, width // 2 :], turned[:, : width // 2]], axis=1)
        cosine = tab[:, core * width : (core + 1) * width]
        sine = tab[:, ROPE + core * width : ROPE + (core + 1) * width]
        lat_rot.append(turned * cosine + swapped * sine)
        ctx_rot.append(rot[lat:])
    keys = jnp.concatenate(
        [jnp.concatenate(lat_rot, axis=1), jnp.concatenate(ctx_rot, axis=1)], axis=0
    )
    pieces = rank // ROPE
    low = (lat + ctx) // pieces
    keys = jnp.concatenate(
        [keys[i * low : (i + 1) * low] for i in range(pieces)], axis=1
    ).astype(jnp.bfloat16)
    kv_ref[: lat + ctx] = jnp.concatenate([lat_kv, ctx_kv], axis=0)
    kv_ref[lat + ctx :] = keys


def norm_query_kernel(own_ref, other_ref, gain_ref, kv_ref, near_ref):
    size, lat = kv_ref.shape[0], near_ref.shape[0] - kv_ref.shape[0]
    near_ref[:size] = kv_ref[...]
    near_ref[size:] = normed(halves_of(own_ref, other_ref), 0, lat, gain_ref)


def gather_kernel(*refs):
    size = refs[0].shape[0]
    for i, ref in enumerate(refs[:-1]):
        refs[-1][i * size : (i + 1) * size] = ref[...]


def unpack(chunks, kv_ref, key_ref, lat, ctx):
    count = lat + ctx
    rank = kv_ref.shape[1]
    row = lax.broadcasted_iota(jnp.int32, (count, 128 - ROPE), 0)
    lane = lax.broadcasted_iota(jnp.int32, (count, 128 - ROPE), 1)
    flags = jnp.where((row >= lat) & (lane < 3), 1.0, 0.0)
    for i, (ref, at) in enumerate(chunks):
        kv_ref[i * count : (i + 1) * count] = ref[at : at + count]
        low = count * ROPE // rank
        packed = ref[at + count : at + count + low].astype(jnp.float32)
        rot = [packed[:, j * ROPE : (j + 1) * ROPE] for j in range(rank // ROPE)]
        rot = jnp.concatenate([jnp.concatenate(rot, axis=0), flags], axis=1)
        key_ref[i * count : (i + 1) * count] = rot.astype(jnp.bfloat16)


def expanded(kv_ref, w_ref, head):
    weight = w_ref[:, head * (NOPE + DV) : (head + 1) * (NOPE + DV)]
    return jnp.dot(kv_ref[...], weight, preferred_element_type=jnp.float32).astype(jnp.bfloat16)


def weighted(score, values):
    peak = jnp.max(score, axis=1, keepdims=True)
    probs = jnp.exp2((score - peak) * ((NOPE + ROPE) ** -0.5 * LOG2E))
    total = jnp.sum(probs, axis=1, keepdims=True)
    summed = jnp.dot(probs.astype(jnp.bfloat16), values, preferred_element_type=jnp.float32)
    return peak, total, summed


def staged(steps):
    score = steps[0][0]()
    for i, (unused, finish) in enumerate(steps):
        after = steps[i + 1][0]() if i + 1 < len(steps) else None
        finish(score)
        score = after


def near_kernel(tab_ref, lift_ref, wq_ref, wkv_ref, *refs, lat, ctx, chips):
    own_refs, other_refs = refs[:chips], refs[chips : 2 * chips]
    query_ref, stat_ref, sum_ref, cq_ref, kv_ref, key_ref = refs[-6:]
    size = own_refs[0].shape[0]
    unused, here, side, unused = place()
    for hop in range(chips):
        own, other = own_refs[hop][size - lat :], other_refs[hop][size - lat :]
        at = pl.multiple_of(2 * (here ^ hop) * lat, 16)
        cq_ref[pl.ds(at, lat)] = jnp.where(side == 0, own, other)
        cq_ref[pl.ds(at + lat, lat)] = jnp.where(side == 0, other, own)
    chunks = [(ref, 0) for ref in own_refs + other_refs]
    chunks += chunks_of(refs[2 * chips : -6], size - lat)
    unpack(chunks, kv_ref, key_ref, lat, ctx)
    heads = wq_ref.shape[0]
    quarter = ROPE // 4
    lane = lax.broadcasted_iota(jnp.int32, (1, 2 * ROPE), 1)

    def prepare(head):
        pieces = [wq_ref[head]]
        for block in (1, 0, 3, 2):
            pieces.append(wq_ref[head, NOPE + block * quarter : NOPE + (block + 1) * quarter])
        raw = dot_t(cq_ref[...], jnp.concatenate(pieces, axis=0))
        turned = raw[:, NOPE:] * tab_ref[...]
        turned = turned + pltpu.roll(turned, ROPE, 1)
        lift = lift_ref[head : head + 1] * (NOPE + ROPE) ** 0.5
        first = lift.astype(jnp.bfloat16).astype(jnp.float32)
        second = (lift - first).astype(jnp.bfloat16).astype(jnp.float32)
        third = lift - first - second
        lifts = jnp.where(lane == ROPE, first, jnp.where(lane == ROPE + 1, second, third))
        lifts = jnp.where(lane < ROPE + 3, lifts, 0.0)
        turned = jnp.where(lane < ROPE, turned, lifts)
        query = jnp.concatenate([raw[:, :NOPE], turned], axis=1).astype(jnp.bfloat16)
        query_ref[head] = query

    stats = {}

    def step(head):
        def score():
            prepare(head)
            stats[head] = expanded(kv_ref, wkv_ref, head)
            keys = jnp.concatenate([stats[head][:, :NOPE], key_ref[...]], axis=1)
            return dot_t(query_ref[head], keys)

        def finish(values):
            peak, total, summed = weighted(values, stats[head][:, NOPE:])
            stat_ref[:, head : head + 1] = peak
            stat_ref[:, heads + head : heads + head + 1] = total
            sum_ref[head] = summed

        return score, finish

    staged([step(head) for head in range(heads)])


def chunks_of(refs, step):
    return [(ref, at) for ref in refs for at in range(0, refs[0].shape[0], step)]


def expand_kernel(w_ref, *refs, lat, ctx):
    key_ref, value_ref, kv_ref, rot_ref = refs[-4:]
    step = lat + ctx + (lat + ctx) * ROPE // w_ref.shape[0]
    unpack(chunks_of(refs[:-4], step), kv_ref, rot_ref, lat, ctx)
    for head in range(key_ref.shape[0]):
        pairs = expanded(kv_ref, w_ref, head)
        key_ref[head, :, :NOPE] = pairs[:, :NOPE]
        key_ref[head, :, NOPE:] = rot_ref[...]
        value_ref[head] = pairs[:, NOPE:]


def far_kernel(query_ref, stat_ref, sum_ref, key_ref, value_ref, w_ref, *refs, lat, ctx):
    up_ref, out_ref, up_out_ref, kv_ref, rot_ref, done = refs[-6:]
    copy = pltpu.make_async_copy(up_ref, up_out_ref, done)
    copy.start()
    step = lat + ctx + (lat + ctx) * ROPE // w_ref.shape[0]
    unpack(chunks_of(refs[:-6], step), kv_ref, rot_ref, lat, ctx)
    heads = query_ref.shape[0]
    factor = (NOPE + ROPE) ** -0.5 * LOG2E
    held = {}

    def step_of(head):
        def score():
            pairs = expanded(kv_ref, w_ref, head)
            keys = jnp.concatenate([pairs[:, :NOPE], rot_ref[...]], axis=1)
            held[head] = (keys, pairs[:, NOPE:])
            query = query_ref[head]
            return dot_t(query, key_ref[head]), dot_t(query, held[head][0])

        def finish(scores):
            near = stat_ref[:, head : head + 1]
            top = near
            for values in scores:
                top = jnp.maximum(top, jnp.max(values, axis=1, keepdims=True))
            old = jnp.exp2((near - top) * factor)
            total = stat_ref[:, heads + head : heads + head + 1] * old
            summed = sum_ref[head] * old
            for values, weights in zip(scores, (value_ref[head], held[head][1]), strict=True):
                probs = jnp.exp2((values - top) * factor)
                total = total + jnp.sum(probs, axis=1, keepdims=True)
                summed = summed + jnp.dot(
                    probs.astype(jnp.bfloat16), weights, preferred_element_type=jnp.float32
                )
            out_ref[:, head * DV : (head + 1) * DV] = (summed / total).astype(jnp.bfloat16)

        return score, finish

    staged([step_of(head) for head in range(heads)])
    copy.wait()


def share_out_kernel(w_ref, out_ref):
    chips, unused, features = out_ref.shape
    unused, here, side, unused = place()
    for hop in range(chips):
        start = pl.multiple_of((2 * (here ^ hop) + 1 - side) * features, features)
        out_ref[hop] = w_ref[:, pl.ds(start, features)]


def output_own_kernel(heads_ref, w_ref, out_ref):
    chips, unused, features = out_ref.shape
    unused, here, side, unused = place()
    for hop in range(chips):
        start = pl.multiple_of((2 * (here ^ hop) + side) * features, features)
        out_ref[hop] = jnp.dot(
            heads_ref[...], w_ref[:, pl.ds(start, features)], preferred_element_type=jnp.float32
        )


def output_kernel(heads_ref, w_ref, acc_ref, *out_refs):
    for hop in reversed(range(len(out_refs))):
        acc = acc_ref[hop] + jnp.dot(
            heads_ref[...], w_ref[hop], preferred_element_type=jnp.float32
        )
        out_refs[hop][...] = acc.astype(out_refs[hop].dtype)


def mix_kernel(latent_ref, gate_ref, *refs):
    branch = refs[0][...]
    for ref in refs[1:-1]:
        branch = branch + ref[...].astype(jnp.float32)
    refs[-1][...] = (latent_ref[...].astype(jnp.float32) + gate_ref[...] * branch).astype(
        jnp.bfloat16
    )


def split_device(
    latent,
    context,
    cond,
    cond_ctx,
    w_mod,
    g_norm,
    w_dq,
    w_dkv,
    w_kr,
    g_cq,
    g_ckv,
    w_uq,
    w_ukv,
    ctx_lift,
    w_out,
):
    f32, bf16 = jnp.float32, jnp.bfloat16
    sp, tp = lax.axis_size("sp"), lax.axis_size("tp")
    chips = tp // 2
    rows, features = latent.shape
    ctx_rows = context.shape[0]
    heads = w_uq.shape[1]
    rank = w_dq.shape[1]
    lat, ctx = rows // tp, ctx_rows // tp
    half = rank // 2
    across = [(i, i ^ 1) for i in range(tp)]

    def array(shape, dtype=bf16):
        return jax.ShapeDtypeStruct(shape, dtype)

    def hopped(value):
        return [value] + [
            lax.ppermute(value, "tp", [(i, i ^ (2 * hop)) for i in range(tp)])
            for hop in range(1, chips)
        ]

    share = array((features + ROPE // 2 * features // rank, rank))
    modulation, tokens, w_own, w_other = call(
        functools.partial(stats_kernel, sp=sp),
        (
            array((2 * sp, 1, 5 * features), f32),
            array((rows + ctx_rows, features)),
            share,
            share,
        ),
        latent,
        context,
        cond,
        cond_ctx,
        jnp.transpose(w_mod, (1, 0, 2)),
        g_norm,
        w_dq,
        w_dkv,
        w_kr.T,
        held=pltpu.HBM,
    )
    w_other = lax.ppermute(w_other, "tp", across)
    tokens_other = lax.ppermute(tokens, "tp", across)
    columns = [[s * tp + 2 * c + k for s in range(sp) for k in range(2)] for c in range(chips)]
    modulation = lax.all_to_all(modulation, ("sp", "tp"), 0, 0, axis_index_groups=columns)
    squares = call(square_kernel, array((8, rows + ctx_rows), f32), tokens, tokens_other)
    squares = hopped(squares)

    q_part = array((2, half // 128 * lat, 128), f32)
    kv_part = array((2, half // 128 * (lat + ctx) + (lat + ctx) // 4, 128), f32)
    *parts, gate = call(
        functools.partial(project_kernel, sp=sp, tp=tp, rows=rows),
        (kv_part,) * chips + (q_part,) * chips + (array((1, features), f32),),
        tokens,
        tokens_other,
        modulation,
        w_own,
        w_other,
        *squares,
        scratch=[
            pltpu.VMEM((rows, rank), f32),
            pltpu.VMEM((ctx_rows, half), f32),
            pltpu.VMEM((rows, ROPE // 2), f32),
            pltpu.VMEM((ctx_rows, ROPE // 2), f32),
        ],
        flops=4 * (rows + ctx_rows) * features * (rank + 128),
        limit=16,
    )
    *parts, w_kv, w_up, zero = lax.optimization_barrier((*parts, w_ukv, w_out, jnp.float32(0)))

    def collected(parts):
        return [parts[0]] + [
            lax.ppermute(part, "tp", [(i, i ^ (2 * hop + 2)) for i in range(tp)])
            for hop, part in enumerate(parts[1:])
        ]

    def reduced(parts):
        shape = array(parts[0].shape[1:], f32)
        own, other = call(reduce_kernel, (shape, shape), *parts)
        return own, lax.ppermute(other, "tp", across)

    kv_parts = collected(parts[:chips])
    q_parts = collected(parts[chips:])

    quarter = ROPE // 4
    inverse = THETA ** (-np.arange(quarter) / quarter)
    inverse = jnp.asarray(np.tile(inverse, 128 // quarter)[None], f32) + zero
    q_tab = call(tables_kernel, array((rows, 128), f32), inverse, flops=1e9)
    w_kv = call(relay_kernel, array((rank, heads * (NOPE + DV))), w_kv, flops=1e9)
    w_up = w_up.reshape(heads * DV, 2 * chips * features)
    w_up_other = call(
        share_out_kernel, array((chips, heads * DV, features)), w_up, flops=1e9, kept=False
    )
    w_up_other = lax.ppermute(w_up_other, "tp", across)
    count = lat + ctx
    step = count + count * ROPE // rank
    kv = call(
        functools.partial(norm_kernel, lat=lat, ctx=ctx),
        array((step, rank)),
        *reduced(kv_parts),
        g_ckv[None],
        q_tab,
    )
    *q_parts, w_up_other = lax.optimization_barrier((*q_parts, w_up_other))

    even = sp & (sp - 1) == 0
    planes = [
        lax.ppermute(kv, "sp", [(i, i ^ hop if even else (i + hop) % sp) for i in range(sp)])
        for hop in range(1, sp)
    ]
    near = call(norm_query_kernel, array((step + lat, rank)), *reduced(q_parts), g_cq[None], kv)
    near_own = hopped(near)
    near_other = [lax.ppermute(n, "tp", across) for n in near_own]
    far = call(gather_kernel, array(((sp - 1) * step, rank)), *planes)
    far_own = hopped(far)
    far_other = [lax.ppermute(f, "tp", across) for f in far_own]

    keys = (tp + 2 * (sp - 1)) * count
    query, stats, summed = call(
        functools.partial(near_kernel, lat=lat, ctx=ctx, chips=chips),
        (
            array((heads, rows, 2 * NOPE)),
            array((rows, 128), f32),
            array((heads, rows, DV), f32),
        ),
        q_tab,
        jnp.broadcast_to(ctx_lift[:, None], (heads, 128)),
        jnp.transpose(w_uq, (1, 2, 0)),
        w_kv,
        *near_own,
        *near_other,
        far_own[0],
        far_other[0],
        scratch=[
            pltpu.VMEM((rows, rank), bf16),
            pltpu.VMEM((keys, rank), bf16),
            pltpu.VMEM((keys, 128), bf16),
        ],
        flops=heads * rows * (2 * rank * 256 + 2 * keys * 384),
        limit=16,
    )
    keys = (chips - 1) * (sp - 1) * count
    scratch = [pltpu.VMEM((keys, rank), bf16), pltpu.VMEM((keys, 128), bf16)]
    far_keys, far_values = call(
        functools.partial(expand_kernel, lat=lat, ctx=ctx),
        (array((heads, keys, 2 * NOPE)), array((heads, keys, DV))),
        w_kv,
        *far_own[1:],
        scratch=scratch,
        flops=2 * keys * rank * 256 * heads,
    )
    heads_out, w_up_other = call(
        functools.partial(far_kernel, lat=lat, ctx=ctx),
        (array((rows, heads * DV)), array(w_up_other.shape)),
        query,
        stats,
        summed,
        far_keys,
        far_values,
        w_kv,
        *far_other[1:],
        remote=(w_up_other,),
        scratch=scratch + [pltpu.SemaphoreType.DMA],
        flops=2 * heads * keys * (2 * rows * 384 + rank * 256),
        limit=28,
    )

    heads_other = lax.ppermute(heads_out, "tp", across)
    flops = 2 * rows * heads * DV * chips * features
    branch = call(
        output_own_kernel, array((chips, rows, features), f32), heads_out, w_up, flops=flops
    )
    block = array((rows, features))
    branch, *apart = call(
        output_kernel,
        (array((rows, features), f32),) + (block,) * (chips - 1),
        heads_other,
        w_up_other,
        branch,
        flops=flops,
    )
    apart = [
        lax.ppermute(a, "tp", [(i, i ^ (2 * hop + 2)) for i in range(tp)])
        for hop, a in enumerate(apart)
    ]
    return call(mix_kernel, array(latent.shape), latent, gate, branch, *apart, kept=False)


def chosen(*arrays):
    rows, ctx_rows, features = arrays[0].shape[0], arrays[1].shape[0], arrays[0].shape[1]
    tp = lax.axis_size("tp")
    aligned = rows % (16 * tp) == 0 and ctx_rows % (16 * tp) == 0 and features % 128 == 0 and arrays[6].shape[1] % features == 0
    return (split_device if tp in (2, 4, 8, 16) and aligned else plain_device)(*arrays)


def solution(mesh):
    return jax.shard_map(
        chosen,
        mesh=mesh,
        in_specs=(
            P("sp", "tp"),
            P("sp", "tp"),
            P("sp"),
            P("sp"),
            P("sp", None, "tp"),
            P("tp"),
            P("tp", None),
            P("tp", None),
            P("tp", None),
            P(),
            P(),
            P(None, "tp", None),
            P(None, "tp", None),
            P("tp"),
            P("tp", None, None),
        ),
        out_specs=P("sp", "tp"),
        check_vma=False,
    )
```

```python
import functools

import jax
import jax.numpy as jnp
import numpy as np
from jax import lax
from jax.experimental import pallas as pl
from jax.experimental.pallas import tpu as pltpu
from jax.sharding import PartitionSpec as P

D = 2048
NOPE = 128
ROPE = 64
DV = 128
GRID_W = 64


EPS = 1e-06
THETA = 10000.0
LOG2E = 1.4426950408889634


def tables(positions):
    row = (positions // GRID_W).astype(jnp.float32)
    col = (positions % GRID_W).astype(jnp.float32)
    half = ROPE // 2
    inverse = 1.0 / THETA ** (jnp.arange(0, half, 2, dtype=jnp.float32) / half)
    angle = jnp.concatenate([row[:, None] * inverse, col[:, None] * inverse], axis=-1)
    return (jnp.cos(angle), jnp.sin(angle))


def rotate(values, cosine, sine):
    shape = values.shape
    quarter = ROPE // 4
    parts = values.reshape(shape[:-1] + (2, 2, quarter))
    extra = (1,) * (len(shape) - 2)
    cosine = cosine.reshape((shape[0],) + extra + (2, quarter))
    sine = sine.reshape((shape[0],) + extra + (2, quarter))
    front_section = parts[..., 0, :]
    second = parts[..., 1, :]
    turned = jnp.stack(
        [front_section * cosine - second * sine, front_section * sine + second * cosine], axis=-2
    )
    return turned.reshape(shape)


def modulated(values, sumsq, gain, modulation):
    scaled = values * lax.rsqrt(sumsq / D + EPS)[:, None] * gain
    return (scaled * (1.0 + modulation[1]) + modulation[0]).astype(jnp.bfloat16)


def low_norm(values, gain):
    scale = lax.rsqrt(jnp.mean(values * values, axis=-1, keepdims=True) + EPS)
    return (values * scale * gain).astype(jnp.bfloat16)


def plain_device(
    latent,
    context,
    cond,
    cond_ctx,
    w_mod,
    g_norm,
    w_dq,
    w_dkv,
    w_kr,
    g_cq,
    g_ckv,
    w_uq,
    w_ukv,
    ctx_lift,
    w_out,
):
    rows = latent.shape[0]
    device_attention_groups = w_uq.shape[1]
    signal = jnp.stack(
        [jax.nn.silu(cond.astype(jnp.float32)), jax.nn.silu(cond_ctx.astype(jnp.float32))]
    ).astype(jnp.bfloat16)
    partial_mod = jnp.dot(
        signal, w_mod.reshape(w_mod.shape[0], -1), preferred_element_type=jnp.float32
    )
    modulation = lax.psum(partial_mod.reshape(2, 3, -1), "sp")
    lat_f = latent.astype(jnp.float32)
    ctx_f = context.astype(jnp.float32)
    lat_sq, ctx_sq = lax.psum(
        (jnp.sum(lat_f * lat_f, axis=1), jnp.sum(ctx_f * ctx_f, axis=1)), "tp"
    )
    lat_h = modulated(lat_f, lat_sq, g_norm, modulation[0])
    ctx_h = modulated(ctx_f, ctx_sq, g_norm, modulation[1])
    positions = lax.axis_index("sp") * rows + jnp.arange(rows, dtype=jnp.int32)
    cosine, sine = tables(positions)
    lat_q, lat_kv, lat_rot, ctx_kv, ctx_rot = lax.psum(
        (
            jnp.dot(lat_h, w_dq, preferred_element_type=jnp.float32),
            jnp.dot(lat_h, w_dkv, preferred_element_type=jnp.float32),
            jnp.dot(lat_h, w_kr, preferred_element_type=jnp.float32),
            jnp.dot(ctx_h, w_dkv, preferred_element_type=jnp.float32),
            jnp.dot(ctx_h, w_kr, preferred_element_type=jnp.float32),
        ),
        "tp",
    )
    cq_n = low_norm(lat_q, g_cq)
    ckv_n = low_norm(lat_kv, g_ckv)
    lat_kr = rotate(lat_rot, cosine, sine).astype(jnp.bfloat16)
    ctx_ckv_n = low_norm(ctx_kv, g_ckv)
    ctx_kr = ctx_rot.astype(jnp.bfloat16)
    query = jnp.dot(cq_n, w_uq.reshape(w_uq.shape[0], -1), preferred_element_type=jnp.float32)
    query = query.reshape(rows, device_attention_groups, NOPE + ROPE)
    query = jnp.concatenate(
        [query[..., :NOPE], rotate(query[..., NOPE:], cosine, sine)], axis=-1
    ).astype(jnp.bfloat16)
    up_weight = w_ukv.reshape(w_ukv.shape[0], -1)
    scale = (NOPE + ROPE) ** (-0.5)

    def expand(compressed):
        return jnp.dot(compressed, up_weight, preferred_element_type=jnp.float32).astype(
            jnp.bfloat16
        )

    def unpack(front_section):
        return expand(front_section).reshape(
            front_section.shape[0], device_attention_groups, NOPE + DV
        )

    def merged_question_vector(
        cumulative_loop_values, front_section, spinning_section, affinity_offset
    ):
        peak, total, accum = cumulative_loop_values
        pairs = unpack(front_section)
        count = pairs.shape[0]
        keys = jnp.concatenate(
            [
                pairs[..., :NOPE],
                jnp.broadcast_to(
                    spinning_section[:, None, :], (count, device_attention_groups, ROPE)
                ),
            ],
            axis=-1,
        )
        raw_affinity_matrix = (
            jnp.einsum("qhd,khd->hqk", query, keys, preferred_element_type=jnp.float32) * scale
        )
        raw_affinity_matrix = raw_affinity_matrix + affinity_offset[:, None, None]
        fresh = jnp.maximum(peak, jnp.max(raw_affinity_matrix, axis=-1))
        probs = jnp.exp(raw_affinity_matrix - fresh[..., None])
        fade = jnp.exp(peak - fresh)
        total = total * fade + jnp.sum(probs, axis=-1)
        accum = accum * fade[..., None] + jnp.einsum(
            "hqk,khd->hqd",
            probs.astype(jnp.bfloat16),
            pairs[..., NOPE:],
            preferred_element_type=jnp.float32,
        )
        return (fresh, total, accum)

    blank_offset_matrix = jnp.zeros((device_attention_groups,), jnp.float32)
    start_carry = (
        jnp.full((device_attention_groups, rows), -1e30, jnp.float32),
        jnp.zeros((device_attention_groups, rows), jnp.float32),
        jnp.zeros((device_attention_groups, rows, DV), jnp.float32),
    )
    ctx_all_first, ctx_all_kr = (
        lax.all_gather(ctx_ckv_n, "sp", axis=0, tiled=True),
        lax.all_gather(ctx_kr, "sp", axis=0, tiled=True),
    )
    cumulative_loop_values = merged_question_vector(
        start_carry, ctx_all_first, ctx_all_kr, ctx_lift
    )
    fold_cumulative_loop_values = cumulative_loop_values
    front_section = lax.all_gather(ckv_n, "sp", axis=0, tiled=True)
    spinning_section = lax.all_gather(lat_kr, "sp", axis=0, tiled=True)
    count = front_section.shape[0] // rows
    blocks = (
        front_section.reshape(count, rows, front_section.shape[1]),
        spinning_section.reshape(count, rows, spinning_section.shape[1]),
    )

    def step(normalizer_statistics, segment_window):
        return (
            merged_question_vector(
                normalizer_statistics, segment_window[0], segment_window[1], blank_offset_matrix
            ),
            None,
        )

    fold_cumulative_loop_values, _ = lax.scan(step, fold_cumulative_loop_values, blocks)
    cumulative_loop_values = fold_cumulative_loop_values
    _, total, accum = cumulative_loop_values
    heads_out = (accum / total[..., None]).astype(jnp.bfloat16)
    branch = jnp.einsum("hqd,hde->qe", heads_out, w_out, preferred_element_type=jnp.float32)
    branch = lax.psum_scatter(
        branch.astype(jnp.bfloat16), "tp", scatter_dimension=1, tiled=True
    ).astype(jnp.float32)
    return (lat_f + modulation[0, 2] * branch).astype(jnp.bfloat16)


def call(kernel, outs, *args, flops=1e6, scratch=(), limit=8, held=pltpu.VMEM, kept=True, remote=()):
    single = not isinstance(outs, tuple)
    vmem = pl.BlockSpec(memory_space=pltpu.VMEM)
    outs = (outs,) if single else outs
    if kept:
        outs = tuple(pltpu.VMEM(o.shape, o.dtype) for o in outs)
    if held is not None:
        args = tuple(pltpu.with_memory_space_constraint(a, held) for a in args)
    result = pl.pallas_call(
        kernel,
        in_specs=[vmem] * len(args) + [pl.BlockSpec(memory_space=pltpu.HBM)] * len(remote),
        out_specs=(vmem,) * len(outs),
        out_shape=outs,
        scratch_shapes=scratch,
        cost_estimate=pl.CostEstimate(
            flops=int(flops), bytes_accessed=int(1e5), transcendentals=0
        ),
        compiler_params=pltpu.CompilerParams(vmem_limit_bytes=limit << 20),
    )(*args, *remote)
    return result[0] if single else result


def place():
    me = lax.axis_index("tp")
    return lax.axis_index("sp") * lax.axis_size("tp"), me // 2, lax.rem(me, 2), me


def dot_t(left, right, **options):
    return lax.dot_general(
        left, right, (((1,), (1,)), ((), ())), preferred_element_type=jnp.float32, **options
    )


def stats_kernel(
    lat_ref,
    ctx_ref,
    cond_ref,
    cond_ctx_ref,
    w_ref,
    g_ref,
    wq_ref,
    wkv_ref,
    wr_ref,
    out_ref,
    rows_ref,
    own_ref,
    other_ref,
    *,
    sp,
):
    rows_ref[: lat_ref.shape[0]] = lat_ref[...]
    rows_ref[lat_ref.shape[0] :] = ctx_ref[...]
    features, rank = wq_ref.shape
    half, width = rank // 2, ROPE // 2
    side = place()[2]
    for which, ref in ((side, own_ref), (1 - side, other_ref)):
        start = pl.multiple_of(which * half, half)
        ref[:features, :half] = wq_ref[:, pl.ds(start, half)]
        ref[:features, half:] = wkv_ref[:, pl.ds(start, half)]
        rot = wr_ref[pl.ds(pl.multiple_of(which * width, width), width), :]
        count = width * features // rank
        for i in range(rank // features):
            ref[features:, i * features : (i + 1) * features] = rot[i * count : (i + 1) * count]
    inner = cond_ref.shape[0]
    lat_c = jax.nn.silu(cond_ref[...].astype(jnp.float32).reshape(1, inner))
    ctx_c = jax.nn.silu(cond_ctx_ref[...].astype(jnp.float32).reshape(1, inner))
    row = lax.broadcasted_iota(jnp.int32, (16, inner), 0)
    signal = jnp.where(row < 8, lat_c, ctx_c).astype(jnp.bfloat16)
    parts = [jnp.dot(signal, w_ref[j], preferred_element_type=jnp.float32) for j in range(3)]
    gain = g_ref[...].reshape(1, g_ref.shape[0])
    gains = parts[1] * gain + gain * (1.0 / sp)
    modulation = jnp.concatenate(
        [parts[0][:1], gains[:1], parts[0][8:9], gains[8:9], parts[2][:1]], axis=1
    )
    for d in range(out_ref.shape[0]):
        out_ref[d] = modulation


def square_kernel(own_ref, other_ref, out_ref):
    ones = jnp.ones((8, own_ref.shape[1]), jnp.float32)
    total = None
    for ref in (own_ref, other_ref):
        values = ref[...].astype(jnp.float32)
        term = dot_t(ones, values * values, precision=lax.Precision.HIGHEST)
        total = term if total is None else total + term
    out_ref[...] = total


def project_kernel(
    own_ref, other_ref, mod_ref, w_own_ref, w_other_ref, *refs, sp, tp, rows
):
    chips = tp // 2
    squares, kv_refs, q_refs = refs[:chips], refs[chips : 2 * chips], refs[2 * chips : 3 * chips]
    gate_ref, lat_ref, ctx_ref, lat_rot_ref, ctx_rot_ref = refs[3 * chips :]
    count, features = own_ref.shape
    ctx_rows = count - rows
    rank = w_own_ref.shape[1]
    half = rank // 2
    unused, here, side, unused = place()
    total = squares[0][...]
    for ref in squares[1:]:
        total = total + ref[...]
    total = jnp.transpose(total)[:, :1]
    mine, partner = mod_ref[side], mod_ref[1 - side]
    for s in range(1, sp):
        mine = mine + mod_ref[2 * s + side]
        partner = partner + mod_ref[2 * s + 1 - side]
    gate_ref[...] = mine[:, 4 * features :]

    def split(ref):
        packed = ref[features:]
        rot = [packed[:, i * features : (i + 1) * features] for i in range(rank // features)]
        return ref[:features, :half], ref[:features, half:], jnp.concatenate(rot, axis=0)

    w_own, w_other = split(w_own_ref), split(w_other_ref)

    def rows_of(part, kind):
        own, other = own_ref[part].astype(jnp.float32), other_ref[part].astype(jnp.float32)
        inverse = lax.rsqrt(total[part] / D + EPS)
        first = second = rot = None
        for values, vectors, weights in ((own, mine, w_own), (other, partner, w_other)):
            shift = vectors[:, 2 * kind * features : (2 * kind + 1) * features]
            gain = vectors[:, (2 * kind + 1) * features : (2 * kind + 2) * features]
            h = (values * inverse * gain + shift).astype(jnp.bfloat16)
            terms = [None if kind else jnp.dot(h, weights[0], preferred_element_type=jnp.float32)]
            terms.append(jnp.dot(h, weights[1], preferred_element_type=jnp.float32))
            terms.append(dot_t(h, weights[2]))
            if second is None:
                first, second, rot = terms
            else:
                first = None if kind else first + terms[0]
                second, rot = second + terms[1], rot + terms[2]
        return first, second, rot

    lat_q, lat_kv, lat_rot = rows_of(slice(0, rows), 0)
    lat_ref[:, :half], lat_ref[:, half:], lat_rot_ref[...] = lat_q, lat_kv, lat_rot
    unused, ctx_ref[...], ctx_rot_ref[...] = rows_of(slice(rows, count), 1)
    lat, ctx = rows // tp, ctx_rows // tp
    quarter = (lat + ctx) // 4
    for hop in range(chips):
        for core in range(2):
            d = 2 * (here ^ hop) + core
            lats, ctxs = pl.ds(pl.multiple_of(d * lat, 8), lat), pl.ds(pl.multiple_of(d * ctx, 8), ctx)
            for slab in range(half // 128):
                q_refs[hop][core, slab * lat : (slab + 1) * lat, :] = lat_ref[
                    lats, slab * 128 : (slab + 1) * 128
                ]
            at = 0
            for source, part, first, size in (
                (lat_ref, lats, half, lat),
                (ctx_ref, ctxs, 0, ctx),
            ):
                for column in range(first, source.shape[1], 128):
                    kv_refs[hop][core, at : at + size, :] = source[part, column : column + 128]
                    at += size
            rot = jnp.concatenate([lat_rot_ref[lats], ctx_rot_ref[ctxs]], axis=0)
            kv_refs[hop][core, at : at + quarter, :] = jnp.concatenate(
                [rot[i * quarter : (i + 1) * quarter] for i in range(4)], axis=1
            )


def reduce_kernel(*refs):
    own_ref, other_ref = refs[-2:]
    side = place()[2]
    for which, ref in ((side, own_ref), (1 - side, other_ref)):
        total = refs[0][which]
        for part in refs[1:-2]:
            total = total + part[which]
        ref[...] = total


def tables_kernel(inverse_ref, tab_ref):
    rows, lanes = tab_ref.shape
    position = lax.broadcasted_iota(jnp.int32, (rows, lanes), 0) + lax.axis_index("sp") * rows
    lane = lax.broadcasted_iota(jnp.int32, (rows, lanes), 1)
    along = jnp.where(lane % ROPE < ROPE // 2, position // GRID_W, position % GRID_W)
    angle = along.astype(jnp.float32) * inverse_ref[...]
    sine = jnp.sin(angle)
    sine = jnp.where(lane % (ROPE // 2) < ROPE // 4, -sine, sine)
    tab_ref[...] = jnp.where(lane < ROPE, jnp.cos(angle), sine)


def relay_kernel(w_ref, out_ref):
    width = w_ref.shape[2]
    for head in range(w_ref.shape[1]):
        out_ref[:, head * width : (head + 1) * width] = w_ref[:, head, :]


def halves_of(own_ref, other_ref):
    first = place()[2] == 0
    own, other = own_ref[...], other_ref[...]
    return [jnp.where(first, own, other), jnp.where(first, other, own)]


def normed(halves, start, count, gain_ref):
    slabs = gain_ref.shape[1] // 256
    values = jnp.concatenate(
        [
            half[start + i * count : start + (i + 1) * count]
            for half in halves
            for i in range(slabs)
        ],
        axis=1,
    )
    factor = lax.rsqrt(jnp.mean(values * values, axis=1, keepdims=True) + EPS)
    return (values * factor * gain_ref[...]).astype(jnp.bfloat16)


def norm_kernel(own_ref, other_ref, gain_ref, tab_ref, kv_ref, *, lat, ctx):
    me = place()[3]
    tab = tab_ref[pl.ds(pl.multiple_of(me * lat, 8), lat), :]
    halves = halves_of(own_ref, other_ref)
    rank = gain_ref.shape[1]
    slabs = rank // 256
    lat_kv = normed(halves, 0, lat, gain_ref)
    at = slabs * lat
    ctx_kv = normed(halves, at, ctx, gain_ref)
    at += slabs * ctx
    quarter = (lat + ctx) // 4
    width = ROPE // 2
    lat_rot, ctx_rot = [], []
    for core in range(2):
        packed = halves[core][at : at + quarter]
        rot = jnp.concatenate(
            [packed[:, i * width : (i + 1) * width] for i in range(4)], axis=0
        )
        turned = rot[:lat]
        swapped = jnp.concatenate([turned[:, width // 2 :], turned[:, : width // 2]], axis=1)
        cosine = tab[:, core * width : (core + 1) * width]
        sine = tab[:, ROPE + core * width : ROPE + (core + 1) * width]
        lat_rot.append(turned * cosine + swapped * sine)
        ctx_rot.append(rot[lat:])
    keys = jnp.concatenate(
        [jnp.concatenate(lat_rot, axis=1), jnp.concatenate(ctx_rot, axis=1)], axis=0
    )
    pieces = rank // ROPE
    low = (lat + ctx) // pieces
    keys = jnp.concatenate(
        [keys[i * low : (i + 1) * low] for i in range(pieces)], axis=1
    ).astype(jnp.bfloat16)
    kv_ref[: lat + ctx] = jnp.concatenate([lat_kv, ctx_kv], axis=0)
    kv_ref[lat + ctx :] = keys


def norm_query_kernel(own_ref, other_ref, gain_ref, kv_ref, near_ref):
    size, lat = kv_ref.shape[0], near_ref.shape[0] - kv_ref.shape[0]
    near_ref[:size] = kv_ref[...]
    near_ref[size:] = normed(halves_of(own_ref, other_ref), 0, lat, gain_ref)


def gather_kernel(*refs):
    size = refs[0].shape[0]
    for i, ref in enumerate(refs[:-1]):
        refs[-1][i * size : (i + 1) * size] = ref[...]


def unpack(chunks, kv_ref, key_ref, lat, ctx):
    count = lat + ctx
    rank = kv_ref.shape[1]
    row = lax.broadcasted_iota(jnp.int32, (count, 128 - ROPE), 0)
    lane = lax.broadcasted_iota(jnp.int32, (count, 128 - ROPE), 1)
    flags = jnp.where((row >= lat) & (lane < 3), 1.0, 0.0)
    for i, (ref, at) in enumerate(chunks):
        kv_ref[i * count : (i + 1) * count] = ref[at : at + count]
        low = count * ROPE // rank
        packed = ref[at + count : at + count + low].astype(jnp.float32)
        rot = [packed[:, j * ROPE : (j + 1) * ROPE] for j in range(rank // ROPE)]
        rot = jnp.concatenate([jnp.concatenate(rot, axis=0), flags], axis=1)
        key_ref[i * count : (i + 1) * count] = rot.astype(jnp.bfloat16)


def expanded(kv_ref, w_ref, head):
    weight = w_ref[:, head * (NOPE + DV) : (head + 1) * (NOPE + DV)]
    return jnp.dot(kv_ref[...], weight, preferred_element_type=jnp.float32).astype(jnp.bfloat16)


def weighted(score, values):
    peak = jnp.max(score, axis=1, keepdims=True)
    probs = jnp.exp2((score - peak) * ((NOPE + ROPE) ** -0.5 * LOG2E))
    total = jnp.sum(probs, axis=1, keepdims=True)
    summed = jnp.dot(probs.astype(jnp.bfloat16), values, preferred_element_type=jnp.float32)
    return peak, total, summed


def staged(steps):
    score = steps[0][0]()
    for i, (unused, finish) in enumerate(steps):
        after = steps[i + 1][0]() if i + 1 < len(steps) else None
        finish(score)
        score = after


def near_kernel(tab_ref, lift_ref, wq_ref, wkv_ref, *refs, lat, ctx, chips):
    own_refs, other_refs = refs[:chips], refs[chips : 2 * chips]
    query_ref, stat_ref, sum_ref, cq_ref, kv_ref, key_ref = refs[-6:]
    size = own_refs[0].shape[0]
    unused, here, side, unused = place()
    for hop in range(chips):
        own, other = own_refs[hop][size - lat :], other_refs[hop][size - lat :]
        at = pl.multiple_of(2 * (here ^ hop) * lat, 16)
        cq_ref[pl.ds(at, lat)] = jnp.where(side == 0, own, other)
        cq_ref[pl.ds(at + lat, lat)] = jnp.where(side == 0, other, own)
    chunks = [(ref, 0) for ref in own_refs + other_refs]
    chunks += chunks_of(refs[2 * chips : -6], size - lat)
    unpack(chunks, kv_ref, key_ref, lat, ctx)
    heads = wq_ref.shape[0]
    quarter = ROPE // 4
    lane = lax.broadcasted_iota(jnp.int32, (1, 2 * ROPE), 1)

    def prepare(head):
        pieces = [wq_ref[head]]
        for block in (1, 0, 3, 2):
            pieces.append(wq_ref[head, NOPE + block * quarter : NOPE + (block + 1) * quarter])
        raw = dot_t(cq_ref[...], jnp.concatenate(pieces, axis=0))
        turned = raw[:, NOPE:] * tab_ref[...]
        turned = turned + pltpu.roll(turned, ROPE, 1)
        lift = lift_ref[head : head + 1] * (NOPE + ROPE) ** 0.5
        first = lift.astype(jnp.bfloat16).astype(jnp.float32)
        second = (lift - first).astype(jnp.bfloat16).astype(jnp.float32)
        third = lift - first - second
        lifts = jnp.where(lane == ROPE, first, jnp.where(lane == ROPE + 1, second, third))
        lifts = jnp.where(lane < ROPE + 3, lifts, 0.0)
        turned = jnp.where(lane < ROPE, turned, lifts)
        query = jnp.concatenate([raw[:, :NOPE], turned], axis=1).astype(jnp.bfloat16)
        query_ref[head] = query

    stats = {}

    def step(head):
        def score():
            prepare(head)
            stats[head] = expanded(kv_ref, wkv_ref, head)
            keys = jnp.concatenate([stats[head][:, :NOPE], key_ref[...]], axis=1)
            return dot_t(query_ref[head], keys)

        def finish(values):
            peak, total, summed = weighted(values, stats[head][:, NOPE:])
            stat_ref[:, head : head + 1] = peak
            stat_ref[:, heads + head : heads + head + 1] = total
            sum_ref[head] = summed

        return score, finish

    staged([step(head) for head in range(heads)])


def chunks_of(refs, step):
    return [(ref, at) for ref in refs for at in range(0, refs[0].shape[0], step)]


def expand_kernel(w_ref, *refs, lat, ctx):
    key_ref, value_ref, kv_ref, rot_ref = refs[-4:]
    step = lat + ctx + (lat + ctx) * ROPE // w_ref.shape[0]
    unpack(chunks_of(refs[:-4], step), kv_ref, rot_ref, lat, ctx)
    for head in range(key_ref.shape[0]):
        pairs = expanded(kv_ref, w_ref, head)
        key_ref[head, :, :NOPE] = pairs[:, :NOPE]
        key_ref[head, :, NOPE:] = rot_ref[...]
        value_ref[head] = pairs[:, NOPE:]


def far_kernel(query_ref, stat_ref, sum_ref, key_ref, value_ref, w_ref, *refs, lat, ctx):
    up_ref, out_ref, up_out_ref, kv_ref, rot_ref, done = refs[-6:]
    copy = pltpu.make_async_copy(up_ref, up_out_ref, done)
    copy.start()
    step = lat + ctx + (lat + ctx) * ROPE // w_ref.shape[0]
    unpack(chunks_of(refs[:-6], step), kv_ref, rot_ref, lat, ctx)
    heads = query_ref.shape[0]
    factor = (NOPE + ROPE) ** -0.5 * LOG2E
    held = {}

    def step_of(head):
        def score():
            pairs = expanded(kv_ref, w_ref, head)
            keys = jnp.concatenate([pairs[:, :NOPE], rot_ref[...]], axis=1)
            keys = jnp.concatenate([key_ref[head], keys], axis=0)
            held[head] = jnp.concatenate([value_ref[head], pairs[:, NOPE:]], axis=0)
            return dot_t(query_ref[head], keys)

        def finish(values):
            near = stat_ref[:, head : head + 1]
            top = jnp.maximum(near, jnp.max(values, axis=1, keepdims=True))
            old = jnp.exp2((near - top) * factor)
            probs = jnp.exp2((values - top) * factor)
            total = stat_ref[:, heads + head : heads + head + 1] * old
            total = total + jnp.sum(probs, axis=1, keepdims=True)
            summed = sum_ref[head] * old + jnp.dot(
                probs.astype(jnp.bfloat16), held[head], preferred_element_type=jnp.float32
            )
            out_ref[:, head * DV : (head + 1) * DV] = (summed / total).astype(jnp.bfloat16)

        return score, finish

    staged([step_of(head) for head in range(heads)])
    copy.wait()


def share_out_kernel(w_ref, out_ref):
    chips, unused, features = out_ref.shape
    unused, here, side, unused = place()
    for hop in range(chips):
        start = pl.multiple_of((2 * (here ^ hop) + 1 - side) * features, features)
        out_ref[hop] = w_ref[:, pl.ds(start, features)]


def output_own_kernel(heads_ref, w_ref, out_ref):
    chips, unused, features = out_ref.shape
    unused, here, side, unused = place()
    for hop in range(chips):
        start = pl.multiple_of((2 * (here ^ hop) + side) * features, features)
        out_ref[hop] = jnp.dot(
            heads_ref[...], w_ref[:, pl.ds(start, features)], preferred_element_type=jnp.float32
        )


def output_kernel(heads_ref, w_ref, acc_ref, *out_refs):
    for hop in reversed(range(len(out_refs))):
        acc = acc_ref[hop] + jnp.dot(
            heads_ref[...], w_ref[hop], preferred_element_type=jnp.float32
        )
        out_refs[hop][...] = acc.astype(out_refs[hop].dtype)


def mix_kernel(latent_ref, gate_ref, *refs):
    branch = refs[0][...]
    for ref in refs[1:-1]:
        branch = branch + ref[...].astype(jnp.float32)
    refs[-1][...] = (latent_ref[...].astype(jnp.float32) + gate_ref[...] * branch).astype(
        jnp.bfloat16
    )


def split_device(
    latent,
    context,
    cond,
    cond_ctx,
    w_mod,
    g_norm,
    w_dq,
    w_dkv,
    w_kr,
    g_cq,
    g_ckv,
    w_uq,
    w_ukv,
    ctx_lift,
    w_out,
):
    f32, bf16 = jnp.float32, jnp.bfloat16
    sp, tp = lax.axis_size("sp"), lax.axis_size("tp")
    chips = tp // 2
    rows, features = latent.shape
    ctx_rows = context.shape[0]
    heads = w_uq.shape[1]
    rank = w_dq.shape[1]
    lat, ctx = rows // tp, ctx_rows // tp
    half = rank // 2
    across = [(i, i ^ 1) for i in range(tp)]

    def array(shape, dtype=bf16):
        return jax.ShapeDtypeStruct(shape, dtype)

    def hopped(value):
        return [value] + [
            lax.ppermute(value, "tp", [(i, i ^ (2 * hop)) for i in range(tp)])
            for hop in range(1, chips)
        ]

    share = array((features + ROPE // 2 * features // rank, rank))
    modulation, tokens, w_own, w_other = call(
        functools.partial(stats_kernel, sp=sp),
        (
            array((2 * sp, 1, 5 * features), f32),
            array((rows + ctx_rows, features)),
            share,
            share,
        ),
        latent,
        context,
        cond,
        cond_ctx,
        jnp.transpose(w_mod, (1, 0, 2)),
        g_norm,
        w_dq,
        w_dkv,
        w_kr.T,
        held=pltpu.HBM,
    )
    w_other = lax.ppermute(w_other, "tp", across)
    tokens_other = lax.ppermute(tokens, "tp", across)
    columns = [[s * tp + 2 * c + k for s in range(sp) for k in range(2)] for c in range(chips)]
    modulation = lax.all_to_all(modulation, ("sp", "tp"), 0, 0, axis_index_groups=columns)
    squares = call(square_kernel, array((8, rows + ctx_rows), f32), tokens, tokens_other)
    squares = hopped(squares)

    q_part = array((2, half // 128 * lat, 128), f32)
    kv_part = array((2, half // 128 * (lat + ctx) + (lat + ctx) // 4, 128), f32)
    *parts, gate = call(
        functools.partial(project_kernel, sp=sp, tp=tp, rows=rows),
        (kv_part,) * chips + (q_part,) * chips + (array((1, features), f32),),
        tokens,
        tokens_other,
        modulation,
        w_own,
        w_other,
        *squares,
        scratch=[
            pltpu.VMEM((rows, rank), f32),
            pltpu.VMEM((ctx_rows, half), f32),
            pltpu.VMEM((rows, ROPE // 2), f32),
            pltpu.VMEM((ctx_rows, ROPE // 2), f32),
        ],
        flops=4 * (rows + ctx_rows) * features * (rank + 128),
        limit=16,
    )
    *parts, w_kv, w_up, zero = lax.optimization_barrier((*parts, w_ukv, w_out, jnp.float32(0)))

    def collected(parts):
        return [parts[0]] + [
            lax.ppermute(part, "tp", [(i, i ^ (2 * hop + 2)) for i in range(tp)])
            for hop, part in enumerate(parts[1:])
        ]

    def reduced(parts):
        shape = array(parts[0].shape[1:], f32)
        own, other = call(reduce_kernel, (shape, shape), *parts)
        return own, lax.ppermute(other, "tp", across)

    kv_parts = collected(parts[:chips])
    q_parts = collected(parts[chips:])

    quarter = ROPE // 4
    inverse = THETA ** (-np.arange(quarter) / quarter)
    inverse = jnp.asarray(np.tile(inverse, 128 // quarter)[None], f32) + zero
    q_tab = call(tables_kernel, array((rows, 128), f32), inverse, flops=1e9)
    w_kv = call(relay_kernel, array((rank, heads * (NOPE + DV))), w_kv, flops=1e9)
    w_up = w_up.reshape(heads * DV, 2 * chips * features)
    w_up_other = call(
        share_out_kernel, array((chips, heads * DV, features)), w_up, flops=1e9, kept=False
    )
    w_up_other = lax.ppermute(w_up_other, "tp", across)
    count = lat + ctx
    step = count + count * ROPE // rank
    kv = call(
        functools.partial(norm_kernel, lat=lat, ctx=ctx),
        array((step, rank)),
        *reduced(kv_parts),
        g_ckv[None],
        q_tab,
    )

    even = sp & (sp - 1) == 0
    planes = [
        lax.ppermute(kv, "sp", [(i, i ^ hop if even else (i + hop) % sp) for i in range(sp)])
        for hop in range(1, sp)
    ]
    near = call(norm_query_kernel, array((step + lat, rank)), *reduced(q_parts), g_cq[None], kv)
    near_own = hopped(near)
    near_other = [lax.ppermute(n, "tp", across) for n in near_own]
    far = call(gather_kernel, array(((sp - 1) * step, rank)), *planes)
    far_own = hopped(far)
    far_other = [lax.ppermute(f, "tp", across) for f in far_own]

    keys = (tp + 2 * (sp - 1)) * count
    query, stats, summed = call(
        functools.partial(near_kernel, lat=lat, ctx=ctx, chips=chips),
        (
            array((heads, rows, 2 * NOPE)),
            array((rows, 128), f32),
            array((heads, rows, DV), f32),
        ),
        q_tab,
        jnp.broadcast_to(ctx_lift[:, None], (heads, 128)),
        jnp.transpose(w_uq, (1, 2, 0)),
        w_kv,
        *near_own,
        *near_other,
        far_own[0],
        far_other[0],
        scratch=[
            pltpu.VMEM((rows, rank), bf16),
            pltpu.VMEM((keys, rank), bf16),
            pltpu.VMEM((keys, 128), bf16),
        ],
        flops=heads * rows * (2 * rank * 256 + 2 * keys * 384),
        limit=16,
    )
    keys = (chips - 1) * (sp - 1) * count
    scratch = [pltpu.VMEM((keys, rank), bf16), pltpu.VMEM((keys, 128), bf16)]
    far_keys, far_values = call(
        functools.partial(expand_kernel, lat=lat, ctx=ctx),
        (array((heads, keys, 2 * NOPE)), array((heads, keys, DV))),
        w_kv,
        *far_own[1:],
        scratch=scratch,
        flops=2 * keys * rank * 256 * heads,
    )
    heads_out, w_up_other = call(
        functools.partial(far_kernel, lat=lat, ctx=ctx),
        (array((rows, heads * DV)), array(w_up_other.shape)),
        query,
        stats,
        summed,
        far_keys,
        far_values,
        w_kv,
        *far_other[1:],
        remote=(w_up_other,),
        scratch=scratch + [pltpu.SemaphoreType.DMA],
        flops=2 * heads * keys * (2 * rows * 384 + rank * 256),
        limit=28,
    )

    heads_other = lax.ppermute(heads_out, "tp", across)
    flops = 2 * rows * heads * DV * chips * features
    branch = call(
        output_own_kernel, array((chips, rows, features), f32), heads_out, w_up, flops=flops
    )
    block = array((rows, features))
    branch, *apart = call(
        output_kernel,
        (array((rows, features), f32),) + (block,) * (chips - 1),
        heads_other,
        w_up_other,
        branch,
        flops=flops,
    )
    apart = [
        lax.ppermute(a, "tp", [(i, i ^ (2 * hop + 2)) for i in range(tp)])
        for hop, a in enumerate(apart)
    ]
    return call(mix_kernel, array(latent.shape), latent, gate, branch, *apart, kept=False)


def chosen(*arrays):
    rows, ctx_rows, features = arrays[0].shape[0], arrays[1].shape[0], arrays[0].shape[1]
    tp = lax.axis_size("tp")
    aligned = rows % (16 * tp) == 0 and ctx_rows % (16 * tp) == 0 and features % 128 == 0 and arrays[6].shape[1] % features == 0
    return (split_device if tp in (2, 4, 8, 16) and aligned else plain_device)(*arrays)


def solution(mesh):
    return jax.shard_map(
        chosen,
        mesh=mesh,
        in_specs=(
            P("sp", "tp"),
            P("sp", "tp"),
            P("sp"),
            P("sp"),
            P("sp", None, "tp"),
            P("tp"),
            P("tp", None),
            P("tp", None),
            P("tp", None),
            P(),
            P(),
            P(None, "tp", None),
            P(None, "tp", None),
            P("tp"),
            P("tp", None, None),
        ),
        out_specs=P("sp", "tp"),
        check_vma=False,
    )
```
